128 devices in a mesh: kv: 32 (over z, y, core), tp: 4 (over x).
Axes of the slice: x: 4, y: 4, z: 4, core: 2. Of those that a mesh axis runs over, the one named last changes fastest.
Arguments:
- tokens: bfloat16 [128, 4, 4096], P(None, None, ('kv', 'tp')), may hold values from -6 to 6
- input_norm_gain: float32 [4096], replicated, may hold values from 0.1 to 1.9
- w_query: bfloat16 [4096, 4096], P(None, 'kv'), may hold values from -0.09375 to 0.09375
- w_forget: bfloat16 [4096, 4096], P(None, 'kv'), may hold values from -0.09375 to 0.09375
- w_input: bfloat16 [32, 128, 4096], P('kv', 'tp'), may hold values from -0.09375 to 0.09375
- w_gate: bfloat16 [32, 128, 4096], P('kv', 'tp'), may hold values from -0.09375 to 0.09375
- forget_floor: float32 [4096], P('kv'), may hold values from 0 to 0.95
- head_gain: float32 [128], P('tp'), may hold values from 0.1 to 1.9
- w_out: bfloat16 [4096, 4096], P('kv'), may hold values from -0.09375 to 0.09375
- state: float32 [128, 32, 128, 128], P(None, 'kv', 'tp'), may hold values from -12 to 12
- prev_forget: float32 [128, 4, 4096], P(None, None, 'kv'), may hold values from 0.2 to 1
- prev_input: bfloat16 [128, 4, 32, 128], P(None, None, 'kv', 'tp'), may hold values from -6 to 6
- accepted: int32 [128], replicated, may hold values from 0 to 4
Outputs:
- mixed: bfloat16 [128, 4, 4096], P(None, None, ('kv', 'tp'))
- new_state: float32 [128, 32, 128, 128], P(None, 'kv', 'tp')
The draws below stay inside these ranges and needn't reach their ends.
All inputs are finite; a program needn't handle non-finite values.
Results may differ from the reference program's by a relative error of at most 0.019.
Values may be sent and summed in bfloat16 or wider, within the bound.
No kernel may reach another device: no remote copies, remote signals or barrier semaphores. Data moves between devices by JAX's collectives and lax.ppermute only.
A program may use at most 64 MiB of HBM per device.

```python
import jax
import jax.numpy as jnp
from jax import lax

D = 4096
HD = 128
HEADS = 32
PROP = 4
SEQS = 128


def draw_state(key, part):
    heads = D // HD
    shape = (SEQS, heads, HD, HD)
    rising = (0.5 * 3.0 ** (jnp.arange(HD, dtype=jnp.float32) / (HD - 1))).reshape(HD, 1)
    base = jnp.clip(jax.random.normal(jax.random.fold_in(key, 13), shape, jnp.float32), -4.0, 4.0)
    values = base * rising
    return jnp.clip(values, -12.0, 12.0).astype(jnp.float32)


def set_ends(values, rng, least, largest):
    place = [jax.random.randint(jax.random.fold_in(rng, axis), (), 0, length) for axis, length in enumerate(values.shape)]
    main_axis = values.shape.index(max(values.shape))
    neighbour = place[:main_axis] + [(place[main_axis] + 1) % values.shape[main_axis]] + place[main_axis + 1:]
    return values.at[tuple(place)].set(least).at[tuple(neighbour)].set(largest)


def level_of(own_key, extent, shards, least, high):
    def one(dim, parts):
        heights = jax.random.uniform(jax.random.fold_in(jax.random.fold_in(own_key, 6), dim), (parts,), jnp.float32, least / len(shards), high / len(shards))
        return jnp.repeat(jnp.exp(heights), extent[dim] // parts).reshape((-1,) + (1,) * (len(extent) - dim - 1))

    level = one(*shards[0])
    for cut in shards[1:]:
        level = level * one(*cut)
    return level


def gaussian(key, shape, width, bound, pieces=(), held_as=jnp.bfloat16):
    values = width * jax.random.normal(key, shape, jnp.float32)
    if pieces:
        values = values * level_of(key, shape, pieces, -0.22, 0.18)
    return jnp.clip(values, -bound, bound).astype(held_as)


def setup_inputs(seed: int = 0) -> dict:
    key_list = jax.random.split(jax.random.key(seed), 14)
    return {
        "tokens": gaussian(key_list[0], (SEQS, PROP, D), 1.0, 6.0, ((2, 128),)),
        "input_norm_gain": jnp.clip(1.0 + 0.18 * jax.random.normal(key_list[1], (D,), jnp.float32), 0.1, 1.9),
        "w_query": gaussian(key_list[2], (D, D), D ** -0.5, 0.09375, ((1, 32),)),
        "w_forget": gaussian(key_list[3], (D, D), D ** -0.5, 0.09375, ((1, 32),)),
        "w_input": gaussian(key_list[4], (HEADS, HD, D), D ** -0.5, 0.09375, ((0, 32), (1, 4))),
        "w_gate": gaussian(key_list[5], (HEADS, HD, D), D ** -0.5, 0.09375, ((0, 32), (1, 4))),
        "forget_floor": jnp.clip(0.95 * jax.random.uniform(key_list[6], (D,), jnp.float32) ** level_of(key_list[6], (D,), ((0, 32),), -0.2, 0.2), 0.0, 0.95),
        "head_gain": jnp.clip(1.0 + 0.18 * jax.random.normal(key_list[7], (HD,), jnp.float32), 0.1, 1.9),
        "w_out": gaussian(key_list[8], (D, D), D ** -0.5, 0.09375, ((0, 32),)),
        "state": draw_state(jax.random.fold_in(key_list[13], 71), 0),
        "prev_forget": jnp.clip(0.2 + 0.8 * jax.random.uniform(key_list[10], (SEQS, PROP, D), jnp.float32) ** level_of(key_list[10], (SEQS, PROP, D), ((2, 32),), -0.2, 0.2), 0.2, 1.0),
        "prev_input": gaussian(key_list[11], (SEQS, PROP, HEADS, HD), 1.0, 6.0, ((2, 32), (3, 4))),
        "accepted": set_ends(jax.random.randint(key_list[12], (SEQS,), 0, PROP + 1), jax.random.fold_in(key_list[12], 1), 0, PROP).astype(jnp.int32),
    }


NORM_EPSILON = 1e-06

def rms_scale(values, gain):
    return values * lax.rsqrt(lax.optimization_barrier(jnp.mean(values * values, axis=-1, keepdims=True)) + NORM_EPSILON) * gain

def reference(tokens, input_norm_gain, w_query, w_forget, w_input, w_gate, forget_floor, head_gain, w_out, state, prev_forget, prev_input, accepted):
    seq_count = tokens.shape[0]
    heads = D // HD
    row_count = seq_count * PROP
    normed = rms_scale(tokens.astype(jnp.float32), input_norm_gain).astype(jnp.bfloat16).reshape(row_count, D)

    def project(weight):
        return jnp.dot(normed, weight, preferred_element_type=jnp.float32).astype(jnp.bfloat16)
    queries = project(w_query)
    forget_raw = project(w_forget)
    input_proj = project(w_input.reshape(D, D).T)
    gate_raw = project(w_gate.reshape(D, D).T)
    forget = forget_floor + (1.0 - forget_floor) * jax.nn.sigmoid(forget_raw.astype(jnp.float32))

    def head_first(values):
        return values.astype(jnp.float32).reshape(seq_count, PROP, heads, HD).transpose(2, 0, 1, 3)

    def advance_head(inputs_all):
        start_state, prev_gate, earlier_values, query_vector, gate_now_all, fresh = inputs_all
        present_step = start_state
        for token_position in range(PROP):
            alive_mask = (token_position < accepted)[:, None, None]
            gate_now = prev_gate[:, token_position]
            update = gate_now[:, :, None] * present_step + (1.0 - gate_now)[:, :, None] * earlier_values[:, token_position][:, None, :]
            present_step = jnp.where(alive_mask, update, present_step)
        base_state = present_step
        output_tokens = []
        for token_position in range(PROP):
            gate_now = gate_now_all[:, token_position]
            present_step = gate_now[:, :, None] * present_step + (1.0 - gate_now)[:, :, None] * fresh[:, token_position][:, None, :]
            output_tokens.append(jnp.einsum('ue,uef->uf', query_vector[:, token_position], present_step))
        return (base_state, jnp.stack(output_tokens, axis=1))
    inputs_all = (state.transpose(1, 0, 3, 2), head_first(prev_forget), head_first(prev_input), head_first(queries), head_first(forget), head_first(input_proj))
    base_states, head_outputs = lax.map(advance_head, inputs_all)
    new_state = base_states.transpose(1, 0, 3, 2)
    heads_out = head_outputs.transpose(1, 2, 0, 3)
    gate_heads = gate_raw.astype(jnp.float32).reshape(seq_count, PROP, heads, HD)
    hidden = (rms_scale(heads_out, head_gain) * jax.nn.silu(gate_heads)).astype(jnp.bfloat16).reshape(row_count, D)
    mixed = jnp.dot(hidden, w_out, preferred_element_type=jnp.float32).astype(jnp.bfloat16).reshape(seq_count, PROP, D)
    return (mixed, new_state)
```

```python
import jax
import jax.numpy as jnp
from jax import lax
from jax.experimental import pallas as pl
from jax.experimental.pallas import tpu as pltpu
from jax.sharding import Mesh, PartitionSpec as P

NORM_EPSILON = 1e-06
LANES = 128


def whole():
    return pl.BlockSpec(memory_space=pltpu.VMEM)


def shaped(shape, dtype):
    return jax.ShapeDtypeStruct(shape, dtype)


def call(kernel, out_shape, scratch, cost, limit, name, in_specs, out_specs):
    return pl.pallas_call(
        kernel,
        out_shape=out_shape,
        in_specs=in_specs,
        out_specs=out_specs,
        scratch_shapes=scratch,
        name=name,
        cost_estimate=pl.CostEstimate(flops=cost[0], bytes_accessed=cost[1], transcendentals=0),
        compiler_params=pltpu.CompilerParams(vmem_limit_bytes=limit),
    )


def advance_kernel(accepted, prev_forget, prev_input, state, new_state, rounded):
    block = pl.program_id(0)
    count, proposals, size = prev_forget.shape
    lanes = prev_input.shape[2]
    shift = lax.rem(lanes - block * count, lanes)
    values = [
        pltpu.roll(prev_input[p].astype(jnp.float32), shift, 1) for p in range(proposals)
    ]
    for s in range(count):
        live = accepted[block * count + s]
        rest = jnp.ones((1, size), jnp.float32)
        added = None
        for p in reversed(range(proposals)):
            gate = prev_forget[s, pl.ds(p, 1), :]
            gate = jnp.where(p < live, gate, 1.0)
            term = (rest * (1.0 - gate)) * values[p][:, s : s + 1]
            added = term if added is None else added + term
            rest = rest * gate
        fresh = rest * state[s] + added
        new_state[s] = fresh
        rounded[s] = fresh.astype(jnp.bfloat16)


def advance(accepted, prev_forget, prev_input, state):
    seqs, values, keys = state.shape
    proposals = prev_forget.shape[1]
    count = 16
    return pl.pallas_call(
        advance_kernel,
        grid=(seqs // count,),
        in_specs=[
            pl.BlockSpec(memory_space=pltpu.SMEM),
            pl.BlockSpec((count, proposals, keys), lambda i: (i, 0, 0)),
            pl.BlockSpec((proposals, values, seqs), lambda i: (0, 0, 0)),
            pl.BlockSpec((count, values, keys), lambda i: (i, 0, 0)),
        ],
        out_specs=[
            pl.BlockSpec((count, values, keys), lambda i: (i, 0, 0)),
            pl.BlockSpec((count, values, keys), lambda i: (i, 0, 0)),
        ],
        out_shape=[shaped(state.shape, jnp.float32), shaped(state.shape, jnp.bfloat16)],
        name="advance",
        cost_estimate=pl.CostEstimate(flops=4_000_000_000, bytes_accessed=6 << 20, transcendentals=0),
        compiler_params=pltpu.CompilerParams(vmem_limit_bytes=8 << 20),
    )(accepted, prev_forget, prev_input, state)


def turn_kernel(gain, w_query, w_forget, w_out, keyed, outward):
    size = w_out.shape[0]
    for b in range(w_query.shape[0] // size):
        at = pl.ds(b * size, size)
        row = gain[pl.ds(b, 1), :]
        for i, weight in enumerate((w_query, w_forget)):
            block = weight[at, :].astype(jnp.float32).T
            keyed[pl.ds(i * size, size), at] = (block * row).astype(jnp.bfloat16)
        outward[b] = w_out[:, at].astype(jnp.float32).T.astype(jnp.bfloat16)


def turn(gain, w_query, w_forget, w_out):
    width, size = w_query.shape
    return call(
        turn_kernel,
        [
            shaped((2 * size, width), jnp.bfloat16),
            shaped((width // size, size, size), jnp.bfloat16),
        ],
        [],
        (4_000_000_000, 6 << 20),
        16 << 20,
        "turn",
        [whole()] * 4,
        [whole()] * 2,
    )(gain, w_query, w_forget, w_out)


def project_kernel(own, other, gain, keyed, w0, w1, w2, w3, o0, o1, o2, o3, held):
    core = lax.axis_index("core")
    blocks, size, seqs = own.shape
    squares = jnp.zeros((8, seqs), jnp.float32)
    for b in range(blocks):
        for half, ref in ((core, own), (1 - core, other)):
            row = 2 * b + half
            part = ref[b]
            held[pl.ds(pl.multiple_of(row * size, size), size), :] = part
            wide = part.astype(jnp.float32)
            squares = squares + jnp.sum((wide * wide).reshape(size // 8, 8, seqs), axis=0)
    total = jnp.sum(squares, axis=0, keepdims=True)
    factor = lax.rsqrt(total / (2 * blocks * size) + NORM_EPSILON)
    rows = held[...]
    first = jnp.dot(keyed[...], rows, preferred_element_type=jnp.float32) * factor
    first = first.astype(jnp.bfloat16)
    keys = first.shape[0]
    for weight, out in ((w0, o0), (w3, o1), (w2, o2), (w1, o3)):
        out[pl.ds(0, keys), :] = first
        second = jnp.dot(weight[...], rows, preferred_element_type=jnp.float32) * factor
        out[pl.ds(keys, second.shape[0]), :] = second.astype(jnp.bfloat16)


def project(own, other, gain, keyed, weights):
    blocks, size, seqs = own.shape
    rows = keyed.shape[0] + weights[0].shape[0]
    return call(
        project_kernel,
        [shaped((rows, seqs), jnp.bfloat16)] * 4,
        [pltpu.VMEM((2 * blocks * size, seqs), jnp.bfloat16)],
        (1_000_000_000, 6 << 20),
        16 << 20,
        "project",
        [whole()] * 8,
        [whole()] * 4,
    )(own, other, gain, keyed, *weights)


def recur_kernel(r0, r1, r2, r3, before, floor, head_gain, o0, o1, o2, o3, seen, ready):
    mine = lax.axis_index("tp")
    size = floor.shape[1]
    values = head_gain.shape[1]
    count = before.shape[0] // values
    steps = 4
    for d, ref in enumerate((r0, r1, r2, r3)):
        seen[lax.rem(mine + steps - d, steps)] = ref[...]
    low = jnp.broadcast_to(floor[...], (count, size)).T
    scale = jnp.broadcast_to(head_gain[...], (count, values)).T
    forget, keys, fresh, sums, asked = [], [], [], [], []
    for t in range(steps):
        gate = low + (1.0 - low) * jax.nn.sigmoid(seen[t, pl.ds(size, size), :].astype(jnp.float32))
        forget.append(gate)
        keys.append(1.0 - gate)
        fresh.append(seen[t, pl.ds(2 * size, values), :].astype(jnp.float32))
    for t in range(steps):
        moved = seen[t, pl.ds(0, size), :].astype(jnp.float32)
        out = None
        for u in reversed(range(t + 1)):
            score = jnp.sum(moved * keys[u], axis=0, keepdims=True)
            term = score * fresh[u]
            out = term if out is None else out + term
            moved = moved * forget[u]
        sums.append(out)
        asked.append(moved.astype(jnp.bfloat16))
    lane = lax.broadcasted_iota(jnp.int32, (values, count), 1)
    asked = jnp.concatenate(asked, axis=1)
    group = 8
    for b in range(count // group):
        read = jnp.dot(
            before[pl.ds(b * group * values, group * values), :],
            asked,
            preferred_element_type=jnp.float32,
        )
        for s in range(group):
            hit = lane == b * group + s
            for t in range(steps):
                part = read[s * values : (s + 1) * values, t * count : (t + 1) * count]
                sums[t] = sums[t] + jnp.where(hit, part, 0.0)
    for t in range(steps):
        out = sums[t]
        square = jnp.sum(out * out, axis=0, keepdims=True)
        gate = seen[t, pl.ds(2 * size + values, values), :].astype(jnp.float32)
        shown = out * scale * (gate * jax.nn.sigmoid(gate))
        ready[t, pl.ds(0, values), :] = shown.astype(jnp.bfloat16)
        high = square.astype(jnp.bfloat16).astype(jnp.float32)
        middle = (square - high).astype(jnp.bfloat16).astype(jnp.float32)
        lower = square - high - middle
        which = lax.broadcasted_iota(jnp.int32, (16, count), 0)
        tail = jnp.where(which == 0, high, jnp.where(which == 1, middle, jnp.where(which == 2, lower, 0.0)))
        ready[t, pl.ds(values, 16), :] = tail.astype(jnp.bfloat16)
    for d, ref in enumerate((o0, o1, o2, o3)):
        ref[...] = ready[lax.rem(mine + d, steps)]


def recur(received, before, floor, head_gain):
    rows, count = received[0].shape
    values = head_gain.shape[1]
    return call(
        recur_kernel,
        [shaped((values + 16, count), jnp.bfloat16)] * 4,
        [
            pltpu.VMEM((4, rows, count), jnp.bfloat16),
            pltpu.VMEM((4, values + 16, count), jnp.bfloat16),
        ],
        (1_000_000_000, 2 << 20),
        16 << 20,
        "recur",
        [whole()] * 7,
        [whole()] * 4,
    )(*received, before, floor, head_gain)


def gathered(parts, joined):
    mine = lax.axis_index("tp")
    values = joined.shape[0] // 4
    total = None
    for d, ref in enumerate(parts):
        at = pl.multiple_of(lax.rem(mine + 4 - d, 4) * values, values)
        joined[pl.ds(at, values), :] = ref[pl.ds(0, values), :]
        square = jnp.sum(ref[pl.ds(values, 16), :].astype(jnp.float32), axis=0, keepdims=True)
        total = square if total is None else total + square
    return lax.rsqrt(total / joined.shape[0] + NORM_EPSILON)


def away_kernel(p0, p1, p2, p3, outward, sent, joined):
    core = lax.axis_index("core")
    factor = gathered((p0, p1, p2, p3), joined)
    for b in range(sent.shape[0]):
        part = jnp.dot(outward[2 * b + 1 - core], joined[...], preferred_element_type=jnp.float32)
        sent[b] = (part * factor).astype(jnp.bfloat16)


def keep_kernel(p0, p1, p2, p3, outward, came, kept, joined):
    core = lax.axis_index("core")
    factor = gathered((p0, p1, p2, p3), joined)
    for b in range(kept.shape[0]):
        part = jnp.dot(outward[2 * b + core], joined[...], preferred_element_type=jnp.float32)
        kept[b] = (part * factor + came[b].astype(jnp.float32)).astype(jnp.bfloat16)


def outward_half(kernel, name, parts, outward, *more):
    blocks, size, count = outward.shape
    return call(
        kernel,
        shaped((blocks // 2, size, parts[0].shape[1]), jnp.bfloat16),
        [pltpu.VMEM((size, parts[0].shape[1]), jnp.bfloat16)],
        (100_000_000, 2 << 20),
        16 << 20,
        name,
        [whole()] * (5 + len(more)),
        whole(),
    )(*parts, outward, *more)


def sum_kernel(parts, out):
    total = parts[0].astype(jnp.float32)
    for b in range(1, parts.shape[0]):
        total = total + parts[b].astype(jnp.float32)
    out[...] = total.astype(out.dtype)


def body(
    tokens,
    input_norm_gain,
    w_query,
    w_forget,
    w_input,
    w_gate,
    forget_floor,
    head_gain,
    w_out,
    state,
    prev_forget,
    prev_input,
    accepted,
):
    planes, group = lax.axis_size("zy"), lax.axis_size("tp")
    seqs, proposals, features = tokens.shape
    size = forget_floor.shape[0]
    swap = [(0, 1), (1, 0)]
    hops = [[(i, (i + d) % group) for i in range(group)] for d in range(group)]

    gain = input_norm_gain.reshape(-1, size)
    mixing = jnp.concatenate([w_input[0], w_gate[0]], axis=0).astype(jnp.float32)
    mixing = (mixing * input_norm_gain[None, :]).astype(jnp.bfloat16)
    weights = [mixing] + [lax.ppermute(mixing, "tp", hops[d]) for d in (1, 2, 3)]

    turned = tokens.transpose(1, 2, 0)
    spread = jnp.broadcast_to(turned[None], (planes, *turned.shape))
    spread = spread.reshape(planes * group, features, seqs)
    own = lax.all_to_all(spread, ("zy", "tp"), 0, 0, tiled=True)
    own = own.reshape(planes, group * features, seqs)
    other = lax.ppermute(own, "core", swap)

    new_state, rounded = advance(
        accepted, prev_forget, prev_input.reshape(seqs, proposals, -1).transpose(1, 2, 0), state[:, 0]
    )
    keyed, outward = turn(gain, w_query, w_forget, w_out)

    sends = project(own, other, gain, keyed, weights)
    received = [sends[0]] + [lax.ppermute(sends[d], "tp", hops[d]) for d in (1, 2, 3)]
    shown = recur(received, rounded.reshape(-1, size), forget_floor[None], head_gain[None])
    parts = [shown[0]] + [lax.ppermute(shown[d], "tp", hops[d]) for d in (1, 2, 3)]
    sent = outward_half(away_kernel, "away", parts, outward)
    came = lax.ppermute(sent, "core", swap)
    kept = outward_half(keep_kernel, "keep", parts, outward, came)
    terms = lax.all_to_all(
        kept.reshape(planes * group, features, seqs), ("zy", "tp"), 0, 0, tiled=True
    )
    mixed = call(
        sum_kernel,
        shaped((group, features, seqs), jnp.bfloat16),
        [],
        (1_000_000, 1 << 20),
        8 << 20,
        "sum",
        [whole()],
        whole(),
    )(terms.reshape(planes, group, features, seqs))
    return mixed.transpose(2, 0, 1), new_state[:, None]


def solution(mesh):
    kv, tp = mesh.shape["kv"], mesh.shape["tp"]
    finer = Mesh(mesh.devices.reshape(kv // 2, 2, tp), ("zy", "core", "tp"))
    rows = ("zy", "core")
    placed = (
        P(None, None, (*rows, "tp")),
        P(),
        P(None, rows),
        P(None, rows),
        P(rows, "tp", None),
        P(rows, "tp", None),
        P(rows),
        P("tp"),
        P(rows, None),
        P(None, rows, "tp", None),
        P(None, None, rows),
        P(None, None, rows, "tp"),
        P(),
    )
    return jax.shard_map(
        body,
        mesh=finer,
        in_specs=placed,
        out_specs=(P(None, None, (*rows, "tp")), P(None, rows, "tp", None)),
        check_vma=False,
    )
```

```python
import functools

import jax
import jax.numpy as jnp
from jax import lax
from jax.experimental import pallas as pl
from jax.experimental.pallas import tpu as pltpu
from jax.sharding import Mesh, PartitionSpec as P

NORM_EPSILON = 1e-06
LANES = 128


def whole():
    return pl.BlockSpec(memory_space=pltpu.VMEM)


def shaped(shape, dtype):
    return jax.ShapeDtypeStruct(shape, dtype)


def call(kernel, out_shape, scratch, cost, limit, name, in_specs, out_specs):
    return pl.pallas_call(
        kernel,
        out_shape=out_shape,
        in_specs=in_specs,
        out_specs=out_specs,
        scratch_shapes=scratch,
        name=name,
        cost_estimate=pl.CostEstimate(flops=cost[0], bytes_accessed=cost[1], transcendentals=0),
        compiler_params=pltpu.CompilerParams(vmem_limit_bytes=limit),
    )


def advance_kernel(first, accepted, prev_forget, prev_input, state, *refs):
    new_state, rounded = refs[-2:]
    block = first + pl.program_id(0)
    count, proposals, size = prev_forget.shape
    lanes = prev_input.shape[2]
    shift = lax.rem(lanes - block * count, lanes)
    values = [
        pltpu.roll(prev_input[p].astype(jnp.float32), shift, 1) for p in range(proposals)
    ]
    for s in range(count):
        live = accepted[block * count + s]
        rest = jnp.ones((1, size), jnp.float32)
        added = None
        for p in reversed(range(proposals)):
            gate = prev_forget[s, pl.ds(p, 1), :]
            gate = jnp.where(p < live, gate, 1.0)
            term = (rest * (1.0 - gate)) * values[p][:, s : s + 1]
            added = term if added is None else added + term
            rest = rest * gate
        fresh = rest * state[s] + added
        new_state[s] = fresh
        rounded[s] = fresh.astype(jnp.bfloat16)


def advance(accepted, prev_forget, prev_input, state, first, blocks, earlier=()):
    seqs, values, keys = state.shape
    proposals = prev_forget.shape[1]
    count = 16
    span = pl.BlockSpec((count, values, keys), lambda i: (first + i, 0, 0))
    return pl.pallas_call(
        functools.partial(advance_kernel, first),
        grid=(blocks,),
        in_specs=[
            pl.BlockSpec(memory_space=pltpu.SMEM),
            pl.BlockSpec((count, proposals, keys), lambda i: (first + i, 0, 0)),
            pl.BlockSpec((proposals, values, seqs), lambda i: (0, 0, 0)),
            span,
        ]
        + [pl.BlockSpec(memory_space=pl.ANY)] * len(earlier),
        out_specs=[span, span],
        out_shape=[shaped(state.shape, jnp.float32), shaped(state.shape, jnp.bfloat16)],
        input_output_aliases={4: 0, 5: 1} if earlier else {},
        name="advance",
        cost_estimate=pl.CostEstimate(
            flops=1_000_000_000, bytes_accessed=blocks << 20, transcendentals=0
        ),
        compiler_params=pltpu.CompilerParams(vmem_limit_bytes=60 << 20),
    )(accepted, prev_forget, prev_input, state, *earlier)


def split_in_three(value):
    high = value.astype(jnp.bfloat16).astype(jnp.float32)
    middle = (value - high).astype(jnp.bfloat16).astype(jnp.float32)
    return high, middle, value - high - middle


def three_rows(parts, width):
    rest = jnp.zeros((16 - 3 * parts[0].shape[0], width), jnp.float32)
    return jnp.concatenate([*parts, rest], axis=0).astype(jnp.bfloat16)


def source_kernel(tokens, gain, out, columns):
    steps, features, seqs = tokens.shape
    size = gain.shape[1]
    row = 2 * lax.axis_index("zy") + lax.axis_index("core")
    columns[...] = jnp.broadcast_to(gain[pl.ds(row, 1), :], (size, size)).T
    at = pl.multiple_of(lax.axis_index("tp") * features, features)
    scale = columns[pl.ds(at, features), :]
    squares = []
    for t in range(steps):
        wide = tokens[t].astype(jnp.float32)
        squares.append(jnp.sum(wide * wide, axis=0, keepdims=True))
        scaled = (wide * scale).astype(jnp.bfloat16)
        for z in range(out.shape[0]):
            out[z, pl.ds(t * features, features), :] = scaled
    tail = three_rows(split_in_three(jnp.concatenate(squares, axis=0)), seqs)
    for z in range(out.shape[0]):
        out[z, pl.ds(steps * features, 16), :] = tail


def source(tokens, gain, planes):
    steps, features, seqs = tokens.shape
    size = gain.shape[1]
    return call(
        source_kernel,
        shaped((planes, steps * features + 16, seqs), jnp.bfloat16),
        [pltpu.VMEM((size, seqs), jnp.float32)],
        (1_000_000, 1 << 20),
        8 << 20,
        "source",
        [whole()] * 2,
        whole(),
    )(tokens, gain)


def turn_kernel(w_query, w_forget, w_input, w_gate, keyed, m0, m1, m2, m3, rows, mixed, sems):
    mine = lax.axis_index("tp")
    group, part, size = 4, rows.shape[2], w_query.shape[2]
    at = pl.multiple_of(mine * part, part)
    copies = [
        pltpu.make_async_copy(w_input.at[0], mixed.at[0], sems.at[0]),
        pltpu.make_async_copy(w_gate.at[0], mixed.at[1], sems.at[1]),
        pltpu.make_async_copy(w_query.at[:, pl.ds(at, part), :], rows.at[0], sems.at[2]),
        pltpu.make_async_copy(w_forget.at[:, pl.ds(at, part), :], rows.at[1], sems.at[3]),
    ]
    for copy in copies:
        copy.start()
    copies[0].wait()
    copies[1].wait()
    lane = lax.broadcasted_iota(jnp.int32, (2 * part, size), 1) // part
    for q in range(rows.shape[1] // group):
        to = pl.ds(q * size, size)
        blocks = []
        for k in range(group):
            cut = pl.ds((q * group + k) * size, size)
            both = [mixed[i, :, cut].astype(jnp.float32) for i in range(2)]
            blocks.append(jnp.concatenate(both, axis=0))
        for d, out in enumerate((m0, m1, m2, m3)):
            theirs = lax.rem(mine + d, group)
            total = None
            for k in range(group):
                turned = pltpu.roll(blocks[k], lax.rem(group + k - theirs, group) * part, 1)
                total = turned if total is None else jnp.where(lane == k, turned, total)
            out[:, to] = total.astype(jnp.bfloat16)
    copies[2].wait()
    copies[3].wait()
    for q in range(rows.shape[1] // group):
        for i in range(2):
            block = rows[i, pl.ds(q * group, group)].astype(jnp.float32).reshape(size, size)
            keyed[pl.ds(i * size, size), pl.ds(q * size, size)] = block.T.astype(jnp.bfloat16)


def turn(w_query, w_forget, w_input, w_gate):
    width, size = w_query.shape
    values = w_input.shape[1]
    far = pl.BlockSpec(memory_space=pltpu.HBM)
    outs = call(
        turn_kernel,
        [shaped((2 * size, width // 4), jnp.bfloat16)]
        + [shaped((2 * values, width // 4), jnp.bfloat16)] * 4,
        [
            pltpu.VMEM((2, width // size, size // 4, size), jnp.bfloat16),
            pltpu.VMEM((2, values, width), jnp.bfloat16),
            pltpu.SemaphoreType.DMA((4,)),
        ],
        (1_000_000_000, 2 << 20),
        16 << 20,
        "turn",
        [far] * 4,
        [whole()] * 5,
    )(
        w_query.reshape(width // size, size, size),
        w_forget.reshape(width // size, size, size),
        w_input,
        w_gate,
    )
    return outs[0], outs[1:]


def outward_kernel(w_out, outward, held, sems):
    cuts, size, span = held.shape
    copies = [
        pltpu.make_async_copy(w_out.at[:, pl.ds(c * span, span)], held.at[c], sems.at[c])
        for c in range(cuts)
    ]
    for copy in copies:
        copy.start()
    for c in range(cuts):
        copies[c].wait()
        for b in range(span // size):
            block = held[c, :, pl.ds(b * size, size)].astype(jnp.float32)
            outward[c * (span // size) + b] = block.T.astype(jnp.bfloat16)


def turn_outward(w_out):
    size, width = w_out.shape
    return call(
        outward_kernel,
        shaped((width // size, size, size), jnp.bfloat16),
        [pltpu.VMEM((4, size, width // 4), jnp.bfloat16), pltpu.SemaphoreType.DMA((4,))],
        (1_000_000_000, 2 << 20),
        16 << 20,
        "outward",
        [pl.BlockSpec(memory_space=pltpu.HBM)],
        whole(),
    )(w_out)


def project_kernel(own, other, keyed, w0, w1, w2, w3, o0, o1, o2, o3, held, ready):
    core, mine = lax.axis_index("core"), lax.axis_index("tp")
    blocks, _, seqs = own.shape
    group, keys = 4, keyed.shape[0]
    part = held.shape[0] // (2 * blocks)
    squares = jnp.zeros((16, seqs), jnp.float32)
    for half, ref in ((core, own), (1 - core, other)):
        for b in range(blocks):
            at = pl.multiple_of((2 * b + half) * part, part)
            for t in range(group):
                held[pl.ds(at, part), pl.ds(t * seqs, seqs)] = ref[b, pl.ds(t * part, part), :]
            squares = squares + ref[b, pl.ds(group * part, 16), :].astype(jnp.float32)
    totals = squares[0:4] + squares[4:8] + squares[8:12]
    rows = held[...]
    first = jnp.dot(keyed[...], rows, preferred_element_type=jnp.float32).astype(jnp.bfloat16)
    for t in range(group):
        ready[t, pl.ds(0, keys), :] = first[:, t * seqs : (t + 1) * seqs]
        tail = three_rows(split_in_three(totals[t : t + 1]), seqs)
        ready[t, pl.ds(ready.shape[1] - 16, 16), :] = tail
    for d, weight in enumerate((w0, w1, w2, w3)):
        more = weight.shape[0]
        at = pl.multiple_of(keys + lax.rem(mine + group - d, group) * more, more)
        second = jnp.dot(weight[...], rows, preferred_element_type=jnp.float32).astype(jnp.bfloat16)
        for t in range(group):
            ready[t, pl.ds(at, more), :] = second[:, t * seqs : (t + 1) * seqs]
    for d, out in enumerate((o0, o1, o2, o3)):
        out[...] = ready[lax.rem(mine + d, group)]


def project(own, other, keyed, weights):
    blocks, _, seqs = own.shape
    keys, width = keyed.shape
    rows = keys + 4 * weights[0].shape[0] + 16
    return call(
        project_kernel,
        [shaped((rows, seqs), jnp.bfloat16)] * 4,
        [pltpu.VMEM((width, 4 * seqs), jnp.bfloat16), pltpu.VMEM((4, rows, seqs), jnp.bfloat16)],
        (1_000_000_000, 3 << 20),
        16 << 20,
        "project",
        [whole()] * 7,
        [whole()] * 4,
    )(own, other, keyed, *weights)


def finish_kernel(width, p0, p1, p2, p3, o0, o1, o2, o3, held):
    mine = lax.axis_index("tp")
    group = 4
    rows, keys = held.shape[0], o0.shape[0] * 4 // 5
    total = sum(ref[pl.ds(rows, 16), :].astype(jnp.float32) for ref in (p0, p1, p2, p3))
    factor = lax.rsqrt(jnp.sum(total, axis=0, keepdims=True) / width + NORM_EPSILON)
    value = sum(ref[pl.ds(0, rows), :].astype(jnp.float32) for ref in (p0, p1, p2, p3))
    held[...] = (value * factor).astype(jnp.bfloat16)
    more = (rows - keys) // group
    for d, out in enumerate((o0, o1, o2, o3)):
        at = pl.multiple_of(keys + lax.rem(mine + d, group) * more, more)
        out[pl.ds(0, keys), :] = held[pl.ds(0, keys), :]
        out[pl.ds(keys, more), :] = held[pl.ds(at, more), :]


def finish(parts, keys, width):
    rows, seqs = parts[0].shape
    rows = rows - 16
    return call(
        functools.partial(finish_kernel, width),
        [shaped((keys + (rows - keys) // 4, seqs), jnp.bfloat16)] * 4,
        [pltpu.VMEM((rows, seqs), jnp.bfloat16)],
        (100_000_000, 1 << 20),
        16 << 20,
        "finish",
        [whole()] * 4,
        [whole()] * 4,
    )(*parts)


def recur_kernel(r0, r1, r2, r3, before, floor, head_gain, o0, o1, o2, o3, seen, ready):
    mine = lax.axis_index("tp")
    size = floor.shape[1]
    values = head_gain.shape[1]
    count = before.shape[0] // values
    steps = 4
    for d, ref in enumerate((r0, r1, r2, r3)):
        seen[lax.rem(mine + steps - d, steps)] = ref[...]
    low = jnp.broadcast_to(floor[...], (count, size)).T
    scale = jnp.broadcast_to(head_gain[...], (count, values)).T
    forget, keys, fresh, sums, asked = [], [], [], [], []
    for t in range(steps):
        gate = low + (1.0 - low) * jax.nn.sigmoid(seen[t, pl.ds(size, size), :].astype(jnp.float32))
        forget.append(gate)
        keys.append(1.0 - gate)
        fresh.append(seen[t, pl.ds(2 * size, values), :].astype(jnp.float32))
    for t in range(steps):
        moved = seen[t, pl.ds(0, size), :].astype(jnp.float32)
        out = None
        for u in reversed(range(t + 1)):
            score = jnp.sum(moved * keys[u], axis=0, keepdims=True)
            term = score * fresh[u]
            out = term if out is None else out + term
            moved = moved * forget[u]
        sums.append(out)
        asked.append(moved.astype(jnp.bfloat16))
    lane = lax.broadcasted_iota(jnp.int32, (values, count), 1)
    asked = jnp.concatenate(asked, axis=1)
    group = 8
    for b in range(count // group):
        read = jnp.dot(
            before[pl.ds(b * group * values, group * values), :],
            asked,
            preferred_element_type=jnp.float32,
        )
        for s in range(group):
            hit = lane == b * group + s
            for t in range(steps):
                part = read[s * values : (s + 1) * values, t * count : (t + 1) * count]
                sums[t] = sums[t] + jnp.where(hit, part, 0.0)
    for t in range(steps):
        out = sums[t]
        square = jnp.sum(out * out, axis=0, keepdims=True)
        gate = seen[t, pl.ds(2 * size + values, values), :].astype(jnp.float32)
        shown = out * scale * (gate * jax.nn.sigmoid(gate))
        ready[t, pl.ds(0, values), :] = shown.astype(jnp.bfloat16)
        ready[t, pl.ds(values, 16), :] = three_rows(split_in_three(square), count)
    for d, ref in enumerate((o0, o1, o2, o3)):
        ref[...] = ready[lax.rem(mine + d, steps)]


def recur(received, before, floor, head_gain):
    rows, count = received[0].shape
    values = head_gain.shape[1]
    return call(
        recur_kernel,
        [shaped((values + 16, count), jnp.bfloat16)] * 4,
        [
            pltpu.VMEM((4, rows, count), jnp.bfloat16),
            pltpu.VMEM((4, values + 16, count), jnp.bfloat16),
        ],
        (1_000_000_000, 2 << 20),
        16 << 20,
        "recur",
        [whole()] * 7,
        [whole()] * 4,
    )(*received, before, floor, head_gain)


def gathered(parts, joined):
    mine = lax.axis_index("tp")
    values = joined.shape[0] // 4
    total = None
    for d, ref in enumerate(parts):
        at = pl.multiple_of(lax.rem(mine + 4 - d, 4) * values, values)
        joined[pl.ds(at, values), :] = ref[pl.ds(0, values), :]
        square = jnp.sum(ref[pl.ds(values, 16), :].astype(jnp.float32), axis=0, keepdims=True)
        total = square if total is None else total + square
    return lax.rsqrt(total / joined.shape[0] + NORM_EPSILON)


def away_kernel(p0, p1, p2, p3, outward, sent, joined):
    core = lax.axis_index("core")
    factor = gathered((p0, p1, p2, p3), joined)
    for b in range(sent.shape[0]):
        part = jnp.dot(outward[2 * b + 1 - core], joined[...], preferred_element_type=jnp.float32)
        sent[b] = (part * factor).astype(jnp.bfloat16)


def keep_kernel(p0, p1, p2, p3, outward, came, kept, joined):
    core = lax.axis_index("core")
    factor = gathered((p0, p1, p2, p3), joined)
    for b in range(kept.shape[0]):
        part = jnp.dot(outward[2 * b + core], joined[...], preferred_element_type=jnp.float32)
        kept[b] = (part * factor + came[b].astype(jnp.float32)).astype(jnp.bfloat16)


def outward_half(kernel, name, parts, outward, *more):
    blocks, size, count = outward.shape
    return call(
        kernel,
        shaped((blocks // 2, size, parts[0].shape[1]), jnp.bfloat16),
        [pltpu.VMEM((size, parts[0].shape[1]), jnp.bfloat16)],
        (100_000_000, 2 << 20),
        16 << 20,
        name,
        [whole()] * (5 + len(more)),
        whole(),
    )(*parts, outward, *more)


def sum_kernel(parts, o0, o1, o2, o3, held):
    mine = lax.axis_index("tp")
    total = parts[0].astype(jnp.float32)
    for b in range(1, parts.shape[0]):
        total = total + parts[b].astype(jnp.float32)
    held[...] = total.astype(jnp.bfloat16).reshape(held.shape)
    for d, out in enumerate((o0, o1, o2, o3)):
        out[...] = held[lax.rem(mine + d, 4)]


def sums(parts):
    _, size, seqs = parts.shape
    return call(
        sum_kernel,
        [shaped((size // 4, seqs), jnp.bfloat16)] * 4,
        [pltpu.VMEM((4, size // 4, seqs), jnp.bfloat16)],
        (1_000_000, 1 << 20),
        8 << 20,
        "sums",
        [whole()],
        [whole()] * 4,
    )(parts)


def place_kernel(p0, p1, p2, p3, out):
    mine = lax.axis_index("tp")
    for d, ref in enumerate((p0, p1, p2, p3)):
        out[lax.rem(mine + 4 - d, 4)] = ref[...]


def place(parts):
    return call(
        place_kernel,
        shaped((4, *parts[0].shape), jnp.bfloat16),
        [],
        (1_000_000, 1 << 17),
        8 << 20,
        "place",
        [whole()] * 4,
        whole(),
    )(*parts)


def body(
    tokens,
    input_norm_gain,
    w_query,
    w_forget,
    w_input,
    w_gate,
    forget_floor,
    head_gain,
    w_out,
    state,
    prev_forget,
    prev_input,
    accepted,
):
    planes, group = lax.axis_size("zy"), lax.axis_size("tp")
    seqs, proposals, features = tokens.shape
    width, size = w_query.shape
    swap = [(0, 1), (1, 0)]
    hops = [[(i, (i + d) % group) for i in range(group)] for d in range(group)]

    def passed(parts):
        return [parts[0]] + [lax.ppermute(parts[d], "tp", hops[d]) for d in (1, 2, 3)]

    spread = source(tokens.transpose(1, 2, 0), input_norm_gain.reshape(-1, size), planes)
    own = lax.all_to_all(spread, "zy", 0, 0, tiled=True)
    keyed, mixing = turn(w_query, w_forget, w_input, w_gate)
    own, keyed = lax.optimization_barrier((own, keyed))
    other = lax.ppermute(own, "core", swap)
    weights = passed(mixing)

    past = (
        accepted,
        prev_forget,
        prev_input.reshape(seqs, proposals, -1).transpose(1, 2, 0),
        state[:, 0],
    )
    partial = passed(project(own, other, keyed, weights))
    earlier = advance(*past, 0, 4)
    partial[0], *earlier = lax.optimization_barrier((partial[0], *earlier))
    received = passed(finish(partial, 2 * size, width))
    new_state, rounded = advance(*past, 4, 4, earlier)
    shown = recur(received, rounded.reshape(-1, size), forget_floor[None], head_gain[None])
    parts = passed(shown)
    parts[0], w_out = lax.optimization_barrier((parts[0], w_out))
    outward = turn_outward(w_out)
    sent = outward_half(away_kernel, "away", parts, outward)
    came = lax.ppermute(sent, "core", swap)
    kept = outward_half(keep_kernel, "keep", parts, outward, came)
    terms = lax.all_to_all(kept, "zy", 0, 0, tiled=True)
    mixed = place(passed(sums(terms)))
    return mixed.transpose(2, 0, 1), new_state[:, None]


def solution(mesh):
    kv, tp = mesh.shape["kv"], mesh.shape["tp"]
    finer = Mesh(mesh.devices.reshape(kv // 2, 2, tp), ("zy", "core", "tp"))
    rows = ("zy", "core")
    placed = (
        P(None, None, (*rows, "tp")),
        P(),
        P(None, rows),
        P(None, rows),
        P(rows, "tp", None),
        P(rows, "tp", None),
        P(rows),
        P("tp"),
        P(rows, None),
        P(None, rows, "tp", None),
        P(None, None, rows),
        P(None, None, rows, "tp"),
        P(),
    )
    return jax.shard_map(
        body,
        mesh=finer,
        in_specs=placed,
        out_specs=(P(None, None, (*rows, "tp")), P(None, rows, "tp", None)),
        check_vma=False,
    )
```

```python
import functools

import jax
import jax.numpy as jnp
from jax import lax
from jax.experimental import pallas as pl
from jax.experimental.pallas import tpu as pltpu
from jax.sharding import Mesh, PartitionSpec as P


NORM_EPSILON = 1e-06


def whole():
    return pl.BlockSpec(memory_space=pltpu.VMEM)


def shaped(shape, dtype):
    return jax.ShapeDtypeStruct(shape, dtype)


def call(kernel, out_shape, scratch, cost, limit, in_specs, out_specs):
    return pl.pallas_call(
        kernel,
        out_shape=out_shape,
        in_specs=in_specs,
        out_specs=out_specs,
        scratch_shapes=scratch,
        cost_estimate=pl.CostEstimate(flops=cost[0], bytes_accessed=cost[1], transcendentals=0),
        compiler_params=pltpu.CompilerParams(vmem_limit_bytes=limit),
    )


def advance_kernel(accepted, prev_forget, prev_input, state, new_state, rounded, live):
    block = pl.program_id(0)
    count, proposals, size = prev_forget.shape
    lanes = prev_input.shape[2]

    @pl.when(block == 0)
    def _():
        live[...] = jnp.broadcast_to(accepted[...].astype(jnp.float32), (size, lanes)).T

    shift = lax.rem(lanes - block * count, lanes)
    values = [
        pltpu.roll(prev_input[p].astype(jnp.float32), shift, 1) for p in range(proposals)
    ]
    taken = live[pl.ds(pl.multiple_of(block * count, count), count), :]
    rest = jnp.ones((count, size), jnp.float32)
    terms = [None] * proposals
    for p in reversed(range(proposals)):
        gate = jnp.where(taken > p, prev_forget[:, p, :], 1.0)
        terms[p] = rest * (1.0 - gate)
        rest = rest * gate
    for s in range(count):
        fresh = rest[s : s + 1] * state[s]
        for p in range(proposals):
            fresh = fresh + terms[p][s : s + 1] * values[p][:, s : s + 1]
        new_state[s] = fresh
        rounded[s] = fresh.astype(jnp.bfloat16)


def advance(accepted, prev_forget, prev_input, state):
    seqs, values, keys = state.shape
    proposals = prev_forget.shape[1]
    count = 32
    span = pl.BlockSpec((count, values, keys), lambda i: (i, 0, 0))
    return pl.pallas_call(
        advance_kernel,
        grid=(seqs // count,),
        in_specs=[
            pl.BlockSpec((1, seqs), lambda i: (0, 0)),
            pl.BlockSpec((count, proposals, keys), lambda i: (i, 0, 0)),
            pl.BlockSpec((proposals, values, seqs), lambda i: (0, 0, 0)),
            span,
        ],
        out_specs=[span, span],
        out_shape=[shaped(state.shape, jnp.float32), shaped(state.shape, jnp.bfloat16)],
        scratch_shapes=[pltpu.VMEM((keys, seqs), jnp.float32)],
        name="advance",
        cost_estimate=pl.CostEstimate(
            flops=1_000_000_000, bytes_accessed=5 << 20, transcendentals=0
        ),
        compiler_params=pltpu.CompilerParams(vmem_limit_bytes=60 << 20),
    )(accepted[None], prev_forget, prev_input, state)


def split_in_three(value):
    high = value.astype(jnp.bfloat16).astype(jnp.float32)
    middle = (value - high).astype(jnp.bfloat16).astype(jnp.float32)
    return high, middle, value - high - middle


def three_rows(parts, width):
    rest = jnp.zeros((16 - 3 * parts[0].shape[0], width), jnp.float32)
    return jnp.concatenate([*parts, rest], axis=0).astype(jnp.bfloat16)


def source_kernel(tokens, gain, out, columns):
    steps, features, seqs = tokens.shape
    size = gain.shape[1]
    row = 2 * lax.axis_index("zy") + lax.axis_index("core")
    columns[...] = jnp.broadcast_to(gain[pl.ds(row, 1), :], (size, size)).T
    at = pl.multiple_of(lax.axis_index("tp") * features, features)
    scale = columns[pl.ds(at, features), :]
    squares = []
    for t in range(steps):
        wide = tokens[t].astype(jnp.float32)
        squares.append(jnp.sum(wide * wide, axis=0, keepdims=True))
        scaled = (wide * scale).astype(jnp.bfloat16)
        for z in range(out.shape[0]):
            out[z, pl.ds(t * features, features), :] = scaled
    tail = three_rows(split_in_three(jnp.concatenate(squares, axis=0)), seqs)
    for z in range(out.shape[0]):
        out[z, pl.ds(steps * features, 16), :] = tail


def source(tokens, gain, planes):
    steps, features, seqs = tokens.shape
    size = gain.shape[1]
    return call(
        source_kernel,
        shaped((planes, steps * features + 16, seqs), jnp.bfloat16),
        [pltpu.VMEM((size, seqs), jnp.float32)],
        (1_000_000, 1 << 20),
        60 << 20,
        [whole()] * 2,
        whole(),
    )(tokens, gain)


def turn_kernel(w_query, w_forget, w_input, w_gate, keyed, m0, m1, m2, m3, rows, mixed, sems):
    mine = lax.axis_index("tp")
    group, part, size = 4, rows.shape[2], w_query.shape[2]
    at = pl.multiple_of(mine * part, part)
    copies = [
        pltpu.make_async_copy(w_input.at[0], mixed.at[0], sems.at[0]),
        pltpu.make_async_copy(w_gate.at[0], mixed.at[1], sems.at[1]),
        pltpu.make_async_copy(w_query.at[:, pl.ds(at, part), :], rows.at[0], sems.at[2]),
        pltpu.make_async_copy(w_forget.at[:, pl.ds(at, part), :], rows.at[1], sems.at[3]),
    ]
    for copy in copies:
        copy.start()
    copies[0].wait()
    copies[1].wait()
    lane = lax.broadcasted_iota(jnp.int32, (2 * part, size), 1) // part
    for q in range(rows.shape[1] // group):
        to = pl.ds(q * size, size)
        blocks = []
        for k in range(group):
            cut = pl.ds((q * group + k) * size, size)
            both = [mixed[i, :, cut].astype(jnp.float32) for i in range(2)]
            blocks.append(jnp.concatenate(both, axis=0))
        for d, out in enumerate((m0, m1, m2, m3)):
            theirs = (mine ^ d)
            total = None
            for k in range(group):
                turned = pltpu.roll(blocks[k], lax.rem(group + k - theirs, group) * part, 1)
                total = turned if total is None else jnp.where(lane == k, turned, total)
            out[:, to] = total.astype(jnp.bfloat16)
    copies[2].wait()
    copies[3].wait()
    for q in range(rows.shape[1] // group):
        for i in range(2):
            block = rows[i, pl.ds(q * group, group)].astype(jnp.float32).reshape(size, size)
            keyed[pl.ds(i * size, size), pl.ds(q * size, size)] = block.T.astype(jnp.bfloat16)


def turn(w_query, w_forget, w_input, w_gate):
    width, size = w_query.shape
    values = w_input.shape[1]
    far = pl.BlockSpec(memory_space=pltpu.HBM)
    outs = call(
        turn_kernel,
        [shaped((2 * size, width // 4), jnp.bfloat16)]
        + [shaped((2 * values, width // 4), jnp.bfloat16)] * 4,
        [
            pltpu.VMEM((2, width // size, size // 4, size), jnp.bfloat16),
            pltpu.VMEM((2, values, width), jnp.bfloat16),
            pltpu.SemaphoreType.DMA((4,)),
        ],
        (1_000_000_000, 2 << 20),
        16 << 20,
        [far] * 4,
        [whole()] * 5,
    )(
        w_query.reshape(width // size, size, size),
        w_forget.reshape(width // size, size, size),
        w_input,
        w_gate,
    )
    return outs[0], outs[1:]


def outward_kernel(w_out, outward, held, sems):
    cuts, size, span = held.shape
    copies = [
        pltpu.make_async_copy(w_out.at[:, pl.ds(c * span, span)], held.at[c], sems.at[c])
        for c in range(cuts)
    ]
    for copy in copies:
        copy.start()
    for c in range(cuts):
        copies[c].wait()
        for b in range(span // size):
            block = held[c, :, pl.ds(b * size, size)].astype(jnp.float32)
            outward[c * (span // size) + b] = block.T.astype(jnp.bfloat16)


def turn_outward(w_out):
    size, width = w_out.shape
    return call(
        outward_kernel,
        shaped((width // size, size, size), jnp.bfloat16),
        [pltpu.VMEM((4, size, width // 4), jnp.bfloat16), pltpu.SemaphoreType.DMA((4,))],
        (1_000_000_000, 2 << 20),
        16 << 20,
        [pl.BlockSpec(memory_space=pltpu.HBM)],
        whole(),
    )(w_out)


def project_kernel(own, other, keyed, w0, w1, w2, w3, o0, o1, o2, o3, held, ready):
    core, mine = lax.axis_index("core"), lax.axis_index("tp")
    blocks, _, seqs = own.shape
    group, keys = 4, keyed.shape[0]
    part = held.shape[0] // (2 * blocks)
    squares = jnp.zeros((16, seqs), jnp.float32)
    for half, ref in ((core, own), (1 - core, other)):
        for b in range(blocks):
            at = pl.multiple_of((2 * b + half) * part, part)
            for t in range(group):
                held[pl.ds(at, part), pl.ds(t * seqs, seqs)] = ref[b, pl.ds(t * part, part), :]
            squares = squares + ref[b, pl.ds(group * part, 16), :].astype(jnp.float32)
    totals = squares[0:4] + squares[4:8] + squares[8:12]
    rows = held[...]
    first = jnp.dot(keyed[...], rows, preferred_element_type=jnp.float32).astype(jnp.bfloat16)
    for t in range(group):
        ready[t, pl.ds(0, keys), :] = first[:, t * seqs : (t + 1) * seqs]
        tail = three_rows(split_in_three(totals[t : t + 1]), seqs)
        ready[t, pl.ds(ready.shape[1] - 16, 16), :] = tail
    for d, weight in enumerate((w0, w1, w2, w3)):
        more = weight.shape[0]
        at = pl.multiple_of(keys + (mine ^ d) * more, more)
        second = jnp.dot(weight[...], rows, preferred_element_type=jnp.float32).astype(jnp.bfloat16)
        for t in range(group):
            ready[t, pl.ds(at, more), :] = second[:, t * seqs : (t + 1) * seqs]
    for d, out in enumerate((o0, o1, o2, o3)):
        out[...] = ready[(mine ^ d)]


def project(own, other, keyed, weights):
    _, _, seqs = own.shape
    keys, width = keyed.shape
    rows = keys + 4 * weights[0].shape[0] + 16
    return call(
        project_kernel,
        [shaped((rows, seqs), jnp.bfloat16)] * 4,
        [pltpu.VMEM((width, 4 * seqs), jnp.bfloat16), pltpu.VMEM((4, rows, seqs), jnp.bfloat16)],
        (1_000_000_000, 3 << 20),
        16 << 20,
        [whole()] * 7,
        [whole()] * 4,
    )(own, other, keyed, *weights)


def finish_kernel(width, p0, p1, p2, p3, o0, o1, o2, o3, held):
    mine = lax.axis_index("tp")
    group = 4
    rows, keys = held.shape[0], o0.shape[0] * 4 // 5
    total = sum(ref[pl.ds(rows, 16), :].astype(jnp.float32) for ref in (p0, p1, p2, p3))
    factor = lax.rsqrt(jnp.sum(total, axis=0, keepdims=True) / width + NORM_EPSILON)
    value = sum(ref[pl.ds(0, rows), :].astype(jnp.float32) for ref in (p0, p1, p2, p3))
    held[...] = (value * factor).astype(jnp.bfloat16)
    more = (rows - keys) // group
    for d, out in enumerate((o0, o1, o2, o3)):
        at = pl.multiple_of(keys + (mine ^ d) * more, more)
        out[pl.ds(0, keys), :] = held[pl.ds(0, keys), :]
        out[pl.ds(keys, more), :] = held[pl.ds(at, more), :]


def finish(parts, keys, width):
    rows, seqs = parts[0].shape
    rows = rows - 16
    return call(
        functools.partial(finish_kernel, width),
        [shaped((keys + (rows - keys) // 4, seqs), jnp.bfloat16)] * 4,
        [pltpu.VMEM((rows, seqs), jnp.bfloat16)],
        (100_000_000, 1 << 20),
        16 << 20,
        [whole()] * 4,
        [whole()] * 4,
    )(*parts)


def recur_kernel(r0, r1, r2, r3, before, floor, head_gain, o0, o1, o2, o3, seen, ready):
    mine = lax.axis_index("tp")
    size = floor.shape[1]
    values = head_gain.shape[1]
    count = before.shape[0] // values
    steps = 4
    for d, ref in enumerate((r0, r1, r2, r3)):
        seen[mine ^ d] = ref[...]
    low = jnp.broadcast_to(floor[...], (count, size)).T
    scale = jnp.broadcast_to(head_gain[...], (count, values)).T
    forget, keys, fresh, sums, asked = [], [], [], [], []
    for t in range(steps):
        gate = low + (1.0 - low) * jax.nn.sigmoid(seen[t, pl.ds(size, size), :].astype(jnp.float32))
        forget.append(gate)
        keys.append(1.0 - gate)
        fresh.append(seen[t, pl.ds(2 * size, values), :].astype(jnp.float32))
    for t in range(steps):
        moved = seen[t, pl.ds(0, size), :].astype(jnp.float32)
        out = None
        for u in reversed(range(t + 1)):
            score = jnp.sum(moved * keys[u], axis=0, keepdims=True)
            term = score * fresh[u]
            out = term if out is None else out + term
            moved = moved * forget[u]
        sums.append(out)
        asked.append(moved.astype(jnp.bfloat16))
    lane = lax.broadcasted_iota(jnp.int32, (values, count), 1)
    asked = jnp.concatenate(asked, axis=1)
    group = 8
    for b in range(count // group):
        read = jnp.dot(
            before[pl.ds(b * group * values, group * values), :],
            asked,
            preferred_element_type=jnp.float32,
        )
        for s in range(group):
            hit = lane == b * group + s
            for t in range(steps):
                part = read[s * values : (s + 1) * values, t * count : (t + 1) * count]
                sums[t] = sums[t] + jnp.where(hit, part, 0.0)
    for t in range(steps):
        out = sums[t]
        square = jnp.sum(out * out, axis=0, keepdims=True)
        gate = seen[t, pl.ds(2 * size + values, values), :].astype(jnp.float32)
        shown = out * scale * (gate * jax.nn.sigmoid(gate))
        ready[t, pl.ds(0, values), :] = shown.astype(jnp.bfloat16)
        ready[t, pl.ds(values, 16), :] = three_rows(split_in_three(square), count)
    for d, ref in enumerate((o0, o1, o2, o3)):
        ref[...] = ready[mine ^ d]


def recur(received, before, floor, head_gain):
    rows, count = received[0].shape
    values = head_gain.shape[1]
    return call(
        recur_kernel,
        [shaped((values + 16, count), jnp.bfloat16)] * 4,
        [
            pltpu.VMEM((4, rows, count), jnp.bfloat16),
            pltpu.VMEM((4, values + 16, count), jnp.bfloat16),
        ],
        (1_000_000_000, 2 << 20),
        16 << 20,
        [whole()] * 7,
        [whole()] * 4,
    )(*received, before, floor, head_gain)


def gathered(parts, joined):
    mine = lax.axis_index("tp")
    values = joined.shape[0] // 4
    total = None
    for d, ref in enumerate(parts):
        at = pl.multiple_of((mine ^ d) * values, values)
        joined[pl.ds(at, values), :] = ref[pl.ds(0, values), :]
        square = jnp.sum(ref[pl.ds(values, 16), :].astype(jnp.float32), axis=0, keepdims=True)
        total = square if total is None else total + square
    return lax.rsqrt(total / joined.shape[0] + NORM_EPSILON)


def away_kernel(p0, p1, p2, p3, outward, sent, joined):
    core = lax.axis_index("core")
    factor = gathered((p0, p1, p2, p3), joined)
    for b in range(sent.shape[0]):
        part = jnp.dot(outward[2 * b + 1 - core], joined[...], preferred_element_type=jnp.float32)
        sent[b] = (part * factor).astype(jnp.bfloat16)


def keep_kernel(p0, p1, p2, p3, outward, came, kept, joined):
    core = lax.axis_index("core")
    factor = gathered((p0, p1, p2, p3), joined)
    for b in range(kept.shape[0]):
        part = jnp.dot(outward[2 * b + core], joined[...], preferred_element_type=jnp.float32)
        kept[b] = (part * factor + came[b].astype(jnp.float32)).astype(jnp.bfloat16)


def outward_half(kernel, parts, outward, *more):
    blocks, size, _ = outward.shape
    return call(
        kernel,
        shaped((blocks // 2, size, parts[0].shape[1]), jnp.bfloat16),
        [pltpu.VMEM((size, parts[0].shape[1]), jnp.bfloat16)],
        (100_000_000, 2 << 20),
        16 << 20,
        [whole()] * (5 + len(more)),
        whole(),
    )(*parts, outward, *more)


def sum_kernel(parts, out):
    total = parts[0].astype(jnp.float32)
    for b in range(1, parts.shape[0]):
        total = total + parts[b].astype(jnp.float32)
    out[...] = total.astype(out.dtype)


def sums(parts):
    return call(
        sum_kernel,
        shaped(parts.shape[1:], jnp.bfloat16),
        [],
        (1_000_000, 1 << 20),
        8 << 20,
        [whole()],
        whole(),
    )(parts)


def body(
    tokens,
    input_norm_gain,
    w_query,
    w_forget,
    w_input,
    w_gate,
    forget_floor,
    head_gain,
    w_out,
    state,
    prev_forget,
    prev_input,
    accepted,
):
    planes, group = lax.axis_size("zy"), lax.axis_size("tp")
    seqs, proposals, features = tokens.shape
    width, size = w_query.shape
    swap = [(0, 1), (1, 0)]
    hops = [[(i, i ^ d) for i in range(group)] for d in range(group)]

    def passed(parts):
        return [parts[0]] + [lax.ppermute(parts[d], "tp", hops[d]) for d in (1, 2, 3)]

    spread = source(tokens.transpose(1, 2, 0), input_norm_gain.reshape(-1, size), planes)
    own = lax.all_to_all(spread, "zy", 0, 0, tiled=True)
    other = lax.ppermute(own, "core", swap)
    keyed, mixing = turn(w_query, w_forget, w_input, w_gate)
    weights = passed(mixing)
    new_state, rounded = advance(
        accepted,
        prev_forget,
        prev_input.reshape(seqs, proposals, -1).transpose(1, 2, 0),
        state[:, 0],
    )

    partial = passed(project(own, other, keyed, weights))
    received = passed(finish(partial, 2 * size, width))
    shown = recur(received, rounded.reshape(-1, size), forget_floor[None], head_gain[None])
    parts = passed(shown)
    parts[0], w_out = lax.optimization_barrier((parts[0], w_out))
    outward = turn_outward(w_out)
    sent = outward_half(away_kernel, parts, outward)
    came = lax.ppermute(sent, "core", swap)
    kept = outward_half(keep_kernel, parts, outward, came)
    terms = lax.all_to_all(
        kept.reshape(planes * group, features, seqs), ("zy", "tp"), 0, 0, tiled=True
    )
    mixed = sums(terms.reshape(planes, group, features, seqs))
    return mixed.transpose(2, 0, 1), new_state[:, None]


def solution(mesh):
    kv, tp = mesh.shape["kv"], mesh.shape["tp"]
    finer = Mesh(mesh.devices.reshape(kv // 2, 2, tp), ("zy", "core", "tp"))
    rows = ("zy", "core")
    placed = (
        P(None, None, (*rows, "tp")),
        P(),
        P(None, rows),
        P(None, rows),
        P(rows, "tp", None),
        P(rows, "tp", None),
        P(rows),
        P("tp"),
        P(rows, None),
        P(None, rows, "tp", None),
        P(None, None, rows),
        P(None, None, rows, "tp"),
        P(),
    )

    return jax.shard_map(
        body,
        mesh=finer,
        in_specs=placed,
        out_specs=(P(None, None, (*rows, "tp")), P(None, rows, "tp", None)),
        check_vma=False,
    )
```

```python
import jax
import jax.numpy as jnp
from jax import lax
from jax.experimental import pallas as pl
from jax.experimental.pallas import tpu as pltpu
from jax.sharding import Mesh, PartitionSpec as P


NORM_EPSILON = 1e-06


def whole():
    return pl.BlockSpec(memory_space=pltpu.VMEM)


def shaped(shape, dtype):
    return jax.ShapeDtypeStruct(shape, dtype)


def call(kernel, out_shape, scratch, cost, limit, in_specs, out_specs):
    return pl.pallas_call(
        kernel,
        out_shape=out_shape,
        in_specs=in_specs,
        out_specs=out_specs,
        scratch_shapes=scratch,
        cost_estimate=pl.CostEstimate(flops=cost[0], bytes_accessed=cost[1], transcendentals=0),
        compiler_params=pltpu.CompilerParams(vmem_limit_bytes=limit),
    )


def advance_kernel(accepted, prev_forget, prev_input, state, new_state, rounded, live):
    block = pl.program_id(0)
    count, proposals, size = prev_forget.shape
    lanes = prev_input.shape[2]

    @pl.when(block == 0)
    def _():
        live[...] = jnp.broadcast_to(accepted[...].astype(jnp.float32), (size, lanes)).T

    shift = lax.rem(lanes - block * count, lanes)
    values = [
        pltpu.roll(prev_input[p].astype(jnp.float32), shift, 1) for p in range(proposals)
    ]
    taken = live[pl.ds(pl.multiple_of(block * count, count), count), :]
    rest = jnp.ones((count, size), jnp.float32)
    terms = [None] * proposals
    for p in reversed(range(proposals)):
        gate = jnp.where(taken > p, prev_forget[:, p, :], 1.0)
        terms[p] = rest * (1.0 - gate)
        rest = rest * gate
    for s in range(count):
        fresh = rest[s : s + 1] * state[s]
        for p in range(proposals):
            fresh = fresh + terms[p][s : s + 1] * values[p][:, s : s + 1]
        new_state[s] = fresh
        rounded[s] = fresh.astype(jnp.bfloat16)


def advance(accepted, prev_forget, prev_input, state):
    seqs, values, keys = state.shape
    proposals = prev_forget.shape[1]
    count = 32
    span = pl.BlockSpec((count, values, keys), lambda i: (i, 0, 0))
    return pl.pallas_call(
        advance_kernel,
        grid=(seqs // count,),
        in_specs=[
            pl.BlockSpec((1, seqs), lambda i: (0, 0)),
            pl.BlockSpec((count, proposals, keys), lambda i: (i, 0, 0)),
            pl.BlockSpec((proposals, values, seqs), lambda i: (0, 0, 0)),
            span,
        ],
        out_specs=[span, span],
        out_shape=[shaped(state.shape, jnp.float32), shaped(state.shape, jnp.bfloat16)],
        scratch_shapes=[pltpu.VMEM((keys, seqs), jnp.float32)],
        name="advance",
        cost_estimate=pl.CostEstimate(
            flops=1_000_000_000, bytes_accessed=5 << 20, transcendentals=0
        ),
        compiler_params=pltpu.CompilerParams(vmem_limit_bytes=16 << 20),
    )(accepted[None], prev_forget, prev_input, state)


def split_in_three(value):
    high = value.astype(jnp.bfloat16).astype(jnp.float32)
    middle = (value - high).astype(jnp.bfloat16).astype(jnp.float32)
    return high, middle, value - high - middle


def three_rows(parts, width):
    rest = jnp.zeros((16 - 3 * parts[0].shape[0], width), jnp.float32)
    return jnp.concatenate([*parts, rest], axis=0).astype(jnp.bfloat16)


def source_kernel(tokens, out):
    steps = tokens.shape[0]
    for z in range(out.shape[0] // steps):
        out[pl.ds(z * steps, steps)] = tokens[...]


def source(tokens, planes):
    steps, features, seqs = tokens.shape
    return call(
        source_kernel,
        shaped((planes * steps, features, seqs), jnp.bfloat16),
        [],
        (1_000_000, 1 << 20),
        60 << 20,
        [whole()],
        whole(),
    )(tokens)


def turn_kernel(gain, w_query, w_forget, keyed):
    size = gain.shape[1]
    for b in range(w_query.shape[0] // size):
        at = pl.ds(b * size, size)
        row = gain[pl.ds(b, 1), :]
        for i, weight in enumerate((w_query, w_forget)):
            block = weight[at, :].astype(jnp.float32).T
            keyed[pl.ds(i * size, size), at] = (block * row).astype(jnp.bfloat16)


def turn(gain, w_query, w_forget):
    width, size = w_query.shape
    return call(
        turn_kernel,
        shaped((2 * size, width), jnp.bfloat16),
        [],
        (1_000_000_000, 4 << 20),
        16 << 20,
        [whole()] * 3,
        whole(),
    )(gain, w_query, w_forget)


def fold_kernel(gain, w0, w1, w2, w3, out):
    values, size = w0.shape[1], gain.shape[1]
    for b in range(gain.shape[0]):
        at = pl.ds(b * size, size)
        for d, weight in enumerate((w0, w1, w2, w3)):
            value = weight[0, :, at].astype(jnp.float32) * gain[pl.ds(b, 1), :]
            out[pl.ds(d * values, values), at] = value.astype(jnp.bfloat16)


def fold(gain, weights):
    _, values, width = weights[0].shape
    return call(
        fold_kernel,
        shaped((4 * values, width), jnp.bfloat16),
        [],
        (1_000_000_000, 2 << 20),
        16 << 20,
        [whole()] * 5,
        whole(),
    )(gain, *weights)


def project_kernel(own, other, keyed, mixing, o0, o1, o2, o3, held, scale):
    core = lax.axis_index("core")
    blocks, size, seqs = own.shape
    squares = jnp.zeros((8, seqs), jnp.float32)
    for half, ref in ((core, own), (1 - core, other)):
        for b in range(blocks):
            part = ref[b]
            held[pl.ds(pl.multiple_of((2 * b + half) * size, size), size), :] = part
            wide = part.astype(jnp.float32)
            squares = squares + jnp.sum((wide * wide).reshape(size // 8, 8, seqs), axis=0)
    total = jnp.sum(squares, axis=0, keepdims=True)
    factor = lax.rsqrt(total / (2 * blocks * size) + NORM_EPSILON)
    scale[...] = jnp.broadcast_to(factor, scale.shape)
    rows = held[...]
    first = jnp.dot(keyed[...], rows, preferred_element_type=jnp.float32) * factor
    first = first.astype(jnp.bfloat16)
    second = jnp.dot(mixing[...], rows, preferred_element_type=jnp.float32) * factor
    second = second.astype(jnp.bfloat16)
    keys, values = first.shape[0], second.shape[0] // 4
    for d, out in enumerate((o0, o1, o2, o3)):
        out[pl.ds(0, keys), :] = first
        out[pl.ds(keys, values), :] = second[d * values : (d + 1) * values]


def project(own, other, keyed, mixing):
    blocks, size, seqs = own.shape
    rows = keyed.shape[0] + mixing.shape[0] // 4
    outs = call(
        project_kernel,
        [shaped((rows, seqs), jnp.bfloat16)] * 4
        + [shaped((2 * blocks * size, seqs), jnp.bfloat16), shaped((8, seqs), jnp.float32)],
        [],
        (1_000_000_000, 3 << 20),
        16 << 20,
        [whole()] * 4,
        [whole()] * 6,
    )(own, other, keyed, mixing)
    return outs[:4], outs[4], outs[5]


def gate_kernel(gain, w0, w1, w2, w3, rows, scale, out, held):
    values, size = w0.shape[1], gain.shape[1]
    for b in range(gain.shape[0]):
        at = pl.ds(b * size, size)
        for d, weight in enumerate((w0, w1, w2, w3)):
            value = weight[0, :, at].astype(jnp.float32) * gain[pl.ds(b, 1), :]
            held[pl.ds(d * values, values), at] = value.astype(jnp.bfloat16)
    raw = jnp.dot(held[...], rows[...], preferred_element_type=jnp.float32) * scale[0:1]
    raw = raw.astype(jnp.bfloat16).astype(jnp.float32)
    out[...] = raw * jax.nn.sigmoid(raw)


def gate(gain, weights, rows, scale):
    _, values, width = weights[0].shape
    return call(
        gate_kernel,
        shaped((4 * values, rows.shape[1]), jnp.float32),
        [pltpu.VMEM((4 * values, width), jnp.bfloat16)],
        (1_000_000_000, 3 << 20),
        16 << 20,
        [whole()] * 7,
        whole(),
    )(gain, *weights, rows, scale)


def outward_kernel(w_out, outward, held, sems):
    cuts, size, span = held.shape
    copies = [
        pltpu.make_async_copy(w_out.at[:, pl.ds(c * span, span)], held.at[c], sems.at[c])
        for c in range(cuts)
    ]
    for copy in copies:
        copy.start()
    for c in range(cuts):
        copies[c].wait()
        for b in range(span // size):
            block = held[c, :, pl.ds(b * size, size)].astype(jnp.float32)
            outward[c * (span // size) + b] = block.T.astype(jnp.bfloat16)


def turn_outward(w_out):
    size, width = w_out.shape
    return call(
        outward_kernel,
        shaped((width // size, size, size), jnp.bfloat16),
        [pltpu.VMEM((4, size, width // 4), jnp.bfloat16), pltpu.SemaphoreType.DMA((4,))],
        (1_000_000_000, 2 << 20),
        16 << 20,
        [pl.BlockSpec(memory_space=pltpu.HBM)],
        whole(),
    )(w_out)


def recur_kernel(r0, r1, r2, r3, before, floor, head_gain, o0, o1, o2, o3, seen, ready):
    mine = lax.axis_index("tp")
    size = floor.shape[1]
    values = head_gain.shape[1]
    count = before.shape[0] // values
    steps = 4
    for d, ref in enumerate((r0, r1, r2, r3)):
        seen[mine ^ d] = ref[...]
    low = jnp.broadcast_to(floor[...], (count, size)).T
    scale = jnp.broadcast_to(head_gain[...], (count, values)).T
    forget, keys, fresh, sums, asked = [], [], [], [], []
    for t in range(steps):
        gate = low + (1.0 - low) * jax.nn.sigmoid(seen[t, pl.ds(size, size), :].astype(jnp.float32))
        forget.append(gate)
        keys.append(1.0 - gate)
        fresh.append(seen[t, pl.ds(2 * size, values), :].astype(jnp.float32))
    for t in range(steps):
        moved = seen[t, pl.ds(0, size), :].astype(jnp.float32)
        out = None
        for u in reversed(range(t + 1)):
            score = jnp.sum(moved * keys[u], axis=0, keepdims=True)
            term = score * fresh[u]
            out = term if out is None else out + term
            moved = moved * forget[u]
        sums.append(out)
        asked.append(moved.astype(jnp.bfloat16))
    lane = lax.broadcasted_iota(jnp.int32, (values, count), 1)
    asked = jnp.concatenate(asked, axis=1)
    group = 8
    for b in range(count // group):
        read = jnp.dot(
            before[pl.ds(b * group * values, group * values), :],
            asked,
            preferred_element_type=jnp.float32,
        )
        for s in range(group):
            hit = lane == b * group + s
            for t in range(steps):
                part = read[s * values : (s + 1) * values, t * count : (t + 1) * count]
                sums[t] = sums[t] + jnp.where(hit, part, 0.0)
    for t in range(steps):
        out = sums[t]
        square = jnp.sum(out * out, axis=0, keepdims=True)
        ready[t, pl.ds(0, values), :] = (out * scale).astype(jnp.bfloat16)
        ready[t, pl.ds(values, 16), :] = three_rows(split_in_three(square), count)
    for d, ref in enumerate((o0, o1, o2, o3)):
        ref[...] = ready[mine ^ d]


def recur(received, before, floor, head_gain):
    rows, count = received[0].shape
    values = head_gain.shape[1]
    return call(
        recur_kernel,
        [shaped((values + 16, count), jnp.bfloat16)] * 4,
        [
            pltpu.VMEM((4, rows, count), jnp.bfloat16),
            pltpu.VMEM((4, values + 16, count), jnp.bfloat16),
        ],
        (1_000_000_000, 2 << 20),
        16 << 20,
        [whole()] * 7,
        [whole()] * 4,
    )(*received, before, floor, head_gain)


def gathered(parts, gates, joined):
    mine = lax.axis_index("tp")
    values = joined.shape[0] // 4
    total = None
    for d, ref in enumerate(parts):
        at = pl.multiple_of((mine ^ d) * values, values)
        value = ref[pl.ds(0, values), :].astype(jnp.float32) * gates[pl.ds(d * values, values), :]
        joined[pl.ds(at, values), :] = value.astype(jnp.bfloat16)
        square = jnp.sum(ref[pl.ds(values, 16), :].astype(jnp.float32), axis=0, keepdims=True)
        total = square if total is None else total + square
    return lax.rsqrt(total / joined.shape[0] + NORM_EPSILON)


def away_kernel(p0, p1, p2, p3, gates, outward, sent, joined):
    core = lax.axis_index("core")
    factor = gathered((p0, p1, p2, p3), gates, joined)
    for b in range(sent.shape[0]):
        part = jnp.dot(outward[2 * b + 1 - core], joined[...], preferred_element_type=jnp.float32)
        sent[b] = (part * factor).astype(jnp.bfloat16)


def keep_kernel(p0, p1, p2, p3, gates, outward, came, kept, joined):
    core = lax.axis_index("core")
    factor = gathered((p0, p1, p2, p3), gates, joined)
    for b in range(kept.shape[0]):
        part = jnp.dot(outward[2 * b + core], joined[...], preferred_element_type=jnp.float32)
        kept[b] = (part * factor + came[b].astype(jnp.float32)).astype(jnp.bfloat16)


def outward_half(kernel, parts, gates, outward, *more):
    blocks, size, _ = outward.shape
    return call(
        kernel,
        shaped((blocks // 2, size, parts[0].shape[1]), jnp.bfloat16),
        [pltpu.VMEM((size, parts[0].shape[1]), jnp.bfloat16)],
        (100_000_000, 2 << 20),
        16 << 20,
        [whole()] * (6 + len(more)),
        whole(),
    )(*parts, gates, outward, *more)


def sum_kernel(parts, out):
    total = parts[0].astype(jnp.float32)
    for b in range(1, parts.shape[0]):
        total = total + parts[b].astype(jnp.float32)
    out[...] = total.astype(out.dtype)


def sums(parts):
    return call(
        sum_kernel,
        shaped(parts.shape[1:], jnp.bfloat16),
        [],
        (1_000_000, 1 << 20),
        8 << 20,
        [whole()],
        whole(),
    )(parts)


def body(
    tokens,
    input_norm_gain,
    w_query,
    w_forget,
    w_input,
    w_gate,
    forget_floor,
    head_gain,
    w_out,
    state,
    prev_forget,
    prev_input,
    accepted,
):
    planes, group = lax.axis_size("zy"), lax.axis_size("tp")
    seqs, proposals, features = tokens.shape
    _, size = w_query.shape
    swap = [(0, 1), (1, 0)]
    hops = [[(i, i ^ d) for i in range(group)] for d in range(group)]

    def passed(parts):
        return [parts[0]] + [lax.ppermute(parts[d], "tp", hops[d]) for d in (1, 2, 3)]

    gain = input_norm_gain.reshape(-1, size)
    inputs = passed([w_input] * group)
    own = lax.all_to_all(source(tokens.transpose(1, 2, 0), planes), ("zy", "tp"), 0, 0, tiled=True)
    own = own.reshape(planes, group * features, seqs)
    other = lax.ppermute(own, "core", swap)
    gates = passed([w_gate] * group)
    keyed = turn(gain, w_query, w_forget)
    mixing = fold(gain, inputs)
    new_state, rounded = advance(
        accepted,
        prev_forget,
        prev_input.reshape(seqs, proposals, -1).transpose(1, 2, 0),
        state[:, 0],
    )

    sends, rows, scale = project(own, other, keyed, mixing)
    received = passed(sends)
    shown = recur(received, rounded.reshape(-1, size), forget_floor[None], head_gain[None])
    parts = passed(shown)
    outward = turn_outward(w_out)
    opened = gate(gain, gates, rows, scale)
    sent = outward_half(away_kernel, parts, opened, outward)
    came = lax.ppermute(sent, "core", swap)
    kept = outward_half(keep_kernel, parts, opened, outward, came)
    terms = lax.all_to_all(
        kept.reshape(planes * group, features, seqs), ("zy", "tp"), 0, 0, tiled=True
    )
    mixed = sums(terms.reshape(planes, group, features, seqs))
    return mixed.transpose(2, 0, 1), new_state[:, None]


def solution(mesh):
    kv, tp = mesh.shape["kv"], mesh.shape["tp"]
    finer = Mesh(mesh.devices.reshape(kv // 2, 2, tp), ("zy", "core", "tp"))
    rows = ("zy", "core")
    placed = (
        P(None, None, (*rows, "tp")),
        P(),
        P(None, rows),
        P(None, rows),
        P(rows, "tp", None),
        P(rows, "tp", None),
        P(rows),
        P("tp"),
        P(rows, None),
        P(None, rows, "tp", None),
        P(None, None, rows),
        P(None, None, rows, "tp"),
        P(),
    )

    return jax.shard_map(
        body,
        mesh=finer,
        in_specs=placed,
        out_specs=(P(None, None, (*rows, "tp")), P(None, rows, "tp", None)),
        check_vma=False,
    )
```

```python
import jax
import jax.numpy as jnp
from jax import lax
from jax.experimental import pallas as pl
from jax.experimental.pallas import tpu as pltpu
from jax.sharding import Mesh, PartitionSpec as P


NORM_EPSILON = 1e-06


def whole():
    return pl.BlockSpec(memory_space=pltpu.VMEM)


def shaped(shape, dtype):
    return jax.ShapeDtypeStruct(shape, dtype)


def call(kernel, out_shape, scratch, cost, limit, in_specs, out_specs):
    return pl.pallas_call(
        kernel,
        out_shape=out_shape,
        in_specs=in_specs,
        out_specs=out_specs,
        scratch_shapes=scratch,
        cost_estimate=pl.CostEstimate(flops=cost[0], bytes_accessed=cost[1], transcendentals=0),
        compiler_params=pltpu.CompilerParams(vmem_limit_bytes=limit),
    )


def advance_kernel(accepted, prev_forget, prev_input, state, new_state, rounded, live):
    block = pl.program_id(0)
    count, proposals, size = prev_forget.shape
    lanes = prev_input.shape[2]

    @pl.when(block == 0)
    def _():
        live[...] = jnp.broadcast_to(accepted[...].astype(jnp.float32), (size, lanes)).T

    shift = lax.rem(lanes - block * count, lanes)
    values = [
        pltpu.roll(prev_input[p].astype(jnp.float32), shift, 1) for p in range(proposals)
    ]
    taken = live[pl.ds(pl.multiple_of(block * count, count), count), :]
    rest = jnp.ones((count, size), jnp.float32)
    terms = [None] * proposals
    for p in reversed(range(proposals)):
        gate = jnp.where(taken > p, prev_forget[:, p, :], 1.0)
        terms[p] = rest * (1.0 - gate)
        rest = rest * gate
    for s in range(count):
        fresh = rest[s : s + 1] * state[s]
        for p in range(proposals):
            fresh = fresh + terms[p][s : s + 1] * values[p][:, s : s + 1]
        new_state[s] = fresh
        rounded[s] = fresh.astype(jnp.bfloat16)


def advance(accepted, prev_forget, prev_input, state):
    seqs, values, keys = state.shape
    proposals = prev_forget.shape[1]
    count = 32
    span = pl.BlockSpec((count, values, keys), lambda i: (i, 0, 0))
    return pl.pallas_call(
        advance_kernel,
        grid=(seqs // count,),
        in_specs=[
            pl.BlockSpec((1, seqs), lambda i: (0, 0)),
            pl.BlockSpec((count, proposals, keys), lambda i: (i, 0, 0)),
            pl.BlockSpec((proposals, values, seqs), lambda i: (0, 0, 0)),
            span,
        ],
        out_specs=[span, span],
        out_shape=[shaped(state.shape, jnp.float32), shaped(state.shape, jnp.bfloat16)],
        scratch_shapes=[pltpu.VMEM((keys, seqs), jnp.float32)],
        name="advance",
        cost_estimate=pl.CostEstimate(
            flops=1_000_000_000, bytes_accessed=5 << 20, transcendentals=0
        ),
        compiler_params=pltpu.CompilerParams(vmem_limit_bytes=16 << 20),
    )(accepted[None], prev_forget, prev_input, state)


def split_in_three(value):
    high = value.astype(jnp.bfloat16).astype(jnp.float32)
    middle = (value - high).astype(jnp.bfloat16).astype(jnp.float32)
    return high, middle, value - high - middle


def three_rows(parts, width):
    rest = jnp.zeros((16 - 3 * parts[0].shape[0], width), jnp.float32)
    return jnp.concatenate([*parts, rest], axis=0).astype(jnp.bfloat16)


def source_kernel(tokens, out):
    steps = tokens.shape[0]
    for z in range(out.shape[0] // steps):
        out[pl.ds(z * steps, steps)] = tokens[...]


def source(tokens, planes):
    steps, features, seqs = tokens.shape
    return call(
        source_kernel,
        shaped((planes * steps, features, seqs), jnp.bfloat16),
        [],
        (1_000_000, 1 << 20),
        60 << 20,
        [whole()],
        whole(),
    )(tokens)


def join_kernel(w_query, w_forget, joined):
    size = w_query.shape[1]
    joined[:, pl.ds(0, size)] = w_query[...]
    joined[:, pl.ds(size, size)] = w_forget[...]


def join(w_query, w_forget):
    width, size = w_query.shape
    return call(
        join_kernel,
        shaped((width, 2 * size), jnp.bfloat16),
        [],
        (1_000_000_000, 4 << 20),
        16 << 20,
        [whole()] * 2,
        whole(),
    )(w_query, w_forget)


def across(left, right):
    return lax.dot_general(
        left, right, (((1,), (1,)), ((), ())), preferred_element_type=jnp.float32
    )


def project_kernel(own, other, gain, joined, w0, w1, w2, w3, o0, o1, o2, o3, rows, scale):
    core = lax.axis_index("core")
    blocks, size, seqs = own.shape
    squares = jnp.zeros((8, seqs), jnp.float32)
    for half, ref in ((core, own), (1 - core, other)):
        for b in range(blocks):
            wide = ref[b].astype(jnp.float32)
            squares = squares + jnp.sum((wide * wide).reshape(size // 8, 8, seqs), axis=0)
            row = 2 * b + half
            at = pl.ds(pl.multiple_of(row * size, size), size)
            rows[:, at] = (wide.T * gain[pl.ds(row, 1), :]).astype(jnp.bfloat16)
    total = jnp.sum(squares, axis=0, keepdims=True)
    factor = lax.rsqrt(total / (2 * blocks * size) + NORM_EPSILON)
    scale[...] = jnp.broadcast_to(factor, scale.shape)
    first = jnp.dot(rows[...], joined[...], preferred_element_type=jnp.float32)
    keys, values = first.shape[1], w0.shape[1]
    for i in range(keys // size):
        part = (first[:, i * size : (i + 1) * size].T * factor).astype(jnp.bfloat16)
        for out in (o0, o1, o2, o3):
            out[pl.ds(i * size, size), :] = part
    for weight, out in ((w0, o0), (w1, o1), (w2, o2), (w3, o3)):
        second = across(weight[0], rows[...]) * factor
        out[pl.ds(keys, values), :] = second.astype(jnp.bfloat16)


def project(own, other, gain, joined, weights):
    blocks, size, seqs = own.shape
    height = joined.shape[1] + weights[0].shape[1]
    outs = call(
        project_kernel,
        [shaped((height, seqs), jnp.bfloat16)] * 4
        + [shaped((seqs, 2 * blocks * size), jnp.bfloat16), shaped((8, seqs), jnp.float32)],
        [],
        (1_000_000_000, 3 << 20),
        16 << 20,
        [whole()] * 8,
        [whole()] * 6,
    )(own, other, gain, joined, *weights)
    return outs[:4], outs[4], outs[5]


def gate_kernel(w0, w1, w2, w3, rows, scale, out):
    values = w0.shape[1]
    for d, weight in enumerate((w0, w1, w2, w3)):
        raw = across(weight[0], rows[...]) * scale[0:1]
        raw = raw.astype(jnp.bfloat16).astype(jnp.float32)
        out[pl.ds(d * values, values), :] = raw * jax.nn.sigmoid(raw)


def gate(weights, rows, scale):
    values = weights[0].shape[1]
    return call(
        gate_kernel,
        shaped((4 * values, rows.shape[0]), jnp.float32),
        [],
        (1_000_000_000, 3 << 20),
        16 << 20,
        [whole()] * 6,
        whole(),
    )(*weights, rows, scale)


def outward_kernel(w_out, outward, held, sems):
    cuts, size, span = held.shape
    copies = [
        pltpu.make_async_copy(w_out.at[:, pl.ds(c * span, span)], held.at[c], sems.at[c])
        for c in range(cuts)
    ]
    for copy in copies:
        copy.start()
    for c in range(cuts):
        copies[c].wait()
        for b in range(span // size):
            block = held[c, :, pl.ds(b * size, size)].astype(jnp.float32)
            outward[c * (span // size) + b] = block.T.astype(jnp.bfloat16)


def turn_outward(w_out):
    size, width = w_out.shape
    return call(
        outward_kernel,
        shaped((width // size, size, size), jnp.bfloat16),
        [pltpu.VMEM((4, size, width // 4), jnp.bfloat16), pltpu.SemaphoreType.DMA((4,))],
        (1_000_000_000, 2 << 20),
        16 << 20,
        [pl.BlockSpec(memory_space=pltpu.HBM)],
        whole(),
    )(w_out)


def recur_kernel(r0, r1, r2, r3, before, floor, head_gain, o0, o1, o2, o3, seen, ready):
    mine = lax.axis_index("tp")
    size = floor.shape[1]
    values = head_gain.shape[1]
    count = before.shape[0] // values
    steps = 4
    for d, ref in enumerate((r0, r1, r2, r3)):
        seen[mine ^ d] = ref[...]
    low = jnp.broadcast_to(floor[...], (count, size)).T
    scale = jnp.broadcast_to(head_gain[...], (count, values)).T
    forget, keys, fresh, sums, asked = [], [], [], [], []
    for t in range(steps):
        gate = low + (1.0 - low) * jax.nn.sigmoid(seen[t, pl.ds(size, size), :].astype(jnp.float32))
        forget.append(gate)
        keys.append(1.0 - gate)
        fresh.append(seen[t, pl.ds(2 * size, values), :].astype(jnp.float32))
    for t in range(steps):
        moved = seen[t, pl.ds(0, size), :].astype(jnp.float32)
        out = None
        for u in reversed(range(t + 1)):
            score = jnp.sum(moved * keys[u], axis=0, keepdims=True)
            term = score * fresh[u]
            out = term if out is None else out + term
            moved = moved * forget[u]
        sums.append(out)
        asked.append(moved.astype(jnp.bfloat16))
    lane = lax.broadcasted_iota(jnp.int32, (values, count), 1)
    asked = jnp.concatenate(asked, axis=1)
    group = 8
    for b in range(count // group):
        read = jnp.dot(
            before[pl.ds(b * group * values, group * values), :],
            asked,
            preferred_element_type=jnp.float32,
        )
        for s in range(group):
            hit = lane == b * group + s
            for t in range(steps):
                part = read[s * values : (s + 1) * values, t * count : (t + 1) * count]
                sums[t] = sums[t] + jnp.where(hit, part, 0.0)
    for t in range(steps):
        out = sums[t]
        square = jnp.sum(out * out, axis=0, keepdims=True)
        ready[t, pl.ds(0, values), :] = (out * scale).astype(jnp.bfloat16)
        ready[t, pl.ds(values, 16), :] = three_rows(split_in_three(square), count)
    for d, ref in enumerate((o0, o1, o2, o3)):
        ref[...] = ready[mine ^ d]


def recur(received, before, floor, head_gain):
    rows, count = received[0].shape
    values = head_gain.shape[1]
    return call(
        recur_kernel,
        [shaped((values + 16, count), jnp.bfloat16)] * 4,
        [
            pltpu.VMEM((4, rows, count), jnp.bfloat16),
            pltpu.VMEM((4, values + 16, count), jnp.bfloat16),
        ],
        (1_000_000_000, 2 << 20),
        16 << 20,
        [whole()] * 7,
        [whole()] * 4,
    )(*received, before, floor, head_gain)


def gathered(parts, gates, joined):
    mine = lax.axis_index("tp")
    values = joined.shape[0] // 4
    total = None
    for d, ref in enumerate(parts):
        at = pl.multiple_of((mine ^ d) * values, values)
        value = ref[pl.ds(0, values), :].astype(jnp.float32) * gates[pl.ds(d * values, values), :]
        joined[pl.ds(at, values), :] = value.astype(jnp.bfloat16)
        square = jnp.sum(ref[pl.ds(values, 16), :].astype(jnp.float32), axis=0, keepdims=True)
        total = square if total is None else total + square
    return lax.rsqrt(total / joined.shape[0] + NORM_EPSILON)


def away_kernel(p0, p1, p2, p3, gates, outward, sent, joined):
    core = lax.axis_index("core")
    factor = gathered((p0, p1, p2, p3), gates, joined)
    for b in range(sent.shape[0]):
        part = jnp.dot(outward[2 * b + 1 - core], joined[...], preferred_element_type=jnp.float32)
        sent[b] = (part * factor).astype(jnp.bfloat16)


def keep_kernel(p0, p1, p2, p3, gates, outward, came, kept, joined):
    core = lax.axis_index("core")
    factor = gathered((p0, p1, p2, p3), gates, joined)
    for b in range(kept.shape[0]):
        part = jnp.dot(outward[2 * b + core], joined[...], preferred_element_type=jnp.float32)
        kept[b] = (part * factor + came[b].astype(jnp.float32)).astype(jnp.bfloat16)


def outward_half(kernel, parts, gates, outward, *more):
    blocks, size, _ = outward.shape
    return call(
        kernel,
        shaped((blocks // 2, size, parts[0].shape[1]), jnp.bfloat16),
        [pltpu.VMEM((size, parts[0].shape[1]), jnp.bfloat16)],
        (100_000_000, 2 << 20),
        16 << 20,
        [whole()] * (6 + len(more)),
        whole(),
    )(*parts, gates, outward, *more)


def sum_kernel(parts, out):
    total = parts[0].astype(jnp.float32)
    for b in range(1, parts.shape[0]):
        total = total + parts[b].astype(jnp.float32)
    out[...] = total.astype(out.dtype)


def sums(parts):
    return call(
        sum_kernel,
        shaped(parts.shape[1:], jnp.bfloat16),
        [],
        (1_000_000, 1 << 20),
        8 << 20,
        [whole()],
        whole(),
    )(parts)


def body(
    tokens,
    input_norm_gain,
    w_query,
    w_forget,
    w_input,
    w_gate,
    forget_floor,
    head_gain,
    w_out,
    state,
    prev_forget,
    prev_input,
    accepted,
):
    planes, group = lax.axis_size("zy"), lax.axis_size("tp")
    seqs, proposals, features = tokens.shape
    _, size = w_query.shape
    swap = [(0, 1), (1, 0)]
    hops = [[(i, i ^ d) for i in range(group)] for d in range(group)]

    def passed(parts):
        return [parts[0]] + [lax.ppermute(parts[d], "tp", hops[d]) for d in (1, 2, 3)]

    gain = input_norm_gain.reshape(-1, size)
    own = lax.all_to_all(source(tokens.transpose(1, 2, 0), planes), ("zy", "tp"), 0, 0, tiled=True)
    own = own.reshape(planes, group * features, seqs)
    other = lax.ppermute(own, "core", swap)
    inputs = passed([w_input] * group)
    gates = passed([w_gate] * group)
    joined = join(w_query, w_forget)
    new_state, rounded = advance(
        accepted,
        prev_forget,
        prev_input.reshape(seqs, proposals, -1).transpose(1, 2, 0),
        state[:, 0],
    )

    sends, rows, scale = project(own, other, gain, joined, inputs)
    received = passed(sends)
    shown = recur(received, rounded.reshape(-1, size), forget_floor[None], head_gain[None])
    parts = passed(shown)
    outward = turn_outward(w_out)
    opened = gate(gates, rows, scale)
    sent = outward_half(away_kernel, parts, opened, outward)
    came = lax.ppermute(sent, "core", swap)
    kept = outward_half(keep_kernel, parts, opened, outward, came)
    terms = lax.all_to_all(
        kept.reshape(planes * group, features, seqs), ("zy", "tp"), 0, 0, tiled=True
    )
    mixed = sums(terms.reshape(planes, group, features, seqs))
    return mixed.transpose(2, 0, 1), new_state[:, None]


def solution(mesh):
    kv, tp = mesh.shape["kv"], mesh.shape["tp"]
    finer = Mesh(mesh.devices.reshape(kv // 2, 2, tp), ("zy", "core", "tp"))
    rows = ("zy", "core")
    placed = (
        P(None, None, (*rows, "tp")),
        P(),
        P(None, rows),
        P(None, rows),
        P(rows, "tp", None),
        P(rows, "tp", None),
        P(rows),
        P("tp"),
        P(rows, None),
        P(None, rows, "tp", None),
        P(None, None, rows),
        P(None, None, rows, "tp"),
        P(),
    )

    return jax.shard_map(
        body,
        mesh=finer,
        in_specs=placed,
        out_specs=(P(None, None, (*rows, "tp")), P(None, rows, "tp", None)),
        check_vma=False,
    )
```

```python
import jax
import jax.numpy as jnp
from jax import lax
from jax.experimental import pallas as pl
from jax.experimental.pallas import tpu as pltpu
from jax.sharding import Mesh, PartitionSpec as P


NORM_EPSILON = 1e-06


def whole():
    return pl.BlockSpec(memory_space=pltpu.VMEM)


def shaped(shape, dtype):
    return jax.ShapeDtypeStruct(shape, dtype)


def call(kernel, out_shape, scratch, cost, limit, in_specs, out_specs):
    return pl.pallas_call(
        kernel,
        out_shape=out_shape,
        in_specs=in_specs,
        out_specs=out_specs,
        scratch_shapes=scratch,
        cost_estimate=pl.CostEstimate(flops=cost[0], bytes_accessed=cost[1], transcendentals=0),
        compiler_params=pltpu.CompilerParams(vmem_limit_bytes=limit),
    )


def advance_kernel(accepted, prev_forget, prev_input, state, new_state, rounded, live):
    block = pl.program_id(0)
    count, proposals, size = prev_forget.shape
    lanes = prev_input.shape[2]

    @pl.when(block == 0)
    def _():
        live[...] = jnp.broadcast_to(accepted[...].astype(jnp.float32), (size, lanes)).T

    shift = lax.rem(lanes - block * count, lanes)
    values = [
        pltpu.roll(prev_input[p].astype(jnp.float32), shift, 1) for p in range(proposals)
    ]
    taken = live[pl.ds(pl.multiple_of(block * count, count), count), :]
    rest = jnp.ones((count, size), jnp.float32)
    terms = [None] * proposals
    for p in reversed(range(proposals)):
        gate = jnp.where(taken > p, prev_forget[:, p, :], 1.0)
        terms[p] = rest * (1.0 - gate)
        rest = rest * gate
    for s in range(count):
        fresh = rest[s : s + 1] * state[s]
        for p in range(proposals):
            fresh = fresh + terms[p][s : s + 1] * values[p][:, s : s + 1]
        new_state[s] = fresh
        rounded[s] = fresh.astype(jnp.bfloat16)


def advance(accepted, prev_forget, prev_input, state):
    seqs, values, keys = state.shape
    proposals = prev_forget.shape[1]
    count = 32
    span = pl.BlockSpec((count, values, keys), lambda i: (i, 0, 0))
    return pl.pallas_call(
        advance_kernel,
        grid=(seqs // count,),
        in_specs=[
            pl.BlockSpec((1, seqs), lambda i: (0, 0)),
            pl.BlockSpec((count, proposals, keys), lambda i: (i, 0, 0)),
            pl.BlockSpec((proposals, values, seqs), lambda i: (0, 0, 0)),
            span,
        ],
        out_specs=[span, span],
        out_shape=[shaped(state.shape, jnp.float32), shaped(state.shape, jnp.bfloat16)],
        scratch_shapes=[pltpu.VMEM((keys, seqs), jnp.float32)],
        name="advance",
        cost_estimate=pl.CostEstimate(
            flops=1_000_000_000, bytes_accessed=5 << 20, transcendentals=0
        ),
        compiler_params=pltpu.CompilerParams(vmem_limit_bytes=16 << 20),
    )(accepted[None], prev_forget, prev_input, state)


def split_in_three(value):
    high = value.astype(jnp.bfloat16).astype(jnp.float32)
    middle = (value - high).astype(jnp.bfloat16).astype(jnp.float32)
    return high, middle, value - high - middle


def three_rows(parts, width):
    rest = jnp.zeros((16 - 3 * parts[0].shape[0], width), jnp.float32)
    return jnp.concatenate([*parts, rest], axis=0).astype(jnp.bfloat16)


def source_kernel(tokens, out):
    steps = tokens.shape[0]
    for z in range(out.shape[0] // steps):
        out[pl.ds(z * steps, steps)] = tokens[...]


def source(tokens, planes):
    steps, features, seqs = tokens.shape
    return call(
        source_kernel,
        shaped((planes * steps, features, seqs), jnp.bfloat16),
        [],
        (1_000_000, 1 << 20),
        60 << 20,
        [whole()],
        whole(),
    )(tokens)


def turn_kernel(gain, w_query, w_forget, keyed):
    size = gain.shape[1]
    for b in range(w_query.shape[0] // size):
        at = pl.ds(b * size, size)
        row = gain[pl.ds(b, 1), :]
        for i, weight in enumerate((w_query, w_forget)):
            block = weight[at, :].astype(jnp.float32).T
            keyed[pl.ds(i * size, size), at] = (block * row).astype(jnp.bfloat16)


def turn(gain, w_query, w_forget):
    width, size = w_query.shape
    return call(
        turn_kernel,
        shaped((2 * size, width), jnp.bfloat16),
        [],
        (1_000_000_000, 4 << 20),
        16 << 20,
        [whole()] * 3,
        whole(),
    )(gain, w_query, w_forget)


def fold_kernel(gain, w0, w1, w2, w3, out):
    values, size = w0.shape[1], gain.shape[1]
    for b in range(gain.shape[0]):
        at = pl.ds(b * size, size)
        for d, weight in enumerate((w0, w1, w2, w3)):
            value = weight[0, :, at].astype(jnp.float32) * gain[pl.ds(b, 1), :]
            out[pl.ds(d * values, values), at] = value.astype(jnp.bfloat16)


def fold(gain, weights):
    _, values, width = weights[0].shape
    return call(
        fold_kernel,
        shaped((4 * values, width), jnp.bfloat16),
        [],
        (1_000_000_000, 2 << 20),
        16 << 20,
        [whole()] * 5,
        whole(),
    )(gain, *weights)


def project_kernel(own, other, keyed, mixing, o0, o1, o2, o3, held, scale):
    core = lax.axis_index("core")
    blocks, size, seqs = own.shape
    squares = jnp.zeros((8, seqs), jnp.float32)
    for half, ref in ((core, own), (1 - core, other)):
        for b in range(blocks):
            part = ref[b]
            held[pl.ds(pl.multiple_of((2 * b + half) * size, size), size), :] = part
            wide = part.astype(jnp.float32)
            squares = squares + jnp.sum((wide * wide).reshape(size // 8, 8, seqs), axis=0)
    total = jnp.sum(squares, axis=0, keepdims=True)
    factor = lax.rsqrt(total / (2 * blocks * size) + NORM_EPSILON)
    scale[...] = jnp.broadcast_to(factor, scale.shape)
    rows = held[...]
    first = jnp.dot(keyed[...], rows, preferred_element_type=jnp.float32) * factor
    first = first.astype(jnp.bfloat16)
    second = jnp.dot(mixing[...], rows, preferred_element_type=jnp.float32) * factor
    second = second.astype(jnp.bfloat16)
    keys, values = first.shape[0], second.shape[0] // 4
    for d, out in enumerate((o0, o1, o2, o3)):
        out[pl.ds(0, keys), :] = first
        out[pl.ds(keys, values), :] = second[d * values : (d + 1) * values]


def project(own, other, keyed, mixing):
    blocks, size, seqs = own.shape
    rows = keyed.shape[0] + mixing.shape[0] // 4
    outs = call(
        project_kernel,
        [shaped((rows, seqs), jnp.bfloat16)] * 4
        + [shaped((2 * blocks * size, seqs), jnp.bfloat16), shaped((8, seqs), jnp.float32)],
        [],
        (1_000_000_000, 3 << 20),
        16 << 20,
        [whole()] * 4,
        [whole()] * 6,
    )(own, other, keyed, mixing)
    return outs[:4], outs[4], outs[5]


def gate_kernel(gain, w0, w1, w2, w3, rows, scale, out, held):
    values, size = w0.shape[1], gain.shape[1]
    for b in range(gain.shape[0]):
        at = pl.ds(b * size, size)
        for d, weight in enumerate((w0, w1, w2, w3)):
            value = weight[0, :, at].astype(jnp.float32) * gain[pl.ds(b, 1), :]
            held[pl.ds(d * values, values), at] = value.astype(jnp.bfloat16)
    raw = jnp.dot(held[...], rows[...], preferred_element_type=jnp.float32) * scale[0:1]
    raw = raw.astype(jnp.bfloat16).astype(jnp.float32)
    out[...] = raw * jax.nn.sigmoid(raw)


def gate(gain, weights, rows, scale):
    _, values, width = weights[0].shape
    return call(
        gate_kernel,
        shaped((4 * values, rows.shape[1]), jnp.float32),
        [pltpu.VMEM((4 * values, width), jnp.bfloat16)],
        (1_000_000_000, 3 << 20),
        16 << 20,
        [whole()] * 7,
        whole(),
    )(gain, *weights, rows, scale)


def outward_kernel(w_out, mine, theirs, held, sems):
    core = lax.axis_index("core")
    cuts, size, span = held.shape
    copies = [
        pltpu.make_async_copy(w_out.at[:, pl.ds(c * span, span)], held.at[c], sems.at[c])
        for c in range(cuts)
    ]
    for copy in copies:
        copy.start()
    pairs = span // size // 2
    for c in range(cuts):
        copies[c].wait()
        for b in range(pairs):
            for half, out in ((core, mine), (1 - core, theirs)):
                at = pl.multiple_of((2 * b + half) * size, size)
                block = held[c, :, pl.ds(at, size)].astype(jnp.float32)
                out[c * pairs + b] = block.T.astype(jnp.bfloat16)


def turn_outward(w_out):
    size, width = w_out.shape
    return call(
        outward_kernel,
        [shaped((width // size // 2, size, size), jnp.bfloat16)] * 2,
        [pltpu.VMEM((4, size, width // 4), jnp.bfloat16), pltpu.SemaphoreType.DMA((4,))],
        (1_000_000_000, 2 << 20),
        16 << 20,
        [pl.BlockSpec(memory_space=pltpu.HBM)],
        [whole()] * 2,
    )(w_out)


def recur_kernel(r0, r1, r2, r3, before, floor, head_gain, o0, o1, o2, o3, seen, ready):
    mine = lax.axis_index("tp")
    size = floor.shape[1]
    values = head_gain.shape[1]
    count = before.shape[0] // values
    steps = 4
    for d, ref in enumerate((r0, r1, r2, r3)):
        seen[mine ^ d] = ref[...]
    low = jnp.broadcast_to(floor[...], (count, size)).T
    scale = jnp.broadcast_to(head_gain[...], (count, values)).T
    forget, keys, fresh, sums, asked = [], [], [], [], []
    for t in range(steps):
        gate = low + (1.0 - low) * jax.nn.sigmoid(seen[t, pl.ds(size, size), :].astype(jnp.float32))
        forget.append(gate)
        keys.append(1.0 - gate)
        fresh.append(seen[t, pl.ds(2 * size, values), :].astype(jnp.float32))
    for t in range(steps):
        moved = seen[t, pl.ds(0, size), :].astype(jnp.float32)
        out = None
        for u in reversed(range(t + 1)):
            score = jnp.sum(moved * keys[u], axis=0, keepdims=True)
            term = score * fresh[u]
            out = term if out is None else out + term
            moved = moved * forget[u]
        sums.append(out)
        asked.append(moved.astype(jnp.bfloat16))
    lane = lax.broadcasted_iota(jnp.int32, (values, count), 1)
    asked = jnp.concatenate(asked, axis=1)
    group = 8
    for b in range(count // group):
        read = jnp.dot(
            before[pl.ds(b * group * values, group * values), :],
            asked,
            preferred_element_type=jnp.float32,
        )
        for s in range(group):
            hit = lane == b * group + s
            for t in range(steps):
                part = read[s * values : (s + 1) * values, t * count : (t + 1) * count]
                sums[t] = sums[t] + jnp.where(hit, part, 0.0)
    for t in range(steps):
        out = sums[t]
        square = jnp.sum(out * out, axis=0, keepdims=True)
        ready[t, pl.ds(0, values), :] = (out * scale).astype(jnp.bfloat16)
        ready[t, pl.ds(values, 16), :] = three_rows(split_in_three(square), count)
    for d, ref in enumerate((o0, o1, o2, o3)):
        ref[...] = ready[mine ^ d]


def recur(received, before, floor, head_gain):
    rows, count = received[0].shape
    values = head_gain.shape[1]
    return call(
        recur_kernel,
        [shaped((values + 16, count), jnp.bfloat16)] * 4,
        [
            pltpu.VMEM((4, rows, count), jnp.bfloat16),
            pltpu.VMEM((4, values + 16, count), jnp.bfloat16),
        ],
        (1_000_000_000, 2 << 20),
        16 << 20,
        [whole()] * 7,
        [whole()] * 4,
    )(*received, before, floor, head_gain)


def hide_kernel(p0, p1, p2, p3, gates, hidden):
    mine = lax.axis_index("tp")
    values = hidden.shape[0] // 4
    parts = (p0, p1, p2, p3)
    total = None
    for ref in parts:
        square = jnp.sum(ref[pl.ds(values, 16), :].astype(jnp.float32), axis=0, keepdims=True)
        total = square if total is None else total + square
    factor = lax.rsqrt(total / hidden.shape[0] + NORM_EPSILON)
    for d, ref in enumerate(parts):
        at = pl.multiple_of((mine ^ d) * values, values)
        value = ref[pl.ds(0, values), :].astype(jnp.float32) * factor
        value = value * gates[pl.ds(d * values, values), :]
        hidden[pl.ds(at, values), :] = value.astype(jnp.bfloat16)


def hide(parts, gates):
    return call(
        hide_kernel,
        shaped(gates.shape, jnp.bfloat16),
        [],
        (1_000_000, 1 << 18),
        16 << 20,
        [whole()] * 5,
        whole(),
    )(*parts, gates)


def emit_kernel(hidden, other, ours, theirs, out):
    for b in range(out.shape[0]):
        part = jnp.dot(ours[b], hidden[...], preferred_element_type=jnp.float32)
        part = part + jnp.dot(theirs[b], other[...], preferred_element_type=jnp.float32)
        out[b] = part.astype(jnp.bfloat16)


def emit(hidden, other, ours, theirs):
    blocks, size, _ = ours.shape
    return call(
        emit_kernel,
        shaped((blocks, size, hidden.shape[1]), jnp.bfloat16),
        [],
        (100_000_000, 2 << 20),
        16 << 20,
        [whole()] * 4,
        whole(),
    )(hidden, other, ours, theirs)


def sum_kernel(parts, out):
    total = parts[0].astype(jnp.float32)
    for b in range(1, parts.shape[0]):
        total = total + parts[b].astype(jnp.float32)
    out[...] = total.astype(out.dtype)


def sums(parts):
    return call(
        sum_kernel,
        shaped(parts.shape[1:], jnp.bfloat16),
        [],
        (1_000_000, 1 << 20),
        8 << 20,
        [whole()],
        whole(),
    )(parts)


def body(
    tokens,
    input_norm_gain,
    w_query,
    w_forget,
    w_input,
    w_gate,
    forget_floor,
    head_gain,
    w_out,
    state,
    prev_forget,
    prev_input,
    accepted,
):
    planes, group = lax.axis_size("zy"), lax.axis_size("tp")
    seqs, proposals, features = tokens.shape
    _, size = w_query.shape
    swap = [(0, 1), (1, 0)]
    hops = [[(i, i ^ d) for i in range(group)] for d in range(group)]

    def passed(parts):
        return [parts[0]] + [lax.ppermute(parts[d], "tp", hops[d]) for d in (1, 2, 3)]

    gain = input_norm_gain.reshape(-1, size)
    own = lax.all_to_all(
        source(tokens.transpose(1, 2, 0), planes), ("zy", "tp"), 0, 0, tiled=True
    )
    own = own.reshape(planes, group * features, seqs)
    other = lax.ppermute(own, "core", swap)
    inputs = passed([w_input] * group)
    gates = passed([w_gate] * group)
    keyed = turn(gain, w_query, w_forget)
    mixing = fold(gain, inputs)
    new_state, rounded = advance(
        accepted,
        prev_forget,
        prev_input.reshape(seqs, proposals, -1).transpose(1, 2, 0),
        state[:, 0],
    )

    sends, rows, scale = project(own, other, keyed, mixing)
    received = passed(sends)
    ours, theirs = turn_outward(w_out)
    theirs = lax.ppermute(theirs, "core", swap)
    shown = recur(received, rounded.reshape(-1, size), forget_floor[None], head_gain[None])
    parts = passed(shown)
    opened = gate(gain, gates, rows, scale)
    hidden = hide(parts, opened)
    kept = emit(hidden, lax.ppermute(hidden, "core", swap), ours, theirs)
    terms = lax.all_to_all(
        kept.reshape(planes * group, features, seqs), ("zy", "tp"), 0, 0, tiled=True
    )
    mixed = sums(terms.reshape(planes, group, features, seqs))
    return mixed.transpose(2, 0, 1), new_state[:, None]


def solution(mesh):
    kv, tp = mesh.shape["kv"], mesh.shape["tp"]
    finer = Mesh(mesh.devices.reshape(kv // 2, 2, tp), ("zy", "core", "tp"))
    rows = ("zy", "core")
    placed = (
        P(None, None, (*rows, "tp")),
        P(),
        P(None, rows),
        P(None, rows),
        P(rows, "tp", None),
        P(rows, "tp", None),
        P(rows),
        P("tp"),
        P(rows, None),
        P(None, rows, "tp", None),
        P(None, None, rows),
        P(None, None, rows, "tp"),
        P(),
    )

    return jax.shard_map(
        body,
        mesh=finer,
        in_specs=placed,
        out_specs=(P(None, None, (*rows, "tp")), P(None, rows, "tp", None)),
        check_vma=False,
    )
```

```python
import jax
import jax.numpy as jnp
from jax import lax
from jax.experimental import pallas as pl
from jax.experimental.pallas import tpu as pltpu
from jax.sharding import Mesh, PartitionSpec as P


NORM_EPSILON = 1e-06


def whole():
    return pl.BlockSpec(memory_space=pltpu.VMEM)


def shaped(shape, dtype):
    return jax.ShapeDtypeStruct(shape, dtype)


def call(kernel, out_shape, scratch, cost, limit, in_specs, out_specs):
    return pl.pallas_call(
        kernel,
        out_shape=out_shape,
        in_specs=in_specs,
        out_specs=out_specs,
        scratch_shapes=scratch,
        cost_estimate=pl.CostEstimate(flops=cost[0], bytes_accessed=cost[1], transcendentals=0),
        compiler_params=pltpu.CompilerParams(vmem_limit_bytes=limit),
    )


def advance_kernel(accepted, prev_forget, prev_input, state, new_state, live):
    block = pl.program_id(0)
    count, proposals, size = prev_forget.shape
    lanes = prev_input.shape[2]

    @pl.when(block == 0)
    def _():
        live[...] = jnp.broadcast_to(accepted[...].astype(jnp.float32), (size, lanes)).T

    shift = lax.rem(lanes - block * count, lanes)
    values = [
        pltpu.roll(prev_input[p].astype(jnp.float32), shift, 1) for p in range(proposals)
    ]
    taken = live[pl.ds(pl.multiple_of(block * count, count), count), :]
    rest = jnp.ones((count, size), jnp.float32)
    terms = [None] * proposals
    for p in reversed(range(proposals)):
        gate = jnp.where(taken > p, prev_forget[:, p, :], 1.0)
        terms[p] = rest * (1.0 - gate)
        rest = rest * gate
    for s in range(count):
        fresh = rest[s : s + 1] * state[s]
        for p in range(proposals):
            fresh = fresh + terms[p][s : s + 1] * values[p][:, s : s + 1]
        new_state[s] = fresh


def advance(accepted, prev_forget, prev_input, state):
    seqs, values, keys = state.shape
    proposals = prev_forget.shape[1]
    count = 32
    span = pl.BlockSpec((count, values, keys), lambda i: (i, 0, 0))
    return pl.pallas_call(
        advance_kernel,
        grid=(seqs // count,),
        in_specs=[
            pl.BlockSpec((1, seqs), lambda i: (0, 0)),
            pl.BlockSpec((count, proposals, keys), lambda i: (i, 0, 0)),
            pl.BlockSpec((proposals, values, seqs), lambda i: (0, 0, 0)),
            span,
        ],
        out_specs=span,
        out_shape=shaped(state.shape, jnp.float32),
        scratch_shapes=[pltpu.VMEM((keys, seqs), jnp.float32)],
        name="advance",
        cost_estimate=pl.CostEstimate(
            flops=1_000_000_000, bytes_accessed=5 << 20, transcendentals=0
        ),
        compiler_params=pltpu.CompilerParams(vmem_limit_bytes=16 << 20),
    )(accepted[None], prev_forget, prev_input, state)


def split_in_three(value):
    high = value.astype(jnp.bfloat16).astype(jnp.float32)
    middle = (value - high).astype(jnp.bfloat16).astype(jnp.float32)
    return high, middle, value - high - middle


def three_rows(parts, width):
    rest = jnp.zeros((16 - 3 * parts[0].shape[0], width), jnp.float32)
    return jnp.concatenate([*parts, rest], axis=0).astype(jnp.bfloat16)


def source_kernel(tokens, gain, weight, out, folded):
    steps = tokens.shape[0]
    for z in range(out.shape[0] // steps):
        out[pl.ds(z * steps, steps)] = tokens[...]
    size = gain.shape[1]
    for b in range(gain.shape[0]):
        at = pl.ds(b * size, size)
        value = weight[0, :, at].astype(jnp.float32) * gain[pl.ds(b, 1), :]
        folded[:, at] = value.astype(jnp.bfloat16)


def source(tokens, gain, weight, planes):
    steps, features, seqs = tokens.shape
    return call(
        source_kernel,
        [
            shaped((planes * steps, features, seqs), jnp.bfloat16),
            shaped(weight.shape[1:], jnp.bfloat16),
        ],
        [],
        (1_000_000, 1 << 20),
        60 << 20,
        [whole()] * 3,
        [whole()] * 2,
    )(tokens, gain, weight)


def turn_kernel(gain, w_query, w_forget, keyed):
    size = gain.shape[1]
    for b in range(w_query.shape[0] // size):
        at = pl.ds(b * size, size)
        row = gain[pl.ds(b, 1), :]
        for i, weight in enumerate((w_query, w_forget)):
            block = weight[at, :].astype(jnp.float32).T
            keyed[pl.ds(i * size, size), at] = (block * row).astype(jnp.bfloat16)


def turn(gain, w_query, w_forget):
    width, size = w_query.shape
    return call(
        turn_kernel,
        shaped((2 * size, width), jnp.bfloat16),
        [],
        (1_000_000_000, 4 << 20),
        16 << 20,
        [whole()] * 3,
        whole(),
    )(gain, w_query, w_forget)


def project_kernel(own, other, keyed, w0, w1, w2, w3, o0, o1, o2, o3, held, scale, mixing):
    values = w0.shape[0]
    for d, weight in enumerate((w0, w1, w2, w3)):
        mixing[pl.ds(d * values, values), :] = weight[...]
    core = lax.axis_index("core")
    blocks, size, seqs = own.shape
    squares = jnp.zeros((8, seqs), jnp.float32)
    for half, ref in ((core, own), (1 - core, other)):
        for b in range(blocks):
            part = ref[b]
            held[pl.ds(pl.multiple_of((2 * b + half) * size, size), size), :] = part
            wide = part.astype(jnp.float32)
            squares = squares + jnp.sum((wide * wide).reshape(size // 8, 8, seqs), axis=0)
    total = jnp.sum(squares, axis=0, keepdims=True)
    factor = lax.rsqrt(total / (2 * blocks * size) + NORM_EPSILON)
    scale[...] = jnp.broadcast_to(factor, scale.shape)
    rows = held[...]
    first = jnp.dot(keyed[...], rows, preferred_element_type=jnp.float32) * factor
    first = first.astype(jnp.bfloat16)
    second = jnp.dot(mixing[...], rows, preferred_element_type=jnp.float32) * factor
    second = second.astype(jnp.bfloat16)
    keys = first.shape[0]
    for d, out in enumerate((o0, o1, o2, o3)):
        out[pl.ds(0, keys), :] = first
        out[pl.ds(keys, values), :] = second[d * values : (d + 1) * values]


def project(own, other, keyed, weights):
    blocks, size, seqs = own.shape
    values, width = weights[0].shape
    rows = keyed.shape[0] + values
    outs = call(
        project_kernel,
        [shaped((rows, seqs), jnp.bfloat16)] * 4
        + [shaped((2 * blocks * size, seqs), jnp.bfloat16), shaped((8, seqs), jnp.float32)],
        [pltpu.VMEM((4 * values, width), jnp.bfloat16)],
        (1_000_000_000, 3 << 20),
        16 << 20,
        [whole()] * 7,
        [whole()] * 6,
    )(own, other, keyed, *weights)
    return outs[:4], outs[4], outs[5]


def gate_kernel(gain, w0, w1, w2, w3, rows, scale, out, held):
    values, size = w0.shape[1], gain.shape[1]
    for b in range(gain.shape[0]):
        at = pl.ds(b * size, size)
        for d, weight in enumerate((w0, w1, w2, w3)):
            value = weight[0, :, at].astype(jnp.float32) * gain[pl.ds(b, 1), :]
            held[pl.ds(d * values, values), at] = value.astype(jnp.bfloat16)
    raw = jnp.dot(held[...], rows[...], preferred_element_type=jnp.float32) * scale[0:1]
    raw = raw.astype(jnp.bfloat16).astype(jnp.float32)
    out[...] = raw * jax.nn.sigmoid(raw)


def gate(gain, weights, rows, scale):
    _, values, width = weights[0].shape
    return call(
        gate_kernel,
        shaped((4 * values, rows.shape[1]), jnp.float32),
        [pltpu.VMEM((4 * values, width), jnp.bfloat16)],
        (1_000_000_000, 3 << 20),
        16 << 20,
        [whole()] * 7,
        whole(),
    )(gain, *weights, rows, scale)


def outward_kernel(w_out, mine, theirs, held, sems):
    core = lax.axis_index("core")
    cuts, size, span = held.shape
    copies = [
        pltpu.make_async_copy(w_out.at[:, pl.ds(c * span, span)], held.at[c], sems.at[c])
        for c in range(cuts)
    ]
    for copy in copies:
        copy.start()
    pairs = span // size // 2
    for c in range(cuts):
        copies[c].wait()
        for b in range(pairs):
            for half, out in ((core, mine), (1 - core, theirs)):
                at = pl.multiple_of((2 * b + half) * size, size)
                block = held[c, :, pl.ds(at, size)].astype(jnp.float32)
                out[c * pairs + b] = block.T.astype(jnp.bfloat16)


def turn_outward(w_out):
    size, width = w_out.shape
    return call(
        outward_kernel,
        [shaped((width // size // 2, size, size), jnp.bfloat16)] * 2,
        [pltpu.VMEM((4, size, width // 4), jnp.bfloat16), pltpu.SemaphoreType.DMA((4,))],
        (1_000_000_000, 2 << 20),
        16 << 20,
        [pl.BlockSpec(memory_space=pltpu.HBM)],
        [whole()] * 2,
    )(w_out)


def recur_kernel(r0, r1, r2, r3, before, floor, head_gain, o0, o1, o2, o3, seen, ready):
    mine = lax.axis_index("tp")
    size = floor.shape[1]
    values = head_gain.shape[1]
    count = before.shape[0] // values
    steps = 4
    for d, ref in enumerate((r0, r1, r2, r3)):
        seen[mine ^ d] = ref[...]
    low = jnp.broadcast_to(floor[...], (count, size)).T
    scale = jnp.broadcast_to(head_gain[...], (count, values)).T
    forget, keys, fresh, sums, asked = [], [], [], [], []
    for t in range(steps):
        gate = low + (1.0 - low) * jax.nn.sigmoid(seen[t, pl.ds(size, size), :].astype(jnp.float32))
        forget.append(gate)
        keys.append(1.0 - gate)
        fresh.append(seen[t, pl.ds(2 * size, values), :].astype(jnp.float32))
    for t in range(steps):
        moved = seen[t, pl.ds(0, size), :].astype(jnp.float32)
        out = None
        for u in reversed(range(t + 1)):
            score = jnp.sum(moved * keys[u], axis=0, keepdims=True)
            term = score * fresh[u]
            out = term if out is None else out + term
            moved = moved * forget[u]
        sums.append(out)
        asked.append(moved.astype(jnp.bfloat16))
    lane = lax.broadcasted_iota(jnp.int32, (values, count), 1)
    asked = jnp.concatenate(asked, axis=1)
    group = 8
    for b in range(count // group):
        read = jnp.dot(
            before[pl.ds(b * group * values, group * values), :].astype(jnp.bfloat16),
            asked,
            preferred_element_type=jnp.float32,
        )
        for s in range(group):
            hit = lane == b * group + s
            for t in range(steps):
                part = read[s * values : (s + 1) * values, t * count : (t + 1) * count]
                sums[t] = sums[t] + jnp.where(hit, part, 0.0)
    for t in range(steps):
        out = sums[t]
        square = jnp.sum(out * out, axis=0, keepdims=True)
        ready[t, pl.ds(0, values), :] = (out * scale).astype(jnp.bfloat16)
        ready[t, pl.ds(values, 16), :] = three_rows(split_in_three(square), count)
    for d, ref in enumerate((o0, o1, o2, o3)):
        ref[...] = ready[mine ^ d]


def recur(received, before, floor, head_gain):
    rows, count = received[0].shape
    values = head_gain.shape[1]
    return call(
        recur_kernel,
        [shaped((values + 16, count), jnp.bfloat16)] * 4,
        [
            pltpu.VMEM((4, rows, count), jnp.bfloat16),
            pltpu.VMEM((4, values + 16, count), jnp.bfloat16),
        ],
        (1_000_000_000, 2 << 20),
        16 << 20,
        [whole()] * 7,
        [whole()] * 4,
    )(*received, before, floor, head_gain)


def hide_kernel(p0, p1, p2, p3, gates, hidden):
    mine = lax.axis_index("tp")
    values = hidden.shape[0] // 4
    parts = (p0, p1, p2, p3)
    total = None
    for ref in parts:
        square = jnp.sum(ref[pl.ds(values, 16), :].astype(jnp.float32), axis=0, keepdims=True)
        total = square if total is None else total + square
    factor = lax.rsqrt(total / hidden.shape[0] + NORM_EPSILON)
    for d, ref in enumerate(parts):
        at = pl.multiple_of((mine ^ d) * values, values)
        value = ref[pl.ds(0, values), :].astype(jnp.float32) * factor
        value = value * gates[pl.ds(d * values, values), :]
        hidden[pl.ds(at, values), :] = value.astype(jnp.bfloat16)


def hide(parts, gates):
    return call(
        hide_kernel,
        shaped(gates.shape, jnp.bfloat16),
        [],
        (1_000_000, 1 << 18),
        16 << 20,
        [whole()] * 5,
        whole(),
    )(*parts, gates)


def emit_kernel(hidden, other, ours, theirs, out):
    for b in range(out.shape[0]):
        part = jnp.dot(ours[b], hidden[...], preferred_element_type=jnp.float32)
        part = part + jnp.dot(theirs[b], other[...], preferred_element_type=jnp.float32)
        out[b] = part.astype(jnp.bfloat16)


def emit(hidden, other, ours, theirs):
    blocks, size, _ = ours.shape
    return call(
        emit_kernel,
        shaped((blocks, size, hidden.shape[1]), jnp.bfloat16),
        [],
        (100_000_000, 2 << 20),
        16 << 20,
        [whole()] * 4,
        whole(),
    )(hidden, other, ours, theirs)


def sum_kernel(parts, out):
    total = parts[0].astype(jnp.float32)
    for b in range(1, parts.shape[0]):
        total = total + parts[b].astype(jnp.float32)
    out[...] = total.astype(out.dtype)


def sums(parts):
    return call(
        sum_kernel,
        shaped(parts.shape[1:], jnp.bfloat16),
        [],
        (1_000_000, 1 << 20),
        8 << 20,
        [whole()],
        whole(),
    )(parts)


def body(
    tokens,
    input_norm_gain,
    w_query,
    w_forget,
    w_input,
    w_gate,
    forget_floor,
    head_gain,
    w_out,
    state,
    prev_forget,
    prev_input,
    accepted,
):
    planes, group = lax.axis_size("zy"), lax.axis_size("tp")
    seqs, proposals, features = tokens.shape
    _, size = w_query.shape
    swap = [(0, 1), (1, 0)]
    hops = [[(i, i ^ d) for i in range(group)] for d in range(group)]

    def passed(parts):
        return [parts[0]] + [lax.ppermute(parts[d], "tp", hops[d]) for d in (1, 2, 3)]

    gain = input_norm_gain.reshape(-1, size)
    spread, folded = source(tokens.transpose(1, 2, 0), gain, w_input, planes)
    own = lax.all_to_all(spread, ("zy", "tp"), 0, 0, tiled=True)
    own = own.reshape(planes, group * features, seqs)
    other = lax.ppermute(own, "core", swap)
    inputs = passed([folded] * group)
    gates = passed([w_gate] * group)
    keyed = turn(gain, w_query, w_forget)
    new_state = advance(
        accepted,
        prev_forget,
        prev_input.reshape(seqs, proposals, -1).transpose(1, 2, 0),
        state[:, 0],
    )

    sends, rows, scale = project(own, other, keyed, inputs)
    received = passed(sends)
    ours, theirs = turn_outward(w_out)
    theirs = lax.ppermute(theirs, "core", swap)
    shown = recur(received, new_state.reshape(-1, size), forget_floor[None], head_gain[None])
    parts = passed(shown)
    opened = gate(gain, gates, rows, scale)
    hidden = hide(parts, opened)
    kept = emit(hidden, lax.ppermute(hidden, "core", swap), ours, theirs)
    terms = lax.all_to_all(
        kept.reshape(planes * group, features, seqs), ("zy", "tp"), 0, 0, tiled=True
    )
    mixed = sums(terms.reshape(planes, group, features, seqs))
    return mixed.transpose(2, 0, 1), new_state[:, None]


def solution(mesh):
    kv, tp = mesh.shape["kv"], mesh.shape["tp"]
    finer = Mesh(mesh.devices.reshape(kv // 2, 2, tp), ("zy", "core", "tp"))
    rows = ("zy", "core")
    placed = (
        P(None, None, (*rows, "tp")),
        P(),
        P(None, rows),
        P(None, rows),
        P(rows, "tp", None),
        P(rows, "tp", None),
        P(rows),
        P("tp"),
        P(rows, None),
        P(None, rows, "tp", None),
        P(None, None, rows),
        P(None, None, rows, "tp"),
        P(),
    )

    return jax.shard_map(
        body,
        mesh=finer,
        in_specs=placed,
        out_specs=(P(None, None, (*rows, "tp")), P(None, rows, "tp", None)),
        check_vma=False,
    )
```

```python
import jax
import jax.numpy as jnp
from jax import lax
from jax.experimental import pallas as pl
from jax.experimental.pallas import tpu as pltpu
from jax.sharding import Mesh, PartitionSpec as P


NORM_EPSILON = 1e-06


def whole():
    return pl.BlockSpec(memory_space=pltpu.VMEM)


def shaped(shape, dtype):
    return jax.ShapeDtypeStruct(shape, dtype)


def call(kernel, out_shape, scratch, cost, limit, in_specs, out_specs):
    return pl.pallas_call(
        kernel,
        out_shape=out_shape,
        in_specs=in_specs,
        out_specs=out_specs,
        scratch_shapes=scratch,
        cost_estimate=pl.CostEstimate(flops=cost[0], bytes_accessed=cost[1], transcendentals=0),
        compiler_params=pltpu.CompilerParams(vmem_limit_bytes=limit),
    )


def advance_kernel(accepted, prev_forget, prev_input, state, new_state, rounded, live):
    block = pl.program_id(0)
    count, proposals, size = prev_forget.shape
    lanes = prev_input.shape[2]

    @pl.when(block == 0)
    def _():
        live[...] = jnp.broadcast_to(accepted[...].astype(jnp.float32), (size, lanes)).T

    shift = lax.rem(lanes - block * count, lanes)
    values = [
        pltpu.roll(prev_input[p].astype(jnp.float32), shift, 1) for p in range(proposals)
    ]
    taken = live[pl.ds(pl.multiple_of(block * count, count), count), :]
    rest = jnp.ones((count, size), jnp.float32)
    terms = [None] * proposals
    for p in reversed(range(proposals)):
        gate = jnp.where(taken > p, prev_forget[:, p, :], 1.0)
        terms[p] = rest * (1.0 - gate)
        rest = rest * gate
    for s in range(count):
        fresh = rest[s : s + 1] * state[s]
        for p in range(proposals):
            fresh = fresh + terms[p][s : s + 1] * values[p][:, s : s + 1]
        new_state[s] = fresh
        rounded[s] = fresh.astype(jnp.bfloat16)


def advance(accepted, prev_forget, prev_input, state):
    seqs, values, keys = state.shape
    proposals = prev_forget.shape[1]
    count = 32
    span = pl.BlockSpec((count, values, keys), lambda i: (i, 0, 0))
    return pl.pallas_call(
        advance_kernel,
        grid=(seqs // count,),
        in_specs=[
            pl.BlockSpec((1, seqs), lambda i: (0, 0)),
            pl.BlockSpec((count, proposals, keys), lambda i: (i, 0, 0)),
            pl.BlockSpec((proposals, values, seqs), lambda i: (0, 0, 0)),
            span,
        ],
        out_specs=[span, span],
        out_shape=[shaped(state.shape, jnp.float32), shaped(state.shape, jnp.bfloat16)],
        scratch_shapes=[pltpu.VMEM((keys, seqs), jnp.float32)],
        name="advance",
        cost_estimate=pl.CostEstimate(
            flops=1_000_000_000, bytes_accessed=5 << 20, transcendentals=0
        ),
        compiler_params=pltpu.CompilerParams(vmem_limit_bytes=16 << 20),
    )(accepted[None], prev_forget, prev_input, state)


def split_in_three(value):
    high = value.astype(jnp.bfloat16).astype(jnp.float32)
    middle = (value - high).astype(jnp.bfloat16).astype(jnp.float32)
    return high, middle, value - high - middle


def three_rows(parts, width):
    rest = jnp.zeros((16 - 3 * parts[0].shape[0], width), jnp.float32)
    return jnp.concatenate([*parts, rest], axis=0).astype(jnp.bfloat16)


def source_kernel(tokens, gain, w_input, w_gate, out, folded):
    steps = tokens.shape[0]
    for z in range(out.shape[0] // steps):
        out[pl.ds(z * steps, steps)] = tokens[...]
    size = gain.shape[1]
    for b in range(gain.shape[0]):
        at = pl.ds(b * size, size)
        for i, weight in enumerate((w_input, w_gate)):
            value = weight[0, :, at].astype(jnp.float32) * gain[pl.ds(b, 1), :]
            folded[i, :, at] = value.astype(jnp.bfloat16)


def source(tokens, gain, w_input, w_gate, planes):
    steps, features, seqs = tokens.shape
    return call(
        source_kernel,
        [
            shaped((planes * steps, features, seqs), jnp.bfloat16),
            shaped((2, *w_input.shape[1:]), jnp.bfloat16),
        ],
        [],
        (1_000_000, 1 << 20),
        60 << 20,
        [whole()] * 4,
        [whole()] * 2,
    )(tokens, gain, w_input, w_gate)


def turn_kernel(gain, w_query, w_forget, keyed):
    size = gain.shape[1]
    for b in range(w_query.shape[0] // size):
        at = pl.ds(b * size, size)
        row = gain[pl.ds(b, 1), :]
        for i, weight in enumerate((w_query, w_forget)):
            block = weight[at, :].astype(jnp.float32).T
            keyed[pl.ds(i * size, size), at] = (block * row).astype(jnp.bfloat16)


def turn(gain, w_query, w_forget):
    width, size = w_query.shape
    return call(
        turn_kernel,
        shaped((2 * size, width), jnp.bfloat16),
        [],
        (1_000_000_000, 4 << 20),
        16 << 20,
        [whole()] * 3,
        whole(),
    )(gain, w_query, w_forget)


def bring(which, weights, held, sems):
    copies = [
        pltpu.make_async_copy(ref.at[which if ref.shape[0] > 1 else 0], held.at[d], sems.at[d])
        for d, ref in enumerate(weights)
    ]
    for copy in copies:
        copy.start()
    return copies


def project_kernel(
    own, other, keyed, w0, w1, w2, w3, o0, o1, o2, o3, held, scale, mixing, sems
):
    copies = bring(0, (w0, w1, w2, w3), mixing, sems)
    core = lax.axis_index("core")
    blocks, size, seqs = own.shape
    squares = jnp.zeros((8, seqs), jnp.float32)
    for half, ref in ((core, own), (1 - core, other)):
        for b in range(blocks):
            part = ref[b]
            held[pl.ds(pl.multiple_of((2 * b + half) * size, size), size), :] = part
            wide = part.astype(jnp.float32)
            squares = squares + jnp.sum((wide * wide).reshape(size // 8, 8, seqs), axis=0)
    total = jnp.sum(squares, axis=0, keepdims=True)
    factor = lax.rsqrt(total / (2 * blocks * size) + NORM_EPSILON)
    scale[...] = jnp.broadcast_to(factor, scale.shape)
    rows = held[...]
    first = jnp.dot(keyed[...], rows, preferred_element_type=jnp.float32) * factor
    first = first.astype(jnp.bfloat16)
    for copy in copies:
        copy.wait()
    group, values, width = mixing.shape
    mixed = mixing[...].reshape(group * values, width)
    second = jnp.dot(mixed, rows, preferred_element_type=jnp.float32) * factor
    second = second.astype(jnp.bfloat16)
    keys = first.shape[0]
    for d, out in enumerate((o0, o1, o2, o3)):
        out[pl.ds(0, keys), :] = first
        out[pl.ds(keys, values), :] = second[d * values : (d + 1) * values]


def project(own, other, keyed, weights):
    blocks, size, seqs = own.shape
    _, values, width = weights[0].shape
    rows = keyed.shape[0] + values
    outs = call(
        project_kernel,
        [shaped((rows, seqs), jnp.bfloat16)] * 4
        + [shaped((2 * blocks * size, seqs), jnp.bfloat16), shaped((8, seqs), jnp.float32)],
        [pltpu.VMEM((4, values, width), jnp.bfloat16), pltpu.SemaphoreType.DMA((4,))],
        (1_000_000_000, 3 << 20),
        16 << 20,
        [whole()] * 3 + [pl.BlockSpec(memory_space=pltpu.HBM)] * 4,
        [whole()] * 6,
    )(own, other, keyed, *weights)
    return outs[:4], outs[4], outs[5]


def gate_kernel(w0, w1, w2, w3, rows, scale, out, mixing, sems):
    for copy in bring(1, (w0, w1, w2, w3), mixing, sems):
        copy.wait()
    group, values, width = mixing.shape
    mixed = mixing[...].reshape(group * values, width)
    raw = jnp.dot(mixed, rows[...], preferred_element_type=jnp.float32) * scale[0:1]
    raw = raw.astype(jnp.bfloat16).astype(jnp.float32)
    out[...] = raw * jax.nn.sigmoid(raw)


def gate(weights, rows, scale):
    _, values, width = weights[0].shape
    return call(
        gate_kernel,
        shaped((4 * values, rows.shape[1]), jnp.float32),
        [pltpu.VMEM((4, values, width), jnp.bfloat16), pltpu.SemaphoreType.DMA((4,))],
        (1_000_000_000, 3 << 20),
        16 << 20,
        [pl.BlockSpec(memory_space=pltpu.HBM)] * 4 + [whole()] * 2,
        whole(),
    )(*weights, rows, scale)


def outward_kernel(w_out, outward, held, sems):
    cuts, size, span = held.shape
    copies = [
        pltpu.make_async_copy(w_out.at[:, pl.ds(c * span, span)], held.at[c], sems.at[c])
        for c in range(cuts)
    ]
    for copy in copies:
        copy.start()
    for c in range(cuts):
        copies[c].wait()
        for b in range(span // size):
            block = held[c, :, pl.ds(b * size, size)].astype(jnp.float32)
            outward[c * (span // size) + b] = block.T.astype(jnp.bfloat16)


def turn_outward(w_out):
    size, width = w_out.shape
    return call(
        outward_kernel,
        shaped((width // size, size, size), jnp.bfloat16),
        [pltpu.VMEM((4, size, width // 4), jnp.bfloat16), pltpu.SemaphoreType.DMA((4,))],
        (1_000_000_000, 2 << 20),
        16 << 20,
        [pl.BlockSpec(memory_space=pltpu.HBM)],
        whole(),
    )(w_out)


def recur_kernel(r0, r1, r2, r3, before, floor, head_gain, o0, o1, o2, o3, seen, ready):
    mine = lax.axis_index("tp")
    size = floor.shape[1]
    values = head_gain.shape[1]
    count = before.shape[0] // values
    steps = 4
    for d, ref in enumerate((r0, r1, r2, r3)):
        seen[mine ^ d] = ref[...]
    low = jnp.broadcast_to(floor[...], (count, size)).T
    scale = jnp.broadcast_to(head_gain[...], (count, values)).T
    forget, keys, fresh, sums, asked = [], [], [], [], []
    for t in range(steps):
        gate = low + (1.0 - low) * jax.nn.sigmoid(seen[t, pl.ds(size, size), :].astype(jnp.float32))
        forget.append(gate)
        keys.append(1.0 - gate)
        fresh.append(seen[t, pl.ds(2 * size, values), :].astype(jnp.float32))
    for t in range(steps):
        moved = seen[t, pl.ds(0, size), :].astype(jnp.float32)
        out = None
        for u in reversed(range(t + 1)):
            score = jnp.sum(moved * keys[u], axis=0, keepdims=True)
            term = score * fresh[u]
            out = term if out is None else out + term
            moved = moved * forget[u]
        sums.append(out)
        asked.append(moved.astype(jnp.bfloat16))
    lane = lax.broadcasted_iota(jnp.int32, (values, count), 1)
    asked = jnp.concatenate(asked, axis=1)
    group = 8
    for b in range(count // group):
        read = jnp.dot(
            before[pl.ds(b * group * values, group * values), :],
            asked,
            preferred_element_type=jnp.float32,
        )
        for s in range(group):
            hit = lane == b * group + s
            for t in range(steps):
                part = read[s * values : (s + 1) * values, t * count : (t + 1) * count]
                sums[t] = sums[t] + jnp.where(hit, part, 0.0)
    for t in range(steps):
        out = sums[t]
        square = jnp.sum(out * out, axis=0, keepdims=True)
        ready[t, pl.ds(0, values), :] = (out * scale).astype(jnp.bfloat16)
        ready[t, pl.ds(values, 16), :] = three_rows(split_in_three(square), count)
    for d, ref in enumerate((o0, o1, o2, o3)):
        ref[...] = ready[mine ^ d]


def recur(received, before, floor, head_gain):
    rows, count = received[0].shape
    values = head_gain.shape[1]
    return call(
        recur_kernel,
        [shaped((values + 16, count), jnp.bfloat16)] * 4,
        [
            pltpu.VMEM((4, rows, count), jnp.bfloat16),
            pltpu.VMEM((4, values + 16, count), jnp.bfloat16),
        ],
        (1_000_000_000, 2 << 20),
        16 << 20,
        [whole()] * 7,
        [whole()] * 4,
    )(*received, before, floor, head_gain)


def gathered(parts, gates, joined):
    mine = lax.axis_index("tp")
    values = joined.shape[0] // 4
    total = None
    for d, ref in enumerate(parts):
        at = pl.multiple_of((mine ^ d) * values, values)
        value = ref[pl.ds(0, values), :].astype(jnp.float32) * gates[pl.ds(d * values, values), :]
        joined[pl.ds(at, values), :] = value.astype(jnp.bfloat16)
        square = jnp.sum(ref[pl.ds(values, 16), :].astype(jnp.float32), axis=0, keepdims=True)
        total = square if total is None else total + square
    return lax.rsqrt(total / joined.shape[0] + NORM_EPSILON)


def away_kernel(p0, p1, p2, p3, gates, outward, sent, joined):
    core = lax.axis_index("core")
    factor = gathered((p0, p1, p2, p3), gates, joined)
    for b in range(sent.shape[0]):
        part = jnp.dot(outward[2 * b + 1 - core], joined[...], preferred_element_type=jnp.float32)
        sent[b] = (part * factor).astype(jnp.bfloat16)


def keep_kernel(p0, p1, p2, p3, gates, outward, came, kept, joined):
    core = lax.axis_index("core")
    factor = gathered((p0, p1, p2, p3), gates, joined)
    for b in range(kept.shape[0]):
        part = jnp.dot(outward[2 * b + core], joined[...], preferred_element_type=jnp.float32)
        kept[b] = (part * factor + came[b].astype(jnp.float32)).astype(jnp.bfloat16)


def outward_half(kernel, parts, gates, outward, *more):
    blocks, size, _ = outward.shape
    return call(
        kernel,
        shaped((blocks // 2, size, parts[0].shape[1]), jnp.bfloat16),
        [pltpu.VMEM((size, parts[0].shape[1]), jnp.bfloat16)],
        (100_000_000, 2 << 20),
        16 << 20,
        [whole()] * (6 + len(more)),
        whole(),
    )(*parts, gates, outward, *more)


def sum_kernel(parts, out):
    total = parts[0].astype(jnp.float32)
    for b in range(1, parts.shape[0]):
        total = total + parts[b].astype(jnp.float32)
    out[...] = total.astype(out.dtype)


def sums(parts):
    return call(
        sum_kernel,
        shaped(parts.shape[1:], jnp.bfloat16),
        [],
        (1_000_000, 1 << 20),
        8 << 20,
        [whole()],
        whole(),
    )(parts)


def body(
    tokens,
    input_norm_gain,
    w_query,
    w_forget,
    w_input,
    w_gate,
    forget_floor,
    head_gain,
    w_out,
    state,
    prev_forget,
    prev_input,
    accepted,
):
    planes, group = lax.axis_size("zy"), lax.axis_size("tp")
    seqs, proposals, features = tokens.shape
    _, size = w_query.shape
    swap = [(0, 1), (1, 0)]
    hops = [[(i, i ^ d) for i in range(group)] for d in range(group)]

    def passed(parts):
        return [parts[0]] + [lax.ppermute(parts[d], "tp", hops[d]) for d in (1, 2, 3)]

    gain = input_norm_gain.reshape(-1, size)
    spread, folded = source(tokens.transpose(1, 2, 0), gain, w_input, w_gate, planes)
    far = lax.ppermute(folded, "tp", hops[2])
    own = lax.all_to_all(spread, ("zy", "tp"), 0, 0, tiled=True)
    own = own.reshape(planes, group * features, seqs)
    other = lax.ppermute(own, "core", swap)
    near = [lax.ppermute(folded[:1], "tp", hops[d]) for d in (1, 3)]
    inputs = [folded, near[0], far, near[1]]
    near = [lax.ppermute(folded[1:], "tp", hops[d]) for d in (1, 3)]
    gates = [folded, near[0], far, near[1]]
    keyed = turn(gain, w_query, w_forget)
    new_state, rounded = advance(
        accepted,
        prev_forget,
        prev_input.reshape(seqs, proposals, -1).transpose(1, 2, 0),
        state[:, 0],
    )

    sends, rows, scale = project(own, other, keyed, inputs)
    received = passed(sends)
    shown = recur(received, rounded.reshape(-1, size), forget_floor[None], head_gain[None])
    parts = passed(shown)
    outward = turn_outward(w_out)
    opened = gate(gates, rows, scale)
    sent = outward_half(away_kernel, parts, opened, outward)
    came = lax.ppermute(sent, "core", swap)
    kept = outward_half(keep_kernel, parts, opened, outward, came)
    terms = lax.all_to_all(
        kept.reshape(planes * group, features, seqs), ("zy", "tp"), 0, 0, tiled=True
    )
    mixed = sums(terms.reshape(planes, group, features, seqs))
    return mixed.transpose(2, 0, 1), new_state[:, None]


def solution(mesh):
    kv, tp = mesh.shape["kv"], mesh.shape["tp"]
    finer = Mesh(mesh.devices.reshape(kv // 2, 2, tp), ("zy", "core", "tp"))
    rows = ("zy", "core")
    placed = (
        P(None, None, (*rows, "tp")),
        P(),
        P(None, rows),
        P(None, rows),
        P(rows, "tp", None),
        P(rows, "tp", None),
        P(rows),
        P("tp"),
        P(rows, None),
        P(None, rows, "tp", None),
        P(None, None, rows),
        P(None, None, rows, "tp"),
        P(),
    )

    return jax.shard_map(
        body,
        mesh=finer,
        in_specs=placed,
        out_specs=(P(None, None, (*rows, "tp")), P(None, rows, "tp", None)),
        check_vma=False,
    )
```

```python
import functools

import jax
import jax.numpy as jnp
from jax import lax
from jax.experimental import pallas as pl
from jax.experimental.pallas import tpu as pltpu
from jax.sharding import Mesh, PartitionSpec as P


NORM_EPSILON = 1e-06


def whole():
    return pl.BlockSpec(memory_space=pltpu.VMEM)


def shaped(shape, dtype):
    return jax.ShapeDtypeStruct(shape, dtype)


def call(kernel, out_shape, scratch, cost, limit, in_specs, out_specs):
    return pl.pallas_call(
        kernel,
        out_shape=out_shape,
        in_specs=in_specs,
        out_specs=out_specs,
        scratch_shapes=scratch,
        cost_estimate=pl.CostEstimate(flops=cost[0], bytes_accessed=cost[1], transcendentals=0),
        compiler_params=pltpu.CompilerParams(vmem_limit_bytes=limit),
    )


def advance_kernel(accepted, prev_forget, prev_input, state, new_state, rounded, live):
    block = pl.program_id(0)
    count, proposals, size = prev_forget.shape
    lanes = prev_input.shape[2]

    @pl.when(block == 0)
    def _():
        live[...] = jnp.broadcast_to(accepted[...].astype(jnp.float32), (size, lanes)).T

    shift = lax.rem(lanes - block * count, lanes)
    values = [
        pltpu.roll(prev_input[p].astype(jnp.float32), shift, 1) for p in range(proposals)
    ]
    taken = live[pl.ds(pl.multiple_of(block * count, count), count), :]
    rest = jnp.ones((count, size), jnp.float32)
    terms = [None] * proposals
    for p in reversed(range(proposals)):
        gate = jnp.where(taken > p, prev_forget[:, p, :], 1.0)
        terms[p] = rest * (1.0 - gate)
        rest = rest * gate
    for s in range(count):
        fresh = rest[s : s + 1] * state[s]
        for p in range(proposals):
            fresh = fresh + terms[p][s : s + 1] * values[p][:, s : s + 1]
        new_state[s] = fresh
        rounded[s] = fresh.astype(jnp.bfloat16)


def advance(accepted, prev_forget, prev_input, state):
    seqs, values, keys = state.shape
    proposals = prev_forget.shape[1]
    count = 32
    span = pl.BlockSpec((count, values, keys), lambda i: (i, 0, 0))
    return pl.pallas_call(
        advance_kernel,
        grid=(seqs // count,),
        in_specs=[
            pl.BlockSpec((1, seqs), lambda i: (0, 0)),
            pl.BlockSpec((count, proposals, keys), lambda i: (i, 0, 0)),
            pl.BlockSpec((proposals, values, seqs), lambda i: (0, 0, 0)),
            span,
        ],
        out_specs=[span, span],
        out_shape=[shaped(state.shape, jnp.float32), shaped(state.shape, jnp.bfloat16)],
        scratch_shapes=[pltpu.VMEM((keys, seqs), jnp.float32)],
        name="advance",
        cost_estimate=pl.CostEstimate(
            flops=1_000_000_000, bytes_accessed=5 << 20, transcendentals=0
        ),
        compiler_params=pltpu.CompilerParams(vmem_limit_bytes=16 << 20),
    )(accepted[None], prev_forget, prev_input, state)


def split_in_three(value):
    high = value.astype(jnp.bfloat16).astype(jnp.float32)
    middle = (value - high).astype(jnp.bfloat16).astype(jnp.float32)
    return high, middle, value - high - middle


def three_rows(parts, width):
    rest = jnp.zeros((16 - 3 * parts[0].shape[0], width), jnp.float32)
    return jnp.concatenate([*parts, rest], axis=0).astype(jnp.bfloat16)


def source_kernel(tokens, gain, out, columns):
    steps, features, seqs = tokens.shape
    size = gain.shape[1]
    row = 2 * lax.axis_index("zy") + lax.axis_index("core")
    columns[...] = jnp.broadcast_to(gain[pl.ds(row, 1), :], (size, size)).T
    at = pl.multiple_of(lax.axis_index("tp") * features, features)
    scale = columns[pl.ds(at, features), :]
    squares = []
    for t in range(steps):
        wide = tokens[t].astype(jnp.float32)
        squares.append(jnp.sum(wide * wide, axis=0, keepdims=True))
        scaled = (wide * scale).astype(jnp.bfloat16)
        for z in range(out.shape[0]):
            out[z, pl.ds(t * features, features), :] = scaled
    tail = three_rows(split_in_three(jnp.concatenate(squares, axis=0)), seqs)
    for z in range(out.shape[0]):
        out[z, pl.ds(steps * features, 16), :] = tail


def source(tokens, gain, planes):
    steps, features, seqs = tokens.shape
    size = gain.shape[1]
    return call(
        source_kernel,
        shaped((planes, steps * features + 16, seqs), jnp.bfloat16),
        [pltpu.VMEM((size, seqs), jnp.float32)],
        (1_000_000, 1 << 20),
        60 << 20,
        [whole()] * 2,
        whole(),
    )(tokens, gain)


def turn_kernel(w_query, w_forget, w_input, w_gate, keyed, m0, m1, m2, m3, rows, mixed, sems):
    mine = lax.axis_index("tp")
    group, part, size = 4, rows.shape[2], w_query.shape[2]
    at = pl.multiple_of(mine * part, part)
    copies = [
        pltpu.make_async_copy(w_input.at[0], mixed.at[0], sems.at[0]),
        pltpu.make_async_copy(w_gate.at[0], mixed.at[1], sems.at[1]),
        pltpu.make_async_copy(w_query.at[:, pl.ds(at, part), :], rows.at[0], sems.at[2]),
        pltpu.make_async_copy(w_forget.at[:, pl.ds(at, part), :], rows.at[1], sems.at[3]),
    ]
    for copy in copies:
        copy.start()
    copies[0].wait()
    copies[1].wait()
    lane = lax.broadcasted_iota(jnp.int32, (2 * part, size), 1) // part
    for q in range(rows.shape[1] // group):
        to = pl.ds(q * size, size)
        blocks = []
        for k in range(group):
            cut = pl.ds((q * group + k) * size, size)
            both = [mixed[i, :, cut].astype(jnp.float32) for i in range(2)]
            blocks.append(jnp.concatenate(both, axis=0))
        for d, out in enumerate((m0, m1, m2, m3)):
            theirs = (mine ^ d)
            total = None
            for k in range(group):
                turned = pltpu.roll(blocks[k], lax.rem(group + k - theirs, group) * part, 1)
                total = turned if total is None else jnp.where(lane == k, turned, total)
            out[:, to] = total.astype(jnp.bfloat16)
    copies[2].wait()
    copies[3].wait()
    for q in range(rows.shape[1] // group):
        for i in range(2):
            block = rows[i, pl.ds(q * group, group)].astype(jnp.float32).reshape(size, size)
            keyed[pl.ds(i * size, size), pl.ds(q * size, size)] = block.T.astype(jnp.bfloat16)


def turn(w_query, w_forget, w_input, w_gate):
    width, size = w_query.shape
    values = w_input.shape[1]
    far = pl.BlockSpec(memory_space=pltpu.HBM)
    outs = call(
        turn_kernel,
        [shaped((2 * size, width // 4), jnp.bfloat16)]
        + [shaped((2 * values, width // 4), jnp.bfloat16)] * 4,
        [
            pltpu.VMEM((2, width // size, size // 4, size), jnp.bfloat16),
            pltpu.VMEM((2, values, width), jnp.bfloat16),
            pltpu.SemaphoreType.DMA((4,)),
        ],
        (1_000_000_000, 2 << 20),
        60 << 20,
        [far] * 4,
        [whole()] * 5,
    )(
        w_query.reshape(width // size, size, size),
        w_forget.reshape(width // size, size, size),
        w_input,
        w_gate,
    )
    return outs[0], outs[1:]


def outward_kernel(w_out, outward, held, sems):
    cuts, size, span = held.shape
    copies = [
        pltpu.make_async_copy(w_out.at[:, pl.ds(c * span, span)], held.at[c], sems.at[c])
        for c in range(cuts)
    ]
    for copy in copies:
        copy.start()
    for c in range(cuts):
        copies[c].wait()
        for b in range(span // size):
            block = held[c, :, pl.ds(b * size, size)].astype(jnp.float32)
            outward[c * (span // size) + b] = block.T.astype(jnp.bfloat16)


def turn_outward(w_out):
    size, width = w_out.shape
    return call(
        outward_kernel,
        shaped((width // size, size, size), jnp.bfloat16),
        [pltpu.VMEM((4, size, width // 4), jnp.bfloat16), pltpu.SemaphoreType.DMA((4,))],
        (1_000_000_000, 2 << 20),
        16 << 20,
        [pl.BlockSpec(memory_space=pltpu.HBM)],
        whole(),
    )(w_out)


def project_kernel(
    own, other, keyed, w0, w1, w2, w3, o0, o1, o2, o3, held, ready, weights, sems
):
    core, mine = lax.axis_index("core"), lax.axis_index("tp")
    blocks, _, seqs = own.shape
    group, keys, more = 4, keyed.shape[0], w0.shape[0]
    copies = [pltpu.make_async_copy(keyed, weights.at[pl.ds(0, keys), :], sems.at[4])]
    for d, ref in enumerate((w0, w1, w2, w3)):
        at = pl.multiple_of(keys + (mine ^ d) * more, more)
        copies.append(pltpu.make_async_copy(ref, weights.at[pl.ds(at, more), :], sems.at[d]))
    for copy in copies:
        copy.start()
    part = held.shape[0] // (2 * blocks)
    squares = jnp.zeros((16, seqs), jnp.float32)
    for half, ref in ((core, own), (1 - core, other)):
        for b in range(blocks):
            at = pl.multiple_of((2 * b + half) * part, part)
            for t in range(group):
                held[pl.ds(at, part), pl.ds(t * seqs, seqs)] = ref[b, pl.ds(t * part, part), :]
            squares = squares + ref[b, pl.ds(group * part, 16), :].astype(jnp.float32)
    totals = squares[0:4] + squares[4:8] + squares[8:12]
    height = weights.shape[0]
    for t in range(group):
        ready[t, pl.ds(height, 16), :] = three_rows(split_in_three(totals[t : t + 1]), seqs)
    for copy in copies:
        copy.wait()
    both = jnp.dot(weights[...], held[...], preferred_element_type=jnp.float32)
    both = both.astype(jnp.bfloat16)
    for t in range(group):
        ready[t, pl.ds(0, height), :] = both[:, t * seqs : (t + 1) * seqs]
    for d, out in enumerate((o0, o1, o2, o3)):
        out[...] = ready[mine ^ d]


def project(own, other, keyed, weights):
    _, _, seqs = own.shape
    keys, width = keyed.shape
    height = keys + 4 * weights[0].shape[0]
    far = pl.BlockSpec(memory_space=pltpu.HBM)
    return call(
        project_kernel,
        [shaped((height + 16, seqs), jnp.bfloat16)] * 4,
        [
            pltpu.VMEM((width, 4 * seqs), jnp.bfloat16),
            pltpu.VMEM((4, height + 16, seqs), jnp.bfloat16),
            pltpu.VMEM((height, width), jnp.bfloat16),
            pltpu.SemaphoreType.DMA((5,)),
        ],
        (1_000_000_000, 3 << 20),
        16 << 20,
        [whole()] * 2 + [far] * 5,
        [whole()] * 4,
    )(own, other, keyed, *weights)


def finish_kernel(width, p0, p1, p2, p3, o0, o1, o2, o3, gates, held):
    mine = lax.axis_index("tp")
    group = 4
    values = gates.shape[0] // group
    rows, keys = held.shape[0], o0.shape[0] - values
    total = sum(ref[pl.ds(rows, 16), :].astype(jnp.float32) for ref in (p0, p1, p2, p3))
    factor = lax.rsqrt(jnp.sum(total, axis=0, keepdims=True) / width + NORM_EPSILON)
    value = sum(ref[pl.ds(0, rows), :].astype(jnp.float32) for ref in (p0, p1, p2, p3))
    held[...] = (value * factor).astype(jnp.bfloat16)
    for d, out in enumerate((o0, o1, o2, o3)):
        at = pl.multiple_of(keys + (mine ^ d) * 2 * values, 2 * values)
        out[pl.ds(0, keys), :] = held[pl.ds(0, keys), :]
        out[pl.ds(keys, values), :] = held[pl.ds(at, values), :]
    for c in range(group):
        raw = held[pl.ds(keys + c * 2 * values + values, values), :].astype(jnp.float32)
        gates[pl.ds(c * values, values), :] = raw * jax.nn.sigmoid(raw)


def finish(parts, keys, width):
    rows, seqs = parts[0].shape
    rows = rows - 16
    values = (rows - keys) // 8
    outs = call(
        functools.partial(finish_kernel, width),
        [shaped((keys + values, seqs), jnp.bfloat16)] * 4
        + [shaped((4 * values, seqs), jnp.float32)],
        [pltpu.VMEM((rows, seqs), jnp.bfloat16)],
        (100_000_000, 1 << 20),
        16 << 20,
        [whole()] * 4,
        [whole()] * 5,
    )(*parts)
    return outs[:4], outs[4]


def recur_kernel(r0, r1, r2, r3, before, floor, head_gain, o0, o1, o2, o3, seen, ready):
    mine = lax.axis_index("tp")
    size = floor.shape[1]
    values = head_gain.shape[1]
    count = before.shape[0] // values
    steps = 4
    for d, ref in enumerate((r0, r1, r2, r3)):
        seen[mine ^ d] = ref[...]
    low = jnp.broadcast_to(floor[...], (count, size)).T
    scale = jnp.broadcast_to(head_gain[...], (count, values)).T
    forget, keys, fresh, sums, asked = [], [], [], [], []
    for t in range(steps):
        gate = low + (1.0 - low) * jax.nn.sigmoid(seen[t, pl.ds(size, size), :].astype(jnp.float32))
        forget.append(gate)
        keys.append(1.0 - gate)
        fresh.append(seen[t, pl.ds(2 * size, values), :].astype(jnp.float32))
    for t in range(steps):
        moved = seen[t, pl.ds(0, size), :].astype(jnp.float32)
        out = None
        for u in reversed(range(t + 1)):
            score = jnp.sum(moved * keys[u], axis=0, keepdims=True)
            term = score * fresh[u]
            out = term if out is None else out + term
            moved = moved * forget[u]
        sums.append(out)
        asked.append(moved.astype(jnp.bfloat16))
    lane = lax.broadcasted_iota(jnp.int32, (values, count), 1)
    asked = jnp.concatenate(asked, axis=1)
    group = 8
    for b in range(count // group):
        read = jnp.dot(
            before[pl.ds(b * group * values, group * values), :],
            asked,
            preferred_element_type=jnp.float32,
        )
        for s in range(group):
            hit = lane == b * group + s
            for t in range(steps):
                part = read[s * values : (s + 1) * values, t * count : (t + 1) * count]
                sums[t] = sums[t] + jnp.where(hit, part, 0.0)
    for t in range(steps):
        out = sums[t]
        square = jnp.sum(out * out, axis=0, keepdims=True)
        ready[t, pl.ds(0, values), :] = (out * scale).astype(jnp.bfloat16)
        ready[t, pl.ds(values, 16), :] = three_rows(split_in_three(square), count)
    for d, ref in enumerate((o0, o1, o2, o3)):
        ref[...] = ready[mine ^ d]


def recur(received, before, floor, head_gain):
    rows, count = received[0].shape
    values = head_gain.shape[1]
    return call(
        recur_kernel,
        [shaped((values + 16, count), jnp.bfloat16)] * 4,
        [
            pltpu.VMEM((4, rows, count), jnp.bfloat16),
            pltpu.VMEM((4, values + 16, count), jnp.bfloat16),
        ],
        (1_000_000_000, 2 << 20),
        16 << 20,
        [whole()] * 7,
        [whole()] * 4,
    )(*received, before, floor, head_gain)


def gathered(parts, gates, joined):
    mine = lax.axis_index("tp")
    values = joined.shape[0] // 4
    total = None
    for d, ref in enumerate(parts):
        at = pl.multiple_of((mine ^ d) * values, values)
        value = ref[pl.ds(0, values), :].astype(jnp.float32) * gates[pl.ds(at, values), :]
        joined[pl.ds(at, values), :] = value.astype(jnp.bfloat16)
        square = jnp.sum(ref[pl.ds(values, 16), :].astype(jnp.float32), axis=0, keepdims=True)
        total = square if total is None else total + square
    return lax.rsqrt(total / joined.shape[0] + NORM_EPSILON)


def away_kernel(p0, p1, p2, p3, gates, outward, sent, joined):
    core = lax.axis_index("core")
    factor = gathered((p0, p1, p2, p3), gates, joined)
    for b in range(sent.shape[0]):
        part = jnp.dot(outward[2 * b + 1 - core], joined[...], preferred_element_type=jnp.float32)
        sent[b] = (part * factor).astype(jnp.bfloat16)


def keep_kernel(p0, p1, p2, p3, gates, outward, came, kept, joined):
    core = lax.axis_index("core")
    factor = gathered((p0, p1, p2, p3), gates, joined)
    for b in range(kept.shape[0]):
        part = jnp.dot(outward[2 * b + core], joined[...], preferred_element_type=jnp.float32)
        kept[b] = (part * factor + came[b].astype(jnp.float32)).astype(jnp.bfloat16)


def outward_half(kernel, parts, gates, outward, *more):
    blocks, size, _ = outward.shape
    return call(
        kernel,
        shaped((blocks // 2, size, parts[0].shape[1]), jnp.bfloat16),
        [pltpu.VMEM((size, parts[0].shape[1]), jnp.bfloat16)],
        (100_000_000, 2 << 20),
        16 << 20,
        [whole()] * (6 + len(more)),
        whole(),
    )(*parts, gates, outward, *more)


def sum_kernel(parts, out):
    total = parts[0].astype(jnp.float32)
    for b in range(1, parts.shape[0]):
        total = total + parts[b].astype(jnp.float32)
    out[...] = total.astype(out.dtype)


def sums(parts):
    return call(
        sum_kernel,
        shaped(parts.shape[1:], jnp.bfloat16),
        [],
        (1_000_000, 1 << 20),
        8 << 20,
        [whole()],
        whole(),
    )(parts)


def body(
    tokens,
    input_norm_gain,
    w_query,
    w_forget,
    w_input,
    w_gate,
    forget_floor,
    head_gain,
    w_out,
    state,
    prev_forget,
    prev_input,
    accepted,
):
    planes, group = lax.axis_size("zy"), lax.axis_size("tp")
    seqs, proposals, features = tokens.shape
    width, size = w_query.shape
    swap = [(0, 1), (1, 0)]
    hops = [[(i, i ^ d) for i in range(group)] for d in range(group)]

    def passed(parts):
        return [parts[0]] + [lax.ppermute(parts[d], "tp", hops[d]) for d in (1, 2, 3)]

    spread = source(tokens.transpose(1, 2, 0), input_norm_gain.reshape(-1, size), planes)
    own = lax.all_to_all(spread, "zy", 0, 0, tiled=True)
    other = lax.ppermute(own, "core", swap)
    keyed, mixing = turn(w_query, w_forget, w_input, w_gate)
    weights = passed(mixing)
    new_state, rounded = advance(
        accepted,
        prev_forget,
        prev_input.reshape(seqs, proposals, -1).transpose(1, 2, 0),
        state[:, 0],
    )

    partial = passed(project(own, other, keyed, weights))
    sends, opened = finish(partial, 2 * size, width)
    received = passed(sends)
    outward = turn_outward(w_out)
    shown = recur(received, rounded.reshape(-1, size), forget_floor[None], head_gain[None])
    parts = passed(shown)
    sent = outward_half(away_kernel, parts, opened, outward)
    came = lax.ppermute(sent, "core", swap)
    kept = outward_half(keep_kernel, parts, opened, outward, came)
    terms = lax.all_to_all(
        kept.reshape(planes * group, features, seqs), ("zy", "tp"), 0, 0, tiled=True
    )
    mixed = sums(terms.reshape(planes, group, features, seqs))
    return mixed.transpose(2, 0, 1), new_state[:, None]


def solution(mesh):
    kv, tp = mesh.shape["kv"], mesh.shape["tp"]
    finer = Mesh(mesh.devices.reshape(kv // 2, 2, tp), ("zy", "core", "tp"))
    rows = ("zy", "core")
    placed = (
        P(None, None, (*rows, "tp")),
        P(),
        P(None, rows),
        P(None, rows),
        P(rows, "tp", None),
        P(rows, "tp", None),
        P(rows),
        P("tp"),
        P(rows, None),
        P(None, rows, "tp", None),
        P(None, None, rows),
        P(None, None, rows, "tp"),
        P(),
    )

    return jax.shard_map(
        body,
        mesh=finer,
        in_specs=placed,
        out_specs=(P(None, None, (*rows, "tp")), P(None, rows, "tp", None)),
        check_vma=False,
    )
```

```python
import jax
import jax.numpy as jnp
from jax import lax
from jax.experimental import pallas as pl
from jax.experimental.pallas import tpu as pltpu
from jax.sharding import Mesh, PartitionSpec as P


NORM_EPSILON = 1e-06


def whole():
    return pl.BlockSpec(memory_space=pltpu.VMEM)


def shaped(shape, dtype):
    return jax.ShapeDtypeStruct(shape, dtype)


def call(kernel, out_shape, scratch, cost, limit, in_specs, out_specs):
    return pl.pallas_call(
        kernel,
        out_shape=out_shape,
        in_specs=in_specs,
        out_specs=out_specs,
        scratch_shapes=scratch,
        cost_estimate=pl.CostEstimate(flops=cost[0], bytes_accessed=cost[1], transcendentals=0),
        compiler_params=pltpu.CompilerParams(vmem_limit_bytes=limit),
    )


def advance_kernel(accepted, prev_forget, prev_input, state, new_state, rounded, live):
    block = pl.program_id(0)
    count, proposals, size = prev_forget.shape
    lanes = prev_input.shape[2]

    @pl.when(block == 0)
    def _():
        live[...] = jnp.broadcast_to(accepted[...].astype(jnp.float32), (size, lanes)).T

    shift = lax.rem(lanes - block * count, lanes)
    values = [
        pltpu.roll(prev_input[p].astype(jnp.float32), shift, 1) for p in range(proposals)
    ]
    taken = live[pl.ds(pl.multiple_of(block * count, count), count), :]
    rest = jnp.ones((count, size), jnp.float32)
    terms = [None] * proposals
    for p in reversed(range(proposals)):
        gate = jnp.where(taken > p, prev_forget[:, p, :], 1.0)
        terms[p] = rest * (1.0 - gate)
        rest = rest * gate
    for s in range(count):
        fresh = rest[s : s + 1] * state[s]
        for p in range(proposals):
            fresh = fresh + terms[p][s : s + 1] * values[p][:, s : s + 1]
        new_state[s] = fresh
        rounded[s] = fresh.astype(jnp.bfloat16)


def advance(accepted, prev_forget, prev_input, state):
    seqs, values, keys = state.shape
    proposals = prev_forget.shape[1]
    count = 32
    span = pl.BlockSpec((count, values, keys), lambda i: (i, 0, 0))
    return pl.pallas_call(
        advance_kernel,
        grid=(seqs // count,),
        in_specs=[
            pl.BlockSpec((1, seqs), lambda i: (0, 0)),
            pl.BlockSpec((count, proposals, keys), lambda i: (i, 0, 0)),
            pl.BlockSpec((proposals, values, seqs), lambda i: (0, 0, 0)),
            span,
        ],
        out_specs=[span, span],
        out_shape=[shaped(state.shape, jnp.float32), shaped(state.shape, jnp.bfloat16)],
        scratch_shapes=[pltpu.VMEM((keys, seqs), jnp.float32)],
        name="advance",
        cost_estimate=pl.CostEstimate(
            flops=1_000_000_000, bytes_accessed=5 << 20, transcendentals=0
        ),
        compiler_params=pltpu.CompilerParams(vmem_limit_bytes=16 << 20),
    )(accepted[None], prev_forget, prev_input, state)


def split_in_three(value):
    high = value.astype(jnp.bfloat16).astype(jnp.float32)
    middle = (value - high).astype(jnp.bfloat16).astype(jnp.float32)
    return high, middle, value - high - middle


def three_rows(parts, width):
    rest = jnp.zeros((16 - 3 * parts[0].shape[0], width), jnp.float32)
    return jnp.concatenate([*parts, rest], axis=0).astype(jnp.bfloat16)


def source_kernel(tokens, gain, w_input, w_gate, out, both, inputs, gates):
    steps = tokens.shape[0]
    for z in range(out.shape[0] // steps):
        out[pl.ds(z * steps, steps)] = tokens[...]
    size = gain.shape[1]
    for b in range(gain.shape[0]):
        at = pl.ds(b * size, size)
        for i, weight in enumerate((w_input, w_gate)):
            value = weight[0, :, at].astype(jnp.float32) * gain[pl.ds(b, 1), :]
            value = value.astype(jnp.bfloat16)
            both[i, :, at] = value
            (inputs, gates)[i][0, :, at] = value


def source(tokens, gain, w_input, w_gate, planes):
    steps, features, seqs = tokens.shape
    return call(
        source_kernel,
        [
            shaped((planes * steps, features, seqs), jnp.bfloat16),
            shaped((2, *w_input.shape[1:]), jnp.bfloat16),
            shaped(w_input.shape, jnp.bfloat16),
            shaped(w_gate.shape, jnp.bfloat16),
        ],
        [],
        (1_000_000, 1 << 20),
        60 << 20,
        [whole()] * 4,
        [whole()] * 4,
    )(tokens, gain, w_input, w_gate)


def turn_kernel(gain, w_query, w_forget, keyed):
    size = gain.shape[1]
    for b in range(w_query.shape[0] // size):
        at = pl.ds(b * size, size)
        row = gain[pl.ds(b, 1), :]
        for i, weight in enumerate((w_query, w_forget)):
            block = weight[at, :].astype(jnp.float32).T
            keyed[pl.ds(i * size, size), at] = (block * row).astype(jnp.bfloat16)


def turn(gain, w_query, w_forget):
    width, size = w_query.shape
    return call(
        turn_kernel,
        shaped((2 * size, width), jnp.bfloat16),
        [],
        (1_000_000_000, 4 << 20),
        16 << 20,
        [whole()] * 3,
        whole(),
    )(gain, w_query, w_forget)


def bring(which, weights, held, sems):
    copies = [
        pltpu.make_async_copy(ref.at[which if ref.shape[0] > 1 else 0], held.at[d], sems.at[d])
        for d, ref in enumerate(weights)
    ]
    for copy in copies:
        copy.start()
    return copies


def collect_kernel(w0, w1, w2, w3, out, sems):
    values = w0.shape[1]
    copies = [
        pltpu.make_async_copy(ref.at[0], out.at[pl.ds(d * values, values), :], sems.at[d])
        for d, ref in enumerate((w0, w1, w2, w3))
    ]
    for copy in copies:
        copy.start()
    for copy in copies:
        copy.wait()


def collect(weights):
    _, values, width = weights[0].shape
    return call(
        collect_kernel,
        shaped((4 * values, width), jnp.bfloat16),
        [pltpu.SemaphoreType.DMA((4,))],
        (1_000_000_000, 2 << 20),
        16 << 20,
        [pl.BlockSpec(memory_space=pltpu.HBM)] * 4,
        whole(),
    )(*weights)


def project_kernel(own, other, keyed, mixing, o0, o1, o2, o3, held, scale):
    core = lax.axis_index("core")
    blocks, size, seqs = own.shape
    squares = jnp.zeros((8, seqs), jnp.float32)
    for half, ref in ((core, own), (1 - core, other)):
        for b in range(blocks):
            part = ref[b]
            held[pl.ds(pl.multiple_of((2 * b + half) * size, size), size), :] = part
            wide = part.astype(jnp.float32)
            squares = squares + jnp.sum((wide * wide).reshape(size // 8, 8, seqs), axis=0)
    total = jnp.sum(squares, axis=0, keepdims=True)
    factor = lax.rsqrt(total / (2 * blocks * size) + NORM_EPSILON)
    scale[...] = jnp.broadcast_to(factor, scale.shape)
    rows = held[...]
    first = jnp.dot(keyed[...], rows, preferred_element_type=jnp.float32) * factor
    first = first.astype(jnp.bfloat16)
    second = jnp.dot(mixing[...], rows, preferred_element_type=jnp.float32) * factor
    second = second.astype(jnp.bfloat16)
    keys, values = first.shape[0], second.shape[0] // 4
    for d, out in enumerate((o0, o1, o2, o3)):
        out[pl.ds(0, keys), :] = first
        out[pl.ds(keys, values), :] = second[d * values : (d + 1) * values]


def project(own, other, keyed, mixing):
    blocks, size, seqs = own.shape
    rows = keyed.shape[0] + mixing.shape[0] // 4
    outs = call(
        project_kernel,
        [shaped((rows, seqs), jnp.bfloat16)] * 4
        + [shaped((2 * blocks * size, seqs), jnp.bfloat16), shaped((8, seqs), jnp.float32)],
        [],
        (1_000_000_000, 3 << 20),
        16 << 20,
        [whole()] * 4,
        [whole()] * 6,
    )(own, other, keyed, mixing)
    return outs[:4], outs[4], outs[5]


def gate_kernel(w0, w1, w2, w3, rows, scale, out, mixing, sems):
    for copy in bring(1, (w0, w1, w2, w3), mixing, sems):
        copy.wait()
    group, values, width = mixing.shape
    mixed = mixing[...].reshape(group * values, width)
    raw = jnp.dot(mixed, rows[...], preferred_element_type=jnp.float32) * scale[0:1]
    raw = raw.astype(jnp.bfloat16).astype(jnp.float32)
    out[...] = raw * jax.nn.sigmoid(raw)


def gate(weights, rows, scale):
    _, values, width = weights[0].shape
    return call(
        gate_kernel,
        shaped((4 * values, rows.shape[1]), jnp.float32),
        [pltpu.VMEM((4, values, width), jnp.bfloat16), pltpu.SemaphoreType.DMA((4,))],
        (1_000_000_000, 3 << 20),
        16 << 20,
        [pl.BlockSpec(memory_space=pltpu.HBM)] * 4 + [whole()] * 2,
        whole(),
    )(*weights, rows, scale)


def outward_kernel(w_out, outward, held, sems):
    cuts, size, span = held.shape
    copies = [
        pltpu.make_async_copy(w_out.at[:, pl.ds(c * span, span)], held.at[c], sems.at[c])
        for c in range(cuts)
    ]
    for copy in copies:
        copy.start()
    for c in range(cuts):
        copies[c].wait()
        for b in range(span // size):
            block = held[c, :, pl.ds(b * size, size)].astype(jnp.float32)
            outward[c * (span // size) + b] = block.T.astype(jnp.bfloat16)


def turn_outward(w_out):
    size, width = w_out.shape
    return call(
        outward_kernel,
        shaped((width // size, size, size), jnp.bfloat16),
        [pltpu.VMEM((4, size, width // 4), jnp.bfloat16), pltpu.SemaphoreType.DMA((4,))],
        (1_000_000_000, 2 << 20),
        60 << 20,
        [pl.BlockSpec(memory_space=pltpu.HBM)],
        whole(),
    )(w_out)


def recur_kernel(r0, r1, r2, r3, before, floor, head_gain, o0, o1, o2, o3, seen, ready):
    mine = lax.axis_index("tp")
    size = floor.shape[1]
    values = head_gain.shape[1]
    count = before.shape[0] // values
    steps = 4
    for d, ref in enumerate((r0, r1, r2, r3)):
        seen[mine ^ d] = ref[...]
    low = jnp.broadcast_to(floor[...], (count, size)).T
    scale = jnp.broadcast_to(head_gain[...], (count, values)).T
    forget, keys, fresh, sums, asked = [], [], [], [], []
    for t in range(steps):
        gate = low + (1.0 - low) * jax.nn.sigmoid(seen[t, pl.ds(size, size), :].astype(jnp.float32))
        forget.append(gate)
        keys.append(1.0 - gate)
        fresh.append(seen[t, pl.ds(2 * size, values), :].astype(jnp.float32))
    for t in range(steps):
        moved = seen[t, pl.ds(0, size), :].astype(jnp.float32)
        out = None
        for u in reversed(range(t + 1)):
            score = jnp.sum(moved * keys[u], axis=0, keepdims=True)
            term = score * fresh[u]
            out = term if out is None else out + term
            moved = moved * forget[u]
        sums.append(out)
        asked.append(moved.astype(jnp.bfloat16))
    lane = lax.broadcasted_iota(jnp.int32, (values, count), 1)
    asked = jnp.concatenate(asked, axis=1)
    group = 8
    for b in range(count // group):
        read = jnp.dot(
            before[pl.ds(b * group * values, group * values), :],
            asked,
            preferred_element_type=jnp.float32,
        )
        for s in range(group):
            hit = lane == b * group + s
            for t in range(steps):
                part = read[s * values : (s + 1) * values, t * count : (t + 1) * count]
                sums[t] = sums[t] + jnp.where(hit, part, 0.0)
    for t in range(steps):
        out = sums[t]
        square = jnp.sum(out * out, axis=0, keepdims=True)
        ready[t, pl.ds(0, values), :] = (out * scale).astype(jnp.bfloat16)
        ready[t, pl.ds(values, 16), :] = three_rows(split_in_three(square), count)
    for d, ref in enumerate((o0, o1, o2, o3)):
        ref[...] = ready[mine ^ d]


def recur(received, before, floor, head_gain):
    rows, count = received[0].shape
    values = head_gain.shape[1]
    return call(
        recur_kernel,
        [shaped((values + 16, count), jnp.bfloat16)] * 4,
        [
            pltpu.VMEM((4, rows, count), jnp.bfloat16),
            pltpu.VMEM((4, values + 16, count), jnp.bfloat16),
        ],
        (1_000_000_000, 2 << 20),
        16 << 20,
        [whole()] * 7,
        [whole()] * 4,
    )(*received, before, floor, head_gain)


def gathered(parts, gates, joined):
    mine = lax.axis_index("tp")
    values = joined.shape[0] // 4
    total = None
    for d, ref in enumerate(parts):
        at = pl.multiple_of((mine ^ d) * values, values)
        value = ref[pl.ds(0, values), :].astype(jnp.float32) * gates[pl.ds(d * values, values), :]
        joined[pl.ds(at, values), :] = value.astype(jnp.bfloat16)
        square = jnp.sum(ref[pl.ds(values, 16), :].astype(jnp.float32), axis=0, keepdims=True)
        total = square if total is None else total + square
    return lax.rsqrt(total / joined.shape[0] + NORM_EPSILON)


def away_kernel(p0, p1, p2, p3, gates, outward, sent, joined):
    core = lax.axis_index("core")
    factor = gathered((p0, p1, p2, p3), gates, joined)
    for b in range(sent.shape[0]):
        part = jnp.dot(outward[2 * b + 1 - core], joined[...], preferred_element_type=jnp.float32)
        sent[b] = (part * factor).astype(jnp.bfloat16)


def keep_kernel(p0, p1, p2, p3, gates, outward, came, kept, joined):
    core = lax.axis_index("core")
    factor = gathered((p0, p1, p2, p3), gates, joined)
    for b in range(kept.shape[0]):
        part = jnp.dot(outward[2 * b + core], joined[...], preferred_element_type=jnp.float32)
        kept[b] = (part * factor + came[b].astype(jnp.float32)).astype(jnp.bfloat16)


def outward_half(kernel, parts, gates, outward, *more):
    blocks, size, _ = outward.shape
    return call(
        kernel,
        shaped((blocks // 2, size, parts[0].shape[1]), jnp.bfloat16),
        [pltpu.VMEM((size, parts[0].shape[1]), jnp.bfloat16)],
        (100_000_000, 2 << 20),
        16 << 20,
        [whole()] * (6 + len(more)),
        whole(),
    )(*parts, gates, outward, *more)


def sum_kernel(parts, out):
    total = parts[0].astype(jnp.float32)
    for b in range(1, parts.shape[0]):
        total = total + parts[b].astype(jnp.float32)
    out[...] = total.astype(out.dtype)


def sums(parts):
    return call(
        sum_kernel,
        shaped(parts.shape[1:], jnp.bfloat16),
        [],
        (1_000_000, 1 << 20),
        8 << 20,
        [whole()],
        whole(),
    )(parts)


def body(
    tokens,
    input_norm_gain,
    w_query,
    w_forget,
    w_input,
    w_gate,
    forget_floor,
    head_gain,
    w_out,
    state,
    prev_forget,
    prev_input,
    accepted,
):
    planes, group = lax.axis_size("zy"), lax.axis_size("tp")
    seqs, proposals, features = tokens.shape
    _, size = w_query.shape
    swap = [(0, 1), (1, 0)]
    hops = [[(i, i ^ d) for i in range(group)] for d in range(group)]

    def passed(parts):
        return [parts[0]] + [lax.ppermute(parts[d], "tp", hops[d]) for d in (1, 2, 3)]

    gain = input_norm_gain.reshape(-1, size)
    spread, both, own_input, own_gate = source(tokens.transpose(1, 2, 0), gain, w_input, w_gate, planes)
    far = lax.ppermute(both, "tp", hops[2])
    own = lax.all_to_all(spread, ("zy", "tp"), 0, 0, tiled=True)
    own = own.reshape(planes, group * features, seqs)
    other = lax.ppermute(own, "core", swap)
    near = [lax.ppermute(own_input, "tp", hops[d]) for d in (1, 3)]
    inputs = [own_input, near[0], far, near[1]]
    near = [lax.ppermute(own_gate, "tp", hops[d]) for d in (1, 3)]
    gates = [own_gate, near[0], far, near[1]]
    keyed = turn(gain, w_query, w_forget)
    mixing = collect(inputs)
    new_state, rounded = advance(
        accepted,
        prev_forget,
        prev_input.reshape(seqs, proposals, -1).transpose(1, 2, 0),
        state[:, 0],
    )

    sends, rows, scale = project(own, other, keyed, mixing)
    received = passed(sends)
    shown = recur(received, rounded.reshape(-1, size), forget_floor[None], head_gain[None])
    parts = passed(shown)
    outward = turn_outward(w_out)
    opened = gate(gates, rows, scale)
    sent = outward_half(away_kernel, parts, opened, outward)
    came = lax.ppermute(sent, "core", swap)
    kept = outward_half(keep_kernel, parts, opened, outward, came)
    terms = lax.all_to_all(
        kept.reshape(planes * group, features, seqs), ("zy", "tp"), 0, 0, tiled=True
    )
    mixed = sums(terms.reshape(planes, group, features, seqs))
    return mixed.transpose(2, 0, 1), new_state[:, None]


def solution(mesh):
    kv, tp = mesh.shape["kv"], mesh.shape["tp"]
    finer = Mesh(mesh.devices.reshape(kv // 2, 2, tp), ("zy", "core", "tp"))
    rows = ("zy", "core")
    placed = (
        P(None, None, (*rows, "tp")),
        P(),
        P(None, rows),
        P(None, rows),
        P(rows, "tp", None),
        P(rows, "tp", None),
        P(rows),
        P("tp"),
        P(rows, None),
        P(None, rows, "tp", None),
        P(None, None, rows),
        P(None, None, rows, "tp"),
        P(),
    )

    return jax.shard_map(
        body,
        mesh=finer,
        in_specs=placed,
        out_specs=(P(None, None, (*rows, "tp")), P(None, rows, "tp", None)),
        check_vma=False,
    )
```

```python
import jax
import jax.numpy as jnp
from jax import lax
from jax.experimental import pallas as pl
from jax.experimental.pallas import tpu as pltpu
from jax.sharding import Mesh, PartitionSpec as P


NORM_EPSILON = 1e-06


def whole():
    return pl.BlockSpec(memory_space=pltpu.VMEM)


def shaped(shape, dtype):
    return jax.ShapeDtypeStruct(shape, dtype)


def call(kernel, out_shape, scratch, cost, limit, in_specs, out_specs):
    return pl.pallas_call(
        kernel,
        out_shape=out_shape,
        in_specs=in_specs,
        out_specs=out_specs,
        scratch_shapes=scratch,
        cost_estimate=pl.CostEstimate(flops=cost[0], bytes_accessed=cost[1], transcendentals=0),
        compiler_params=pltpu.CompilerParams(vmem_limit_bytes=limit),
    )


def advance_kernel(accepted, prev_forget, prev_input, state, new_state, rounded, live):
    block = pl.program_id(0)
    count, proposals, size = prev_forget.shape
    lanes = prev_input.shape[2]

    @pl.when(block == 0)
    def _():
        live[...] = jnp.broadcast_to(accepted[...].astype(jnp.float32), (size, lanes)).T

    shift = lax.rem(lanes - block * count, lanes)
    values = [
        pltpu.roll(prev_input[p].astype(jnp.float32), shift, 1) for p in range(proposals)
    ]
    taken = live[pl.ds(pl.multiple_of(block * count, count), count), :]
    rest = jnp.ones((count, size), jnp.float32)
    terms = [None] * proposals
    for p in reversed(range(proposals)):
        gate = jnp.where(taken > p, prev_forget[:, p, :], 1.0)
        terms[p] = rest * (1.0 - gate)
        rest = rest * gate
    for s in range(count):
        fresh = rest[s : s + 1] * state[s]
        for p in range(proposals):
            fresh = fresh + terms[p][s : s + 1] * values[p][:, s : s + 1]
        new_state[s] = fresh
        rounded[s] = fresh.astype(jnp.bfloat16)


def advance(accepted, prev_forget, prev_input, state):
    seqs, values, keys = state.shape
    proposals = prev_forget.shape[1]
    count = 32
    span = pl.BlockSpec((count, values, keys), lambda i: (i, 0, 0))
    return pl.pallas_call(
        advance_kernel,
        grid=(seqs // count,),
        in_specs=[
            pl.BlockSpec((1, seqs), lambda i: (0, 0)),
            pl.BlockSpec((count, proposals, keys), lambda i: (i, 0, 0)),
            pl.BlockSpec((proposals, values, seqs), lambda i: (0, 0, 0)),
            span,
        ],
        out_specs=[span, span],
        out_shape=[shaped(state.shape, jnp.float32), shaped(state.shape, jnp.bfloat16)],
        scratch_shapes=[pltpu.VMEM((keys, seqs), jnp.float32)],
        name="advance",
        cost_estimate=pl.CostEstimate(
            flops=1_000_000_000, bytes_accessed=5 << 20, transcendentals=0
        ),
        compiler_params=pltpu.CompilerParams(vmem_limit_bytes=16 << 20),
    )(accepted[None], prev_forget, prev_input, state)


def split_in_three(value):
    high = value.astype(jnp.bfloat16).astype(jnp.float32)
    middle = (value - high).astype(jnp.bfloat16).astype(jnp.float32)
    return high, middle, value - high - middle


def three_rows(parts, width):
    rest = jnp.zeros((16 - 3 * parts[0].shape[0], width), jnp.float32)
    return jnp.concatenate([*parts, rest], axis=0).astype(jnp.bfloat16)


def source_kernel(tokens, out, held, sems):
    steps = tokens.shape[0]
    planes = out.shape[0] // steps
    copy = pltpu.make_async_copy(tokens, held, sems.at[planes])
    copy.start()
    copy.wait()
    copies = [
        pltpu.make_async_copy(held, out.at[pl.ds(z * steps, steps)], sems.at[z])
        for z in range(planes)
    ]
    for copy in copies:
        copy.start()
    for copy in copies:
        copy.wait()


def source(tokens, planes):
    steps, features, seqs = tokens.shape
    far = pl.BlockSpec(memory_space=pltpu.HBM)
    return call(
        source_kernel,
        shaped((planes * steps, features, seqs), jnp.bfloat16),
        [pltpu.VMEM(tokens.shape, jnp.bfloat16), pltpu.SemaphoreType.DMA((planes + 1,))],
        (1_000_000, 1 << 20),
        60 << 20,
        [far],
        far,
    )(tokens)


def turn_kernel(gain, w_query, w_forget, keyed):
    size = gain.shape[1]
    for b in range(w_query.shape[0] // size):
        at = pl.ds(b * size, size)
        row = gain[pl.ds(b, 1), :]
        for i, weight in enumerate((w_query, w_forget)):
            block = weight[at, :].astype(jnp.float32).T
            keyed[pl.ds(i * size, size), at] = (block * row).astype(jnp.bfloat16)


def turn(gain, w_query, w_forget):
    width, size = w_query.shape
    return call(
        turn_kernel,
        shaped((2 * size, width), jnp.bfloat16),
        [],
        (1_000_000_000, 4 << 20),
        16 << 20,
        [whole()] * 3,
        whole(),
    )(gain, w_query, w_forget)


def fold_kernel(gain, w0, w1, w2, w3, out):
    values, size = w0.shape[1], gain.shape[1]
    for b in range(gain.shape[0]):
        at = pl.ds(b * size, size)
        for d, weight in enumerate((w0, w1, w2, w3)):
            value = weight[0, :, at].astype(jnp.float32) * gain[pl.ds(b, 1), :]
            out[pl.ds(d * values, values), at] = value.astype(jnp.bfloat16)


def fold(gain, weights):
    _, values, width = weights[0].shape
    return call(
        fold_kernel,
        shaped((4 * values, width), jnp.bfloat16),
        [],
        (1_000_000_000, 2 << 20),
        16 << 20,
        [whole()] * 5,
        whole(),
    )(gain, *weights)


def project_kernel(own, other, keyed, mixing, o0, o1, o2, o3, held, scale):
    core = lax.axis_index("core")
    blocks, size, seqs = own.shape
    squares = jnp.zeros((8, seqs), jnp.float32)
    for half, ref in ((core, own), (1 - core, other)):
        for b in range(blocks):
            part = ref[b]
            held[pl.ds(pl.multiple_of((2 * b + half) * size, size), size), :] = part
            wide = part.astype(jnp.float32)
            squares = squares + jnp.sum((wide * wide).reshape(size // 8, 8, seqs), axis=0)
    total = jnp.sum(squares, axis=0, keepdims=True)
    factor = lax.rsqrt(total / (2 * blocks * size) + NORM_EPSILON)
    scale[...] = jnp.broadcast_to(factor, scale.shape)
    rows = held[...]
    first = jnp.dot(keyed[...], rows, preferred_element_type=jnp.float32) * factor
    first = first.astype(jnp.bfloat16)
    second = jnp.dot(mixing[...], rows, preferred_element_type=jnp.float32) * factor
    second = second.astype(jnp.bfloat16)
    keys, values = first.shape[0], second.shape[0] // 4
    for d, out in enumerate((o0, o1, o2, o3)):
        out[pl.ds(0, keys), :] = first
        out[pl.ds(keys, values), :] = second[d * values : (d + 1) * values]


def project(own, other, keyed, mixing):
    blocks, size, seqs = own.shape
    rows = keyed.shape[0] + mixing.shape[0] // 4
    outs = call(
        project_kernel,
        [shaped((rows, seqs), jnp.bfloat16)] * 4
        + [shaped((2 * blocks * size, seqs), jnp.bfloat16), shaped((8, seqs), jnp.float32)],
        [],
        (1_000_000_000, 3 << 20),
        16 << 20,
        [whole()] * 4,
        [whole()] * 6,
    )(own, other, keyed, mixing)
    return outs[:4], outs[4], outs[5]


def gate_kernel(gain, w0, w1, w2, w3, rows, scale, out, held):
    values, size = w0.shape[1], gain.shape[1]
    for b in range(gain.shape[0]):
        at = pl.ds(b * size, size)
        for d, weight in enumerate((w0, w1, w2, w3)):
            value = weight[0, :, at].astype(jnp.float32) * gain[pl.ds(b, 1), :]
            held[pl.ds(d * values, values), at] = value.astype(jnp.bfloat16)
    raw = jnp.dot(held[...], rows[...], preferred_element_type=jnp.float32) * scale[0:1]
    raw = raw.astype(jnp.bfloat16).astype(jnp.float32)
    out[...] = raw * jax.nn.sigmoid(raw)


def gate(gain, weights, rows, scale):
    _, values, width = weights[0].shape
    return call(
        gate_kernel,
        shaped((4 * values, rows.shape[1]), jnp.float32),
        [pltpu.VMEM((4 * values, width), jnp.bfloat16)],
        (1_000_000_000, 3 << 20),
        16 << 20,
        [whole()] * 7,
        whole(),
    )(gain, *weights, rows, scale)


def outward_kernel(w_out, mine, theirs, held, sems):
    core = lax.axis_index("core")
    cuts, size, span = held.shape
    copies = [
        pltpu.make_async_copy(w_out.at[:, pl.ds(c * span, span)], held.at[c], sems.at[c])
        for c in range(cuts)
    ]
    for copy in copies:
        copy.start()
    pairs = span // size // 2
    for c in range(cuts):
        copies[c].wait()
        for b in range(pairs):
            for half, out in ((core, mine), (1 - core, theirs)):
                at = pl.multiple_of((2 * b + half) * size, size)
                block = held[c, :, pl.ds(at, size)].astype(jnp.float32)
                out[c * pairs + b] = block.T.astype(jnp.bfloat16)


def turn_outward(w_out):
    size, width = w_out.shape
    return call(
        outward_kernel,
        [shaped((width // size // 2, size, size), jnp.bfloat16)] * 2,
        [pltpu.VMEM((4, size, width // 4), jnp.bfloat16), pltpu.SemaphoreType.DMA((4,))],
        (1_000_000_000, 2 << 20),
        16 << 20,
        [pl.BlockSpec(memory_space=pltpu.HBM)],
        [whole()] * 2,
    )(w_out)


def recur_kernel(r0, r1, r2, r3, before, floor, head_gain, o0, o1, o2, o3, seen, ready):
    mine = lax.axis_index("tp")
    size = floor.shape[1]
    values = head_gain.shape[1]
    count = before.shape[0] // values
    steps = 4
    for d, ref in enumerate((r0, r1, r2, r3)):
        seen[mine ^ d] = ref[...]
    low = jnp.broadcast_to(floor[...], (count, size)).T
    scale = jnp.broadcast_to(head_gain[...], (count, values)).T
    forget, keys, fresh, sums, asked = [], [], [], [], []
    for t in range(steps):
        gate = low + (1.0 - low) * jax.nn.sigmoid(seen[t, pl.ds(size, size), :].astype(jnp.float32))
        forget.append(gate)
        keys.append(1.0 - gate)
        fresh.append(seen[t, pl.ds(2 * size, values), :].astype(jnp.float32))
    for t in range(steps):
        moved = seen[t, pl.ds(0, size), :].astype(jnp.float32)
        out = None
        for u in reversed(range(t + 1)):
            score = jnp.sum(moved * keys[u], axis=0, keepdims=True)
            term = score * fresh[u]
            out = term if out is None else out + term
            moved = moved * forget[u]
        sums.append(out)
        asked.append(moved.astype(jnp.bfloat16))
    half = count // 2
    lane = lax.rem(lax.broadcasted_iota(jnp.int32, (values, steps * half), 1), half)
    group = 8
    halves = []
    for h in range(2):
        wanted = jnp.concatenate([a[:, h * half : (h + 1) * half] for a in asked], axis=1)
        total = jnp.zeros((values, steps * half), jnp.float32)
        for b in range(half // group):
            first = h * half + b * group
            read = jnp.dot(
                before[pl.ds(first * values, group * values), :],
                wanted,
                preferred_element_type=jnp.float32,
            )
            for s in range(group):
                part = read[s * values : (s + 1) * values]
                total = total + jnp.where(lane == b * group + s, part, 0.0)
        halves.append(total)
    for t in range(steps):
        cut = [total[:, t * half : (t + 1) * half] for total in halves]
        sums[t] = sums[t] + jnp.concatenate(cut, axis=1)
    for t in range(steps):
        out = sums[t]
        square = jnp.sum(out * out, axis=0, keepdims=True)
        ready[t, pl.ds(0, values), :] = (out * scale).astype(jnp.bfloat16)
        ready[t, pl.ds(values, 16), :] = three_rows(split_in_three(square), count)
    for d, ref in enumerate((o0, o1, o2, o3)):
        ref[...] = ready[mine ^ d]


def recur(received, before, floor, head_gain):
    rows, count = received[0].shape
    values = head_gain.shape[1]
    return call(
        recur_kernel,
        [shaped((values + 16, count), jnp.bfloat16)] * 4,
        [
            pltpu.VMEM((4, rows, count), jnp.bfloat16),
            pltpu.VMEM((4, values + 16, count), jnp.bfloat16),
        ],
        (1_000_000_000, 2 << 20),
        16 << 20,
        [whole()] * 7,
        [whole()] * 4,
    )(*received, before, floor, head_gain)


def hide_kernel(p0, p1, p2, p3, gates, hidden):
    mine = lax.axis_index("tp")
    values = hidden.shape[0] // 4
    parts = (p0, p1, p2, p3)
    total = None
    for ref in parts:
        square = jnp.sum(ref[pl.ds(values, 16), :].astype(jnp.float32), axis=0, keepdims=True)
        total = square if total is None else total + square
    factor = lax.rsqrt(total / hidden.shape[0] + NORM_EPSILON)
    for d, ref in enumerate(parts):
        at = pl.multiple_of((mine ^ d) * values, values)
        value = ref[pl.ds(0, values), :].astype(jnp.float32) * factor
        value = value * gates[pl.ds(d * values, values), :]
        hidden[pl.ds(at, values), :] = value.astype(jnp.bfloat16)


def hide(parts, gates):
    return call(
        hide_kernel,
        shaped(gates.shape, jnp.bfloat16),
        [],
        (1_000_000, 1 << 18),
        16 << 20,
        [whole()] * 5,
        whole(),
    )(*parts, gates)


def emit_kernel(hidden, other, ours, theirs, out):
    for b in range(out.shape[0]):
        part = jnp.dot(ours[b], hidden[...], preferred_element_type=jnp.float32)
        part = part + jnp.dot(theirs[b], other[...], preferred_element_type=jnp.float32)
        out[b] = part.astype(jnp.bfloat16)


def emit(hidden, other, ours, theirs):
    blocks, size, _ = ours.shape
    return call(
        emit_kernel,
        shaped((blocks, size, hidden.shape[1]), jnp.bfloat16),
        [],
        (100_000_000, 2 << 20),
        16 << 20,
        [whole()] * 4,
        whole(),
    )(hidden, other, ours, theirs)


def sum_kernel(parts, out):
    total = parts[0].astype(jnp.float32)
    for b in range(1, parts.shape[0]):
        total = total + parts[b].astype(jnp.float32)
    out[...] = total.astype(out.dtype)


def sums(parts):
    return call(
        sum_kernel,
        shaped(parts.shape[1:], jnp.bfloat16),
        [],
        (1_000_000, 1 << 20),
        8 << 20,
        [whole()],
        whole(),
    )(parts)


def body(
    tokens,
    input_norm_gain,
    w_query,
    w_forget,
    w_input,
    w_gate,
    forget_floor,
    head_gain,
    w_out,
    state,
    prev_forget,
    prev_input,
    accepted,
):
    planes, group = lax.axis_size("zy"), lax.axis_size("tp")
    seqs, proposals, features = tokens.shape
    _, size = w_query.shape
    swap = [(0, 1), (1, 0)]
    hops = [[(i, i ^ d) for i in range(group)] for d in range(group)]

    def passed(parts):
        far = lax.ppermute(parts[2], "tp", hops[2])
        near = [lax.ppermute(parts[d], "tp", hops[d]) for d in (1, 3)]
        return [parts[0], near[0], far, near[1]]

    gain = input_norm_gain.reshape(-1, size)
    inputs = passed([w_input] * group)
    own = lax.all_to_all(source(tokens.transpose(1, 2, 0), planes), ("zy", "tp"), 0, 0, tiled=True)
    own = own.reshape(planes, group * features, seqs)
    other = lax.ppermute(own, "core", swap)
    gates = passed([w_gate] * group)
    keyed = turn(gain, w_query, w_forget)
    mixing = fold(gain, inputs)
    new_state, rounded = advance(
        accepted,
        prev_forget,
        prev_input.reshape(seqs, proposals, -1).transpose(1, 2, 0),
        state[:, 0],
    )

    sends, rows, scale = project(own, other, keyed, mixing)
    received = passed(sends)
    ours, theirs = turn_outward(w_out)
    theirs = lax.ppermute(theirs, "core", swap)
    shown = recur(received, rounded.reshape(-1, size), forget_floor[None], head_gain[None])
    parts = passed(shown)
    opened = gate(gain, gates, rows, scale)
    hidden = hide(parts, opened)
    kept = emit(hidden, lax.ppermute(hidden, "core", swap), ours, theirs)
    terms = lax.all_to_all(
        kept.reshape(planes * group, features, seqs), ("zy", "tp"), 0, 0, tiled=True
    )
    mixed = sums(terms.reshape(planes, group, features, seqs))
    return mixed.transpose(2, 0, 1), new_state[:, None]


def solution(mesh):
    kv, tp = mesh.shape["kv"], mesh.shape["tp"]
    finer = Mesh(mesh.devices.reshape(kv // 2, 2, tp), ("zy", "core", "tp"))
    rows = ("zy", "core")
    placed = (
        P(None, None, (*rows, "tp")),
        P(),
        P(None, rows),
        P(None, rows),
        P(rows, "tp", None),
        P(rows, "tp", None),
        P(rows),
        P("tp"),
        P(rows, None),
        P(None, rows, "tp", None),
        P(None, None, rows),
        P(None, None, rows, "tp"),
        P(),
    )

    return jax.shard_map(
        body,
        mesh=finer,
        in_specs=placed,
        out_specs=(P(None, None, (*rows, "tp")), P(None, rows, "tp", None)),
        check_vma=False,
    )
```

```python
import jax
import jax.numpy as jnp
from jax import lax
from jax.experimental import pallas as pl
from jax.experimental.pallas import tpu as pltpu
from jax.sharding import Mesh, PartitionSpec as P


NORM_EPSILON = 1e-06


def whole():
    return pl.BlockSpec(memory_space=pltpu.VMEM)


def shaped(shape, dtype):
    return jax.ShapeDtypeStruct(shape, dtype)


def call(kernel, out_shape, scratch, cost, limit, in_specs, out_specs):
    return pl.pallas_call(
        kernel,
        out_shape=out_shape,
        in_specs=in_specs,
        out_specs=out_specs,
        scratch_shapes=scratch,
        cost_estimate=pl.CostEstimate(flops=cost[0], bytes_accessed=cost[1], transcendentals=0),
        compiler_params=pltpu.CompilerParams(vmem_limit_bytes=limit),
    )


def advance_kernel(accepted, prev_forget, prev_input, state, new_state, rounded, live):
    block = pl.program_id(0)
    count, proposals, size = prev_forget.shape
    lanes = prev_input.shape[2]

    @pl.when(block == 0)
    def _():
        live[...] = jnp.broadcast_to(accepted[...].astype(jnp.float32), (size, lanes)).T

    shift = lax.rem(lanes - block * count, lanes)
    values = [
        pltpu.roll(prev_input[p].astype(jnp.float32), shift, 1) for p in range(proposals)
    ]
    taken = live[pl.ds(pl.multiple_of(block * count, count), count), :]
    rest = jnp.ones((count, size), jnp.float32)
    terms = [None] * proposals
    for p in reversed(range(proposals)):
        gate = jnp.where(taken > p, prev_forget[:, p, :], 1.0)
        terms[p] = rest * (1.0 - gate)
        rest = rest * gate
    for s in range(count):
        fresh = rest[s : s + 1] * state[s]
        for p in range(proposals):
            fresh = fresh + terms[p][s : s + 1] * values[p][:, s : s + 1]
        new_state[s] = fresh
        rounded[s] = fresh.astype(jnp.bfloat16)


def advance(accepted, prev_forget, prev_input, state):
    seqs, values, keys = state.shape
    proposals = prev_forget.shape[1]
    count = 32
    span = pl.BlockSpec((count, values, keys), lambda i: (i, 0, 0))
    return pl.pallas_call(
        advance_kernel,
        grid=(seqs // count,),
        in_specs=[
            pl.BlockSpec((1, seqs), lambda i: (0, 0)),
            pl.BlockSpec((count, proposals, keys), lambda i: (i, 0, 0)),
            pl.BlockSpec((proposals, values, seqs), lambda i: (0, 0, 0)),
            span,
        ],
        out_specs=[span, span],
        out_shape=[shaped(state.shape, jnp.float32), shaped(state.shape, jnp.bfloat16)],
        scratch_shapes=[pltpu.VMEM((keys, seqs), jnp.float32)],
        name="advance",
        cost_estimate=pl.CostEstimate(
            flops=1_000_000_000, bytes_accessed=5 << 20, transcendentals=0
        ),
        compiler_params=pltpu.CompilerParams(vmem_limit_bytes=16 << 20),
    )(accepted[None], prev_forget, prev_input, state)


def split_in_three(value):
    high = value.astype(jnp.bfloat16).astype(jnp.float32)
    middle = (value - high).astype(jnp.bfloat16).astype(jnp.float32)
    return high, middle, value - high - middle


def three_rows(parts, width):
    rest = jnp.zeros((16 - 3 * parts[0].shape[0], width), jnp.float32)
    return jnp.concatenate([*parts, rest], axis=0).astype(jnp.bfloat16)


def source_kernel(tokens, out, held, sems):
    steps = tokens.shape[0]
    planes = out.shape[0] // steps
    copy = pltpu.make_async_copy(tokens, held, sems.at[planes])
    copy.start()
    copy.wait()
    copies = [
        pltpu.make_async_copy(held, out.at[pl.ds(z * steps, steps)], sems.at[z])
        for z in range(planes)
    ]
    for copy in copies:
        copy.start()
    for copy in copies:
        copy.wait()


def source(tokens, planes):
    steps, features, seqs = tokens.shape
    far = pl.BlockSpec(memory_space=pltpu.HBM)
    return call(
        source_kernel,
        shaped((planes * steps, features, seqs), jnp.bfloat16),
        [pltpu.VMEM(tokens.shape, jnp.bfloat16), pltpu.SemaphoreType.DMA((planes + 1,))],
        (1_000_000, 1 << 20),
        60 << 20,
        [far],
        far,
    )(tokens)


def ordered(blocks, size):
    core = lax.axis_index("core")
    for half in range(2):
        for b in range(blocks // 2):
            row = 2 * b + (core if half == 0 else 1 - core)
            yield row, pl.ds(pl.multiple_of(row * size, size), size), half * (blocks // 2) + b


def turn_kernel(gain, w_query, w_forget, keyed):
    blocks, size = gain.shape
    for row, at, to in ordered(blocks, size):
        scale = gain[pl.ds(row, 1), :]
        for i, weight in enumerate((w_query, w_forget)):
            block = weight[at, :].astype(jnp.float32).T
            keyed[pl.ds(i * size, size), pl.ds(to * size, size)] = (block * scale).astype(jnp.bfloat16)


def turn(gain, w_query, w_forget):
    width, size = w_query.shape
    return call(
        turn_kernel,
        shaped((2 * size, width), jnp.bfloat16),
        [],
        (1_000_000_000, 4 << 20),
        16 << 20,
        [whole()] * 3,
        whole(),
    )(gain, w_query, w_forget)


def fold_kernel(gain, w0, w1, w2, w3, out):
    fold_into(out, gain, (w0, w1, w2, w3))


def fold_into(out, gain, weights):
    blocks, size = gain.shape
    values = weights[0].shape[1]
    for row, at, to in ordered(blocks, size):
        scale = gain[pl.ds(row, 1), :]
        for d, weight in enumerate(weights):
            value = weight[0, :, at].astype(jnp.float32) * scale
            out[pl.ds(d * values, values), pl.ds(to * size, size)] = value.astype(jnp.bfloat16)


def fold(gain, weights):
    _, values, width = weights[0].shape
    return call(
        fold_kernel,
        shaped((4 * values, width), jnp.bfloat16),
        [],
        (1_000_000_000, 2 << 20),
        16 << 20,
        [whole()] * 5,
        whole(),
    )(gain, *weights)


def squared(rows):
    wide = rows[...].astype(jnp.float32)
    return jnp.sum((wide * wide).reshape(rows.shape[0] // 8, 8, rows.shape[1]), axis=0)


def begin_kernel(own, keyed, mixing, out, squares):
    cut, keys = pl.ds(0, own.shape[0]), keyed.shape[0]
    squares[...] = squared(own)
    rows = own[...]
    out[pl.ds(0, keys), :] = jnp.dot(keyed[:, cut], rows, preferred_element_type=jnp.float32)
    out[pl.ds(keys, mixing.shape[0]), :] = jnp.dot(
        mixing[:, cut], rows, preferred_element_type=jnp.float32
    )


def begin(own, keyed, mixing):
    seqs = own.shape[1]
    return call(
        begin_kernel,
        [
            shaped((keyed.shape[0] + mixing.shape[0], seqs), jnp.float32),
            shaped((8, seqs), jnp.float32),
        ],
        [],
        (1_000_000_000, 2 << 20),
        16 << 20,
        [whole()] * 3,
        [whole()] * 2,
    )(own, keyed, mixing)


def project_kernel(other, keyed, mixing, started, squares, o0, o1, o2, o3, scale):
    half, keys = other.shape[0], keyed.shape[0]
    cut = pl.ds(half, half)
    total = jnp.sum(squares[...] + squared(other), axis=0, keepdims=True)
    factor = lax.rsqrt(total / (2 * half) + NORM_EPSILON)
    scale[...] = jnp.broadcast_to(factor, scale.shape)
    rows = other[...]
    first = jnp.dot(keyed[:, cut], rows, preferred_element_type=jnp.float32)
    first = ((first + started[pl.ds(0, keys), :]) * factor).astype(jnp.bfloat16)
    second = jnp.dot(mixing[:, cut], rows, preferred_element_type=jnp.float32)
    second = second + started[pl.ds(keys, second.shape[0]), :]
    second = (second * factor).astype(jnp.bfloat16)
    values = second.shape[0] // 4
    for d, out in enumerate((o0, o1, o2, o3)):
        out[pl.ds(0, keys), :] = first
        out[pl.ds(keys, values), :] = second[d * values : (d + 1) * values]


def project(other, keyed, mixing, started, squares):
    seqs = other.shape[1]
    rows = keyed.shape[0] + mixing.shape[0] // 4
    outs = call(
        project_kernel,
        [shaped((rows, seqs), jnp.bfloat16)] * 4 + [shaped((8, seqs), jnp.float32)],
        [],
        (1_000_000_000, 2 << 20),
        16 << 20,
        [whole()] * 5,
        [whole()] * 5,
    )(other, keyed, mixing, started, squares)
    return outs[:4], outs[4]


def gate_kernel(gain, w0, w1, w2, w3, own, other, scale, out, held):
    fold_into(held, gain, (w0, w1, w2, w3))
    half = own.shape[0]
    raw = jnp.dot(held[:, pl.ds(0, half)], own[...], preferred_element_type=jnp.float32)
    raw = raw + jnp.dot(
        held[:, pl.ds(half, half)], other[...], preferred_element_type=jnp.float32
    )
    raw = (raw * scale[0:1]).astype(jnp.bfloat16).astype(jnp.float32)
    out[...] = raw * jax.nn.sigmoid(raw)


def gate(gain, weights, own, other, scale):
    _, values, width = weights[0].shape
    return call(
        gate_kernel,
        shaped((4 * values, own.shape[1]), jnp.float32),
        [pltpu.VMEM((4 * values, width), jnp.bfloat16)],
        (1_000_000_000, 3 << 20),
        16 << 20,
        [whole()] * 8,
        whole(),
    )(gain, *weights, own, other, scale)


def outward_kernel(w_out, mine, theirs, held, sems):
    core = lax.axis_index("core")
    cuts, size, span = held.shape
    copies = [
        pltpu.make_async_copy(w_out.at[:, pl.ds(c * span, span)], held.at[c], sems.at[c])
        for c in range(cuts)
    ]
    for copy in copies:
        copy.start()
    pairs = span // size // 2
    for c in range(cuts):
        copies[c].wait()
        for b in range(pairs):
            for half, out in ((core, mine), (1 - core, theirs)):
                at = pl.multiple_of((2 * b + half) * size, size)
                block = held[c, :, pl.ds(at, size)].astype(jnp.float32)
                out[c * pairs + b] = block.T.astype(jnp.bfloat16)


def turn_outward(w_out):
    size, width = w_out.shape
    return call(
        outward_kernel,
        [shaped((width // size // 2, size, size), jnp.bfloat16)] * 2,
        [pltpu.VMEM((4, size, width // 4), jnp.bfloat16), pltpu.SemaphoreType.DMA((4,))],
        (1_000_000_000, 2 << 20),
        16 << 20,
        [pl.BlockSpec(memory_space=pltpu.HBM)],
        [whole()] * 2,
    )(w_out)


def recur_kernel(r0, r1, r2, r3, before, floor, head_gain, o0, o1, o2, o3, seen, ready):
    mine = lax.axis_index("tp")
    size = floor.shape[1]
    values = head_gain.shape[1]
    count = before.shape[0] // values
    steps = 4
    for d, ref in enumerate((r0, r1, r2, r3)):
        seen[mine ^ d] = ref[...]
    low = jnp.broadcast_to(floor[...], (count, size)).T
    scale = jnp.broadcast_to(head_gain[...], (count, values)).T
    forget, keys, fresh, sums, asked = [], [], [], [], []
    for t in range(steps):
        gate = low + (1.0 - low) * jax.nn.sigmoid(seen[t, pl.ds(size, size), :].astype(jnp.float32))
        forget.append(gate)
        keys.append(1.0 - gate)
        fresh.append(seen[t, pl.ds(2 * size, values), :].astype(jnp.float32))
    for t in range(steps):
        moved = seen[t, pl.ds(0, size), :].astype(jnp.float32)
        out = None
        for u in reversed(range(t + 1)):
            score = jnp.sum(moved * keys[u], axis=0, keepdims=True)
            term = score * fresh[u]
            out = term if out is None else out + term
            moved = moved * forget[u]
        sums.append(out)
        asked.append(moved.astype(jnp.bfloat16))
    half = count // 2
    lane = lax.rem(lax.broadcasted_iota(jnp.int32, (values, steps * half), 1), half)
    group = 8
    halves = []
    for h in range(2):
        wanted = jnp.concatenate([a[:, h * half : (h + 1) * half] for a in asked], axis=1)
        total = jnp.zeros((values, steps * half), jnp.float32)
        for b in range(half // group):
            first = h * half + b * group
            read = jnp.dot(
                before[pl.ds(first * values, group * values), :],
                wanted,
                preferred_element_type=jnp.float32,
            )
            for s in range(group):
                part = read[s * values : (s + 1) * values]
                total = total + jnp.where(lane == b * group + s, part, 0.0)
        halves.append(total)
    for t in range(steps):
        cut = [total[:, t * half : (t + 1) * half] for total in halves]
        sums[t] = sums[t] + jnp.concatenate(cut, axis=1)
    for t in range(steps):
        out = sums[t]
        square = jnp.sum(out * out, axis=0, keepdims=True)
        ready[t, pl.ds(0, values), :] = (out * scale).astype(jnp.bfloat16)
        ready[t, pl.ds(values, 16), :] = three_rows(split_in_three(square), count)
    for d, ref in enumerate((o0, o1, o2, o3)):
        ref[...] = ready[mine ^ d]


def recur(received, before, floor, head_gain):
    rows, count = received[0].shape
    values = head_gain.shape[1]
    return call(
        recur_kernel,
        [shaped((values + 16, count), jnp.bfloat16)] * 4,
        [
            pltpu.VMEM((4, rows, count), jnp.bfloat16),
            pltpu.VMEM((4, values + 16, count), jnp.bfloat16),
        ],
        (1_000_000_000, 2 << 20),
        16 << 20,
        [whole()] * 7,
        [whole()] * 4,
    )(*received, before, floor, head_gain)


def hide_kernel(p0, p1, p2, p3, gates, hidden):
    mine = lax.axis_index("tp")
    values = hidden.shape[0] // 4
    parts = (p0, p1, p2, p3)
    total = None
    for ref in parts:
        square = jnp.sum(ref[pl.ds(values, 16), :].astype(jnp.float32), axis=0, keepdims=True)
        total = square if total is None else total + square
    factor = lax.rsqrt(total / hidden.shape[0] + NORM_EPSILON)
    for d, ref in enumerate(parts):
        at = pl.multiple_of((mine ^ d) * values, values)
        value = ref[pl.ds(0, values), :].astype(jnp.float32) * factor
        value = value * gates[pl.ds(d * values, values), :]
        hidden[pl.ds(at, values), :] = value.astype(jnp.bfloat16)


def hide(parts, gates):
    return call(
        hide_kernel,
        shaped(gates.shape, jnp.bfloat16),
        [],
        (1_000_000, 1 << 18),
        16 << 20,
        [whole()] * 5,
        whole(),
    )(*parts, gates)


def emit_kernel(hidden, other, ours, theirs, out):
    for b in range(out.shape[0]):
        part = jnp.dot(ours[b], hidden[...], preferred_element_type=jnp.float32)
        part = part + jnp.dot(theirs[b], other[...], preferred_element_type=jnp.float32)
        out[b] = part.astype(jnp.bfloat16)


def emit(hidden, other, ours, theirs):
    blocks, size, _ = ours.shape
    return call(
        emit_kernel,
        shaped((blocks, size, hidden.shape[1]), jnp.bfloat16),
        [],
        (100_000_000, 2 << 20),
        16 << 20,
        [whole()] * 4,
        whole(),
    )(hidden, other, ours, theirs)


def sum_kernel(parts, out):
    total = parts[0].astype(jnp.float32)
    for b in range(1, parts.shape[0]):
        total = total + parts[b].astype(jnp.float32)
    out[...] = total.astype(out.dtype)


def sums(parts):
    return call(
        sum_kernel,
        shaped(parts.shape[1:], jnp.bfloat16),
        [],
        (1_000_000, 1 << 20),
        8 << 20,
        [whole()],
        whole(),
    )(parts)


def body(
    tokens,
    input_norm_gain,
    w_query,
    w_forget,
    w_input,
    w_gate,
    forget_floor,
    head_gain,
    w_out,
    state,
    prev_forget,
    prev_input,
    accepted,
):
    planes, group = lax.axis_size("zy"), lax.axis_size("tp")
    seqs, proposals, features = tokens.shape
    _, size = w_query.shape
    swap = [(0, 1), (1, 0)]
    hops = [[(i, i ^ d) for i in range(group)] for d in range(group)]

    def passed(parts):
        far = lax.ppermute(parts[2], "tp", hops[2])
        wrap = lax.ppermute(parts[3], "tp", hops[3])
        near = lax.ppermute(parts[1], "tp", hops[1])
        return [parts[0], near, far, wrap]

    gain = input_norm_gain.reshape(-1, size)
    inputs = passed([w_input] * group)
    own = lax.all_to_all(source(tokens.transpose(1, 2, 0), planes), ("zy", "tp"), 0, 0, tiled=True)
    own = own.reshape(planes * group * features, seqs)
    other = lax.ppermute(own, "core", swap)
    gates = passed([w_gate] * group)
    keyed = turn(gain, w_query, w_forget)
    mixing = fold(gain, inputs)
    new_state, rounded = advance(
        accepted,
        prev_forget,
        prev_input.reshape(seqs, proposals, -1).transpose(1, 2, 0),
        state[:, 0],
    )

    started, squares = begin(own, keyed, mixing)
    sends, scale = project(other, keyed, mixing, started, squares)
    received = passed(sends)
    ours, theirs = turn_outward(w_out)
    theirs = lax.ppermute(theirs, "core", swap)
    shown = recur(received, rounded.reshape(-1, size), forget_floor[None], head_gain[None])
    parts = passed(shown)
    opened = gate(gain, gates, own, other, scale)
    hidden = hide(parts, opened)
    kept = emit(hidden, lax.ppermute(hidden, "core", swap), ours, theirs)
    terms = lax.all_to_all(
        kept.reshape(planes * group, features, seqs), ("zy", "tp"), 0, 0, tiled=True
    )
    mixed = sums(terms.reshape(planes, group, features, seqs))
    return mixed.transpose(2, 0, 1), new_state[:, None]


def solution(mesh):
    kv, tp = mesh.shape["kv"], mesh.shape["tp"]
    finer = Mesh(mesh.devices.reshape(kv // 2, 2, tp), ("zy", "core", "tp"))
    rows = ("zy", "core")
    placed = (
        P(None, None, (*rows, "tp")),
        P(),
        P(None, rows),
        P(None, rows),
        P(rows, "tp", None),
        P(rows, "tp", None),
        P(rows),
        P("tp"),
        P(rows, None),
        P(None, rows, "tp", None),
        P(None, None, rows),
        P(None, None, rows, "tp"),
        P(),
    )

    return jax.shard_map(
        body,
        mesh=finer,
        in_specs=placed,
        out_specs=(P(None, None, (*rows, "tp")), P(None, rows, "tp", None)),
        check_vma=False,
    )
```

```python
import jax
import jax.numpy as jnp
from jax import lax
from jax.experimental import pallas as pl
from jax.experimental.pallas import tpu as pltpu
from jax.sharding import Mesh, PartitionSpec as P


NORM_EPSILON = 1e-06


def whole():
    return pl.BlockSpec(memory_space=pltpu.VMEM)


def shaped(shape, dtype):
    return jax.ShapeDtypeStruct(shape, dtype)


def call(kernel, out_shape, scratch, cost, limit, in_specs, out_specs):
    return pl.pallas_call(
        kernel,
        out_shape=out_shape,
        in_specs=in_specs,
        out_specs=out_specs,
        scratch_shapes=scratch,
        cost_estimate=pl.CostEstimate(flops=cost[0], bytes_accessed=cost[1], transcendentals=0),
        compiler_params=pltpu.CompilerParams(vmem_limit_bytes=limit),
    )


def advance_kernel(accepted, prev_forget, prev_input, state, new_state, rounded, live):
    block = pl.program_id(0)
    count, proposals, size = prev_forget.shape
    lanes = prev_input.shape[2]

    @pl.when(block == 0)
    def _():
        live[...] = jnp.broadcast_to(accepted[...].astype(jnp.float32), (size, lanes)).T

    shift = lax.rem(lanes - block * count, lanes)
    values = [
        pltpu.roll(prev_input[p].astype(jnp.float32), shift, 1) for p in range(proposals)
    ]
    taken = live[pl.ds(pl.multiple_of(block * count, count), count), :]
    rest = jnp.ones((count, size), jnp.float32)
    terms = [None] * proposals
    for p in reversed(range(proposals)):
        gate = jnp.where(taken > p, prev_forget[:, p, :], 1.0)
        terms[p] = rest * (1.0 - gate)
        rest = rest * gate
    for s in range(count):
        fresh = rest[s : s + 1] * state[s]
        for p in range(proposals):
            fresh = fresh + terms[p][s : s + 1] * values[p][:, s : s + 1]
        new_state[s] = fresh
        rounded[s] = fresh.astype(jnp.bfloat16)


def advance(accepted, prev_forget, prev_input, state):
    seqs, values, keys = state.shape
    proposals = prev_forget.shape[1]
    count = 32
    span = pl.BlockSpec((count, values, keys), lambda i: (i, 0, 0))
    return pl.pallas_call(
        advance_kernel,
        grid=(seqs // count,),
        in_specs=[
            pl.BlockSpec((1, seqs), lambda i: (0, 0)),
            pl.BlockSpec((count, proposals, keys), lambda i: (i, 0, 0)),
            pl.BlockSpec((proposals, values, seqs), lambda i: (0, 0, 0)),
            span,
        ],
        out_specs=[span, span],
        out_shape=[shaped(state.shape, jnp.float32), shaped(state.shape, jnp.bfloat16)],
        scratch_shapes=[pltpu.VMEM((keys, seqs), jnp.float32)],
        name="advance",
        cost_estimate=pl.CostEstimate(
            flops=1_000_000_000, bytes_accessed=5 << 20, transcendentals=0
        ),
        compiler_params=pltpu.CompilerParams(vmem_limit_bytes=16 << 20),
    )(accepted[None], prev_forget, prev_input, state)


def split_in_three(value):
    high = value.astype(jnp.bfloat16).astype(jnp.float32)
    middle = (value - high).astype(jnp.bfloat16).astype(jnp.float32)
    return high, middle, value - high - middle


def three_rows(parts, width):
    rest = jnp.zeros((16 - 3 * parts[0].shape[0], width), jnp.float32)
    return jnp.concatenate([*parts, rest], axis=0).astype(jnp.bfloat16)


def source_kernel(tokens, out, held, sems):
    steps = tokens.shape[0]
    planes = out.shape[0] // steps
    copy = pltpu.make_async_copy(tokens, held, sems.at[planes])
    copy.start()
    copy.wait()
    copies = [
        pltpu.make_async_copy(held, out.at[pl.ds(z * steps, steps)], sems.at[z])
        for z in range(planes)
    ]
    for copy in copies:
        copy.start()
    for copy in copies:
        copy.wait()


def source(tokens, planes):
    steps, features, seqs = tokens.shape
    far = pl.BlockSpec(memory_space=pltpu.HBM)
    return call(
        source_kernel,
        shaped((planes * steps, features, seqs), jnp.bfloat16),
        [pltpu.VMEM(tokens.shape, jnp.bfloat16), pltpu.SemaphoreType.DMA((planes + 1,))],
        (1_000_000, 1 << 20),
        60 << 20,
        [far],
        far,
    )(tokens)


def turn_kernel(gain, w_query, w_forget, keyed):
    size = gain.shape[1]
    for b in range(w_query.shape[0] // size):
        at = pl.ds(b * size, size)
        row = gain[pl.ds(b, 1), :]
        for i, weight in enumerate((w_query, w_forget)):
            block = weight[at, :].astype(jnp.float32).T
            keyed[pl.ds(i * size, size), at] = (block * row).astype(jnp.bfloat16)


def turn(gain, w_query, w_forget):
    width, size = w_query.shape
    return call(
        turn_kernel,
        shaped((2 * size, width), jnp.bfloat16),
        [],
        (1_000_000_000, 4 << 20),
        16 << 20,
        [whole()] * 3,
        whole(),
    )(gain, w_query, w_forget)


def fold_kernel(gain, w0, w1, w2, w3, out):
    values, size = w0.shape[1], gain.shape[1]
    for b in range(gain.shape[0]):
        at = pl.ds(b * size, size)
        for d, weight in enumerate((w0, w1, w2, w3)):
            value = weight[0, :, at].astype(jnp.float32) * gain[pl.ds(b, 1), :]
            out[pl.ds(d * values, values), at] = value.astype(jnp.bfloat16)


def fold(gain, weights):
    _, values, width = weights[0].shape
    return call(
        fold_kernel,
        shaped((4 * values, width), jnp.bfloat16),
        [],
        (1_000_000_000, 2 << 20),
        16 << 20,
        [whole()] * 5,
        whole(),
    )(gain, *weights)


def project_kernel(own, other, keyed, mixing, o0, o1, o2, o3, held, scale):
    core = lax.axis_index("core")
    blocks, size, seqs = own.shape
    squares = jnp.zeros((8, seqs), jnp.float32)
    for half, ref in ((core, own), (1 - core, other)):
        for b in range(blocks):
            part = ref[b]
            held[pl.ds(pl.multiple_of((2 * b + half) * size, size), size), :] = part
            wide = part.astype(jnp.float32)
            squares = squares + jnp.sum((wide * wide).reshape(size // 8, 8, seqs), axis=0)
    total = jnp.sum(squares, axis=0, keepdims=True)
    factor = lax.rsqrt(total / (2 * blocks * size) + NORM_EPSILON)
    scale[...] = jnp.broadcast_to(factor, scale.shape)
    rows = held[...]
    first = jnp.dot(keyed[...], rows, preferred_element_type=jnp.float32) * factor
    first = first.astype(jnp.bfloat16)
    second = jnp.dot(mixing[...], rows, preferred_element_type=jnp.float32) * factor
    second = second.astype(jnp.bfloat16)
    keys, values = first.shape[0], second.shape[0] // 4
    for d, out in enumerate((o0, o1, o2, o3)):
        out[pl.ds(0, keys), :] = first
        out[pl.ds(keys, values), :] = second[d * values : (d + 1) * values]


def project(own, other, keyed, mixing):
    blocks, size, seqs = own.shape
    rows = keyed.shape[0] + mixing.shape[0] // 4
    outs = call(
        project_kernel,
        [shaped((rows, seqs), jnp.bfloat16)] * 4
        + [shaped((2 * blocks * size, seqs), jnp.bfloat16), shaped((8, seqs), jnp.float32)],
        [],
        (1_000_000_000, 3 << 20),
        16 << 20,
        [whole()] * 4,
        [whole()] * 6,
    )(own, other, keyed, mixing)
    return outs[:4], outs[4], outs[5]


def gate_kernel(gain, w0, w1, w2, w3, rows, scale, out, held):
    values, size = w0.shape[1], gain.shape[1]
    for b in range(gain.shape[0]):
        at = pl.ds(b * size, size)
        for d, weight in enumerate((w0, w1, w2, w3)):
            value = weight[0, :, at].astype(jnp.float32) * gain[pl.ds(b, 1), :]
            held[pl.ds(d * values, values), at] = value.astype(jnp.bfloat16)
    raw = jnp.dot(held[...], rows[...], preferred_element_type=jnp.float32) * scale[0:1]
    raw = raw.astype(jnp.bfloat16).astype(jnp.float32)
    out[...] = raw * jax.nn.sigmoid(raw)


def gate(gain, weights, rows, scale):
    _, values, width = weights[0].shape
    return call(
        gate_kernel,
        shaped((4 * values, rows.shape[1]), jnp.float32),
        [pltpu.VMEM((4 * values, width), jnp.bfloat16)],
        (1_000_000_000, 3 << 20),
        16 << 20,
        [whole()] * 7,
        whole(),
    )(gain, *weights, rows, scale)


def outward_kernel(w_out, mine, theirs, held, sems):
    core = lax.axis_index("core")
    cuts, size, span = held.shape
    copies = [
        pltpu.make_async_copy(w_out.at[:, pl.ds(c * span, span)], held.at[c], sems.at[c])
        for c in range(cuts)
    ]
    for copy in copies:
        copy.start()
    pairs = span // size // 2
    for c in range(cuts):
        copies[c].wait()
        for b in range(pairs):
            for half, out in ((core, mine), (1 - core, theirs)):
                at = pl.multiple_of((2 * b + half) * size, size)
                block = held[c, :, pl.ds(at, size)].astype(jnp.float32)
                out[c * pairs + b] = block.T.astype(jnp.bfloat16)


def turn_outward(w_out):
    size, width = w_out.shape
    return call(
        outward_kernel,
        [shaped((width // size // 2, size, size), jnp.bfloat16)] * 2,
        [pltpu.VMEM((4, size, width // 4), jnp.bfloat16), pltpu.SemaphoreType.DMA((4,))],
        (1_000_000_000, 2 << 20),
        16 << 20,
        [pl.BlockSpec(memory_space=pltpu.HBM)],
        [whole()] * 2,
    )(w_out)


def recur_kernel(r0, r1, r2, r3, before, floor, head_gain, o0, o1, o2, o3, seen, ready):
    mine = lax.axis_index("tp")
    size = floor.shape[1]
    values = head_gain.shape[1]
    count = before.shape[0] // values
    steps = 4
    for d, ref in enumerate((r0, r1, r2, r3)):
        seen[mine ^ d] = ref[...]
    low = jnp.broadcast_to(floor[...], (count, size)).T
    scale = jnp.broadcast_to(head_gain[...], (count, values)).T
    forget, keys, fresh, sums, asked = [], [], [], [], []
    for t in range(steps):
        gate = low + (1.0 - low) * jax.nn.sigmoid(seen[t, pl.ds(size, size), :].astype(jnp.float32))
        forget.append(gate)
        keys.append(1.0 - gate)
        fresh.append(seen[t, pl.ds(2 * size, values), :].astype(jnp.float32))
    for t in range(steps):
        moved = seen[t, pl.ds(0, size), :].astype(jnp.float32)
        out = None
        for u in reversed(range(t + 1)):
            score = jnp.sum(moved * keys[u], axis=0, keepdims=True)
            term = score * fresh[u]
            out = term if out is None else out + term
            moved = moved * forget[u]
        sums.append(out)
        asked.append(moved.astype(jnp.bfloat16))
    half = count // 2
    lane = lax.rem(lax.broadcasted_iota(jnp.int32, (values, steps * half), 1), half)
    group = 8
    halves = []
    for h in range(2):
        wanted = jnp.concatenate([a[:, h * half : (h + 1) * half] for a in asked], axis=1)
        total = jnp.zeros((values, steps * half), jnp.float32)
        for b in range(half // group):
            first = h * half + b * group
            read = jnp.dot(
                before[pl.ds(first * values, group * values), :],
                wanted,
                preferred_element_type=jnp.float32,
            )
            for s in range(group):
                part = read[s * values : (s + 1) * values]
                total = total + jnp.where(lane == b * group + s, part, 0.0)
        halves.append(total)
    for t in range(steps):
        cut = [total[:, t * half : (t + 1) * half] for total in halves]
        sums[t] = sums[t] + jnp.concatenate(cut, axis=1)
    for t in range(steps):
        out = sums[t]
        square = jnp.sum(out * out, axis=0, keepdims=True)
        ready[t, pl.ds(0, values), :] = (out * scale).astype(jnp.bfloat16)
        ready[t, pl.ds(values, 16), :] = three_rows(split_in_three(square), count)
    for d, ref in enumerate((o0, o1, o2, o3)):
        ref[...] = ready[mine ^ d]


def recur(received, before, floor, head_gain):
    rows, count = received[0].shape
    values = head_gain.shape[1]
    return call(
        recur_kernel,
        [shaped((values + 16, count), jnp.bfloat16)] * 4,
        [
            pltpu.VMEM((4, rows, count), jnp.bfloat16),
            pltpu.VMEM((4, values + 16, count), jnp.bfloat16),
        ],
        (1_000_000_000, 2 << 20),
        16 << 20,
        [whole()] * 7,
        [whole()] * 4,
    )(*received, before, floor, head_gain)


def hide_kernel(p0, p1, p2, p3, gates, hidden):
    mine = lax.axis_index("tp")
    values = hidden.shape[0] // 4
    parts = (p0, p1, p2, p3)
    total = None
    for ref in parts:
        square = jnp.sum(ref[pl.ds(values, 16), :].astype(jnp.float32), axis=0, keepdims=True)
        total = square if total is None else total + square
    factor = lax.rsqrt(total / hidden.shape[0] + NORM_EPSILON)
    for d, ref in enumerate(parts):
        at = pl.multiple_of((mine ^ d) * values, values)
        value = ref[pl.ds(0, values), :].astype(jnp.float32) * factor
        value = value * gates[pl.ds(d * values, values), :]
        hidden[pl.ds(at, values), :] = value.astype(jnp.bfloat16)


def hide(parts, gates):
    return call(
        hide_kernel,
        shaped(gates.shape, jnp.bfloat16),
        [],
        (1_000_000, 1 << 18),
        16 << 20,
        [whole()] * 5,
        whole(),
    )(*parts, gates)


def emit_kernel(hidden, other, ours, theirs, out):
    for b in range(out.shape[0]):
        part = jnp.dot(ours[b], hidden[...], preferred_element_type=jnp.float32)
        part = part + jnp.dot(theirs[b], other[...], preferred_element_type=jnp.float32)
        out[b] = part.astype(jnp.bfloat16)


def emit(hidden, other, ours, theirs):
    blocks, size, _ = ours.shape
    return call(
        emit_kernel,
        shaped((blocks, size, hidden.shape[1]), jnp.bfloat16),
        [],
        (100_000_000, 2 << 20),
        16 << 20,
        [whole()] * 4,
        whole(),
    )(hidden, other, ours, theirs)


def sum_kernel(parts, out):
    total = parts[0].astype(jnp.float32)
    for b in range(1, parts.shape[0]):
        total = total + parts[b].astype(jnp.float32)
    out[...] = total.astype(out.dtype)


def sums(parts):
    return call(
        sum_kernel,
        shaped(parts.shape[1:], jnp.bfloat16),
        [],
        (1_000_000, 1 << 20),
        8 << 20,
        [whole()],
        whole(),
    )(parts)


def body(
    tokens,
    input_norm_gain,
    w_query,
    w_forget,
    w_input,
    w_gate,
    forget_floor,
    head_gain,
    w_out,
    state,
    prev_forget,
    prev_input,
    accepted,
):
    planes, group = lax.axis_size("zy"), lax.axis_size("tp")
    seqs, proposals, features = tokens.shape
    _, size = w_query.shape
    swap = [(0, 1), (1, 0)]
    hops = [[(i, i ^ d) for i in range(group)] for d in range(group)]

    def passed(parts):
        far = lax.ppermute(parts[2], "tp", hops[2])
        wrap = lax.ppermute(parts[3], "tp", hops[3])
        near = lax.ppermute(parts[1], "tp", hops[1])
        return [parts[0], near, far, wrap]

    gain = input_norm_gain.reshape(-1, size)
    inputs = passed([w_input] * group)
    own = lax.all_to_all(source(tokens.transpose(1, 2, 0), planes), ("zy", "tp"), 0, 0, tiled=True)
    own = own.reshape(planes, group * features, seqs)
    other = lax.ppermute(own, "core", swap)
    gates = passed([w_gate] * group)
    keyed = turn(gain, w_query, w_forget)
    mixing = fold(gain, inputs)
    new_state, rounded = advance(
        accepted,
        prev_forget,
        prev_input.reshape(seqs, proposals, -1).transpose(1, 2, 0),
        state[:, 0],
    )

    sends, rows, scale = project(own, other, keyed, mixing)
    received = passed(sends)
    ours, theirs = turn_outward(w_out)
    theirs = lax.ppermute(theirs, "core", swap)
    shown = recur(received, rounded.reshape(-1, size), forget_floor[None], head_gain[None])
    parts = passed(shown)
    opened = gate(gain, gates, rows, scale)
    hidden = hide(parts, opened)
    kept = emit(hidden, lax.ppermute(hidden, "core", swap), ours, theirs)
    terms = lax.all_to_all(
        kept.reshape(planes * group, features, seqs), ("zy", "tp"), 0, 0, tiled=True
    )
    mixed = sums(terms.reshape(planes, group, features, seqs))
    return mixed.transpose(2, 0, 1), new_state[:, None]


def solution(mesh):
    kv, tp = mesh.shape["kv"], mesh.shape["tp"]
    finer = Mesh(mesh.devices.reshape(kv // 2, 2, tp), ("zy", "core", "tp"))
    rows = ("zy", "core")
    placed = (
        P(None, None, (*rows, "tp")),
        P(),
        P(None, rows),
        P(None, rows),
        P(rows, "tp", None),
        P(rows, "tp", None),
        P(rows),
        P("tp"),
        P(rows, None),
        P(None, rows, "tp", None),
        P(None, None, rows),
        P(None, None, rows, "tp"),
        P(),
    )

    return jax.shard_map(
        body,
        mesh=finer,
        in_specs=placed,
        out_specs=(P(None, None, (*rows, "tp")), P(None, rows, "tp", None)),
        check_vma=False,
    )
```

```python
import jax
import jax.numpy as jnp
from jax import lax
from jax.experimental import pallas as pl
from jax.experimental.pallas import tpu as pltpu
from jax.sharding import Mesh, PartitionSpec as P


NORM_EPSILON = 1e-06


def whole():
    return pl.BlockSpec(memory_space=pltpu.VMEM)


def shaped(shape, dtype):
    return jax.ShapeDtypeStruct(shape, dtype)


def call(kernel, out_shape, scratch, cost, limit, in_specs, out_specs):
    return pl.pallas_call(
        kernel,
        out_shape=out_shape,
        in_specs=in_specs,
        out_specs=out_specs,
        scratch_shapes=scratch,
        cost_estimate=pl.CostEstimate(flops=cost[0], bytes_accessed=cost[1], transcendentals=0),
        compiler_params=pltpu.CompilerParams(vmem_limit_bytes=limit),
    )


def advance_kernel(accepted, prev_forget, prev_input, state, new_state, live):
    block = pl.program_id(0)
    count, proposals, size = prev_forget.shape
    lanes = prev_input.shape[2]

    @pl.when(block == 0)
    def _():
        live[...] = jnp.broadcast_to(accepted[...].astype(jnp.float32), (size, lanes)).T

    shift = lax.rem(lanes - block * count, lanes)
    values = [
        pltpu.roll(prev_input[p].astype(jnp.float32), shift, 1) for p in range(proposals)
    ]
    taken = live[pl.ds(pl.multiple_of(block * count, count), count), :]
    rest = jnp.ones((count, size), jnp.float32)
    terms = [None] * proposals
    for p in reversed(range(proposals)):
        gate = jnp.where(taken > p, prev_forget[:, p, :], 1.0)
        terms[p] = rest * (1.0 - gate)
        rest = rest * gate
    for s in range(count):
        fresh = rest[s : s + 1] * state[s]
        for p in range(proposals):
            fresh = fresh + terms[p][s : s + 1] * values[p][:, s : s + 1]
        new_state[s] = fresh


def advance(accepted, prev_forget, prev_input, state):
    seqs, values, keys = state.shape
    proposals = prev_forget.shape[1]
    count = 16
    span = pl.BlockSpec((count, values, keys), lambda i: (i, 0, 0))
    return pl.pallas_call(
        advance_kernel,
        grid=(seqs // count,),
        in_specs=[
            pl.BlockSpec((1, seqs), lambda i: (0, 0)),
            pl.BlockSpec((count, proposals, keys), lambda i: (i, 0, 0)),
            pl.BlockSpec((proposals, values, seqs), lambda i: (0, 0, 0)),
            span,
        ],
        out_specs=span,
        out_shape=shaped(state.shape, jnp.float32),
        scratch_shapes=[pltpu.VMEM((keys, seqs), jnp.float32)],
        name="advance",
        cost_estimate=pl.CostEstimate(
            flops=1_000_000_000, bytes_accessed=5 << 20, transcendentals=0
        ),
        compiler_params=pltpu.CompilerParams(vmem_limit_bytes=60 << 20),
    )(accepted[None], prev_forget, prev_input, state)


def split_in_three(value):
    high = value.astype(jnp.bfloat16).astype(jnp.float32)
    middle = (value - high).astype(jnp.bfloat16).astype(jnp.float32)
    return high, middle, value - high - middle


def three_rows(parts, width):
    rest = jnp.zeros((16 - 3 * parts[0].shape[0], width), jnp.float32)
    return jnp.concatenate([*parts, rest], axis=0).astype(jnp.bfloat16)


def source_kernel(tokens, out, held, sems):
    steps = tokens.shape[0]
    planes = out.shape[0] // steps
    copy = pltpu.make_async_copy(tokens, held, sems.at[planes])
    copy.start()
    copy.wait()
    copies = [
        pltpu.make_async_copy(held, out.at[pl.ds(z * steps, steps)], sems.at[z])
        for z in range(planes)
    ]
    for copy in copies:
        copy.start()
    for copy in copies:
        copy.wait()


def source(tokens, planes):
    steps, features, seqs = tokens.shape
    far = pl.BlockSpec(memory_space=pltpu.HBM)
    return call(
        source_kernel,
        shaped((planes * steps, features, seqs), jnp.bfloat16),
        [pltpu.VMEM(tokens.shape, jnp.bfloat16), pltpu.SemaphoreType.DMA((planes + 1,))],
        (1_000_000, 1 << 20),
        60 << 20,
        [far],
        far,
    )(tokens)


def turn_kernel(gain, w_query, w_forget, keyed):
    size = gain.shape[1]
    for b in range(w_query.shape[0] // size):
        at = pl.ds(b * size, size)
        row = gain[pl.ds(b, 1), :]
        for i, weight in enumerate((w_query, w_forget)):
            block = weight[at, :].astype(jnp.float32).T
            keyed[pl.ds(i * size, size), at] = (block * row).astype(jnp.bfloat16)


def turn(gain, w_query, w_forget):
    width, size = w_query.shape
    return call(
        turn_kernel,
        shaped((2 * size, width), jnp.bfloat16),
        [],
        (1_000_000_000, 4 << 20),
        16 << 20,
        [whole()] * 3,
        whole(),
    )(gain, w_query, w_forget)


def fold_kernel(gain, w0, w1, w2, w3, out):
    values, size = w0.shape[1], gain.shape[1]
    for b in range(gain.shape[0]):
        at = pl.ds(b * size, size)
        for d, weight in enumerate((w0, w1, w2, w3)):
            value = weight[0, :, at].astype(jnp.float32) * gain[pl.ds(b, 1), :]
            out[pl.ds(d * values, values), at] = value.astype(jnp.bfloat16)


def fold(gain, weights):
    _, values, width = weights[0].shape
    return call(
        fold_kernel,
        shaped((4 * values, width), jnp.bfloat16),
        [],
        (1_000_000_000, 2 << 20),
        16 << 20,
        [whole()] * 5,
        whole(),
    )(gain, *weights)


def project_kernel(own, other, keyed, mixing, o0, o1, o2, o3, held, scale):
    core = lax.axis_index("core")
    blocks, size, seqs = own.shape
    squares = jnp.zeros((8, seqs), jnp.float32)
    for half, ref in ((core, own), (1 - core, other)):
        for b in range(blocks):
            part = ref[b]
            held[pl.ds(pl.multiple_of((2 * b + half) * size, size), size), :] = part
            wide = part.astype(jnp.float32)
            squares = squares + jnp.sum((wide * wide).reshape(size // 8, 8, seqs), axis=0)
    total = jnp.sum(squares, axis=0, keepdims=True)
    factor = lax.rsqrt(total / (2 * blocks * size) + NORM_EPSILON)
    scale[...] = jnp.broadcast_to(factor, scale.shape)
    rows = held[...]
    first = jnp.dot(keyed[...], rows, preferred_element_type=jnp.float32) * factor
    first = first.astype(jnp.bfloat16)
    second = jnp.dot(mixing[...], rows, preferred_element_type=jnp.float32) * factor
    second = second.astype(jnp.bfloat16)
    keys, values = first.shape[0], second.shape[0] // 4
    for d, out in enumerate((o0, o1, o2, o3)):
        out[pl.ds(0, keys), :] = first
        out[pl.ds(keys, values), :] = second[d * values : (d + 1) * values]


def project(own, other, keyed, mixing):
    blocks, size, seqs = own.shape
    rows = keyed.shape[0] + mixing.shape[0] // 4
    outs = call(
        project_kernel,
        [shaped((rows, seqs), jnp.bfloat16)] * 4
        + [shaped((2 * blocks * size, seqs), jnp.bfloat16), shaped((8, seqs), jnp.float32)],
        [],
        (1_000_000_000, 3 << 20),
        16 << 20,
        [whole()] * 4,
        [whole()] * 6,
    )(own, other, keyed, mixing)
    return outs[:4], outs[4], outs[5]


def gate_kernel(gain, w0, w1, w2, w3, rows, scale, out, held):
    values, size = w0.shape[1], gain.shape[1]
    for b in range(gain.shape[0]):
        at = pl.ds(b * size, size)
        for d, weight in enumerate((w0, w1, w2, w3)):
            value = weight[0, :, at].astype(jnp.float32) * gain[pl.ds(b, 1), :]
            held[pl.ds(d * values, values), at] = value.astype(jnp.bfloat16)
    raw = jnp.dot(held[...], rows[...], preferred_element_type=jnp.float32) * scale[0:1]
    raw = raw.astype(jnp.bfloat16).astype(jnp.float32)
    out[...] = raw * jax.nn.sigmoid(raw)


def gate(gain, weights, rows, scale):
    _, values, width = weights[0].shape
    return call(
        gate_kernel,
        shaped((4 * values, rows.shape[1]), jnp.float32),
        [pltpu.VMEM((4 * values, width), jnp.bfloat16)],
        (1_000_000_000, 3 << 20),
        16 << 20,
        [whole()] * 7,
        whole(),
    )(gain, *weights, rows, scale)


def outward_kernel(w_out, mine, theirs, held, sems):
    core = lax.axis_index("core")
    cuts, size, span = held.shape
    copies = [
        pltpu.make_async_copy(w_out.at[:, pl.ds(c * span, span)], held.at[c], sems.at[c])
        for c in range(cuts)
    ]
    for copy in copies:
        copy.start()
    pairs = span // size // 2
    for c in range(cuts):
        copies[c].wait()
        for b in range(pairs):
            for half, out in ((core, mine), (1 - core, theirs)):
                at = pl.multiple_of((2 * b + half) * size, size)
                block = held[c, :, pl.ds(at, size)].astype(jnp.float32)
                out[c * pairs + b] = block.T.astype(jnp.bfloat16)


def turn_outward(w_out):
    size, width = w_out.shape
    return call(
        outward_kernel,
        [shaped((width // size // 2, size, size), jnp.bfloat16)] * 2,
        [pltpu.VMEM((4, size, width // 4), jnp.bfloat16), pltpu.SemaphoreType.DMA((4,))],
        (1_000_000_000, 2 << 20),
        16 << 20,
        [pl.BlockSpec(memory_space=pltpu.HBM)],
        [whole()] * 2,
    )(w_out)


def recur_kernel(r0, r1, r2, r3, before, floor, head_gain, o0, o1, o2, o3, seen, ready):
    mine = lax.axis_index("tp")
    size = floor.shape[1]
    values = head_gain.shape[1]
    count = before.shape[0] // values
    steps = 4
    for d, ref in enumerate((r0, r1, r2, r3)):
        seen[mine ^ d] = ref[...]
    low = jnp.broadcast_to(floor[...], (count, size)).T
    scale = jnp.broadcast_to(head_gain[...], (count, values)).T
    forget, keys, fresh, sums, asked = [], [], [], [], []
    for t in range(steps):
        gate = low + (1.0 - low) * jax.nn.sigmoid(seen[t, pl.ds(size, size), :].astype(jnp.float32))
        forget.append(gate)
        keys.append(1.0 - gate)
        fresh.append(seen[t, pl.ds(2 * size, values), :].astype(jnp.float32))
    for t in range(steps):
        moved = seen[t, pl.ds(0, size), :].astype(jnp.float32)
        out = None
        for u in reversed(range(t + 1)):
            score = jnp.sum(moved * keys[u], axis=0, keepdims=True)
            term = score * fresh[u]
            out = term if out is None else out + term
            moved = moved * forget[u]
        sums.append(out)
        asked.append(moved.astype(jnp.bfloat16))
    half = count // 2
    lane = lax.rem(lax.broadcasted_iota(jnp.int32, (values, steps * half), 1), half)
    group = 8
    halves = []
    for h in range(2):
        wanted = jnp.concatenate([a[:, h * half : (h + 1) * half] for a in asked], axis=1)
        total = jnp.zeros((values, steps * half), jnp.float32)
        for b in range(half // group):
            first = h * half + b * group
            read = jnp.dot(
                before[pl.ds(first * values, group * values), :].astype(jnp.bfloat16),
                wanted,
                preferred_element_type=jnp.float32,
            )
            for s in range(group):
                part = read[s * values : (s + 1) * values]
                total = total + jnp.where(lane == b * group + s, part, 0.0)
        halves.append(total)
    for t in range(steps):
        cut = [total[:, t * half : (t + 1) * half] for total in halves]
        sums[t] = sums[t] + jnp.concatenate(cut, axis=1)
    for t in range(steps):
        out = sums[t]
        square = jnp.sum(out * out, axis=0, keepdims=True)
        ready[t, pl.ds(0, values), :] = (out * scale).astype(jnp.bfloat16)
        ready[t, pl.ds(values, 16), :] = three_rows(split_in_three(square), count)
    for d, ref in enumerate((o0, o1, o2, o3)):
        ref[...] = ready[mine ^ d]


def recur(received, before, floor, head_gain):
    rows, count = received[0].shape
    values = head_gain.shape[1]
    return call(
        recur_kernel,
        [shaped((values + 16, count), jnp.bfloat16)] * 4,
        [
            pltpu.VMEM((4, rows, count), jnp.bfloat16),
            pltpu.VMEM((4, values + 16, count), jnp.bfloat16),
        ],
        (1_000_000_000, 2 << 20),
        16 << 20,
        [whole()] * 7,
        [whole()] * 4,
    )(*received, before, floor, head_gain)


def hide_kernel(p0, p1, p2, p3, gates, hidden):
    mine = lax.axis_index("tp")
    values = hidden.shape[0] // 4
    parts = (p0, p1, p2, p3)
    total = None
    for ref in parts:
        square = jnp.sum(ref[pl.ds(values, 16), :].astype(jnp.float32), axis=0, keepdims=True)
        total = square if total is None else total + square
    factor = lax.rsqrt(total / hidden.shape[0] + NORM_EPSILON)
    for d, ref in enumerate(parts):
        at = pl.multiple_of((mine ^ d) * values, values)
        value = ref[pl.ds(0, values), :].astype(jnp.float32) * factor
        value = value * gates[pl.ds(d * values, values), :]
        hidden[pl.ds(at, values), :] = value.astype(jnp.bfloat16)


def hide(parts, gates):
    return call(
        hide_kernel,
        shaped(gates.shape, jnp.bfloat16),
        [],
        (1_000_000, 1 << 18),
        16 << 20,
        [whole()] * 5,
        whole(),
    )(*parts, gates)


def emit_kernel(hidden, other, ours, theirs, out):
    for b in range(out.shape[0]):
        part = jnp.dot(ours[b], hidden[...], preferred_element_type=jnp.float32)
        part = part + jnp.dot(theirs[b], other[...], preferred_element_type=jnp.float32)
        out[b] = part.astype(jnp.bfloat16)


def emit(hidden, other, ours, theirs):
    blocks, size, _ = ours.shape
    return call(
        emit_kernel,
        shaped((blocks, size, hidden.shape[1]), jnp.bfloat16),
        [],
        (100_000_000, 2 << 20),
        16 << 20,
        [whole()] * 4,
        whole(),
    )(hidden, other, ours, theirs)


def sum_kernel(parts, out):
    total = parts[0].astype(jnp.float32)
    for b in range(1, parts.shape[0]):
        total = total + parts[b].astype(jnp.float32)
    out[...] = total.astype(out.dtype)


def sums(parts):
    return call(
        sum_kernel,
        shaped(parts.shape[1:], jnp.bfloat16),
        [],
        (1_000_000, 1 << 20),
        8 << 20,
        [whole()],
        whole(),
    )(parts)


def body(
    tokens,
    input_norm_gain,
    w_query,
    w_forget,
    w_input,
    w_gate,
    forget_floor,
    head_gain,
    w_out,
    state,
    prev_forget,
    prev_input,
    accepted,
):
    planes, group = lax.axis_size("zy"), lax.axis_size("tp")
    seqs, proposals, features = tokens.shape
    _, size = w_query.shape
    swap = [(0, 1), (1, 0)]
    hops = [[(i, i ^ d) for i in range(group)] for d in range(group)]

    def passed(parts):
        far = lax.ppermute(parts[2], "tp", hops[2])
        wrap = lax.ppermute(parts[3], "tp", hops[3])
        near = lax.ppermute(parts[1], "tp", hops[1])
        return [parts[0], near, far, wrap]

    gain = input_norm_gain.reshape(-1, size)
    inputs = passed([w_input] * group)
    own = lax.all_to_all(source(tokens.transpose(1, 2, 0), planes), ("zy", "tp"), 0, 0, tiled=True)
    own = own.reshape(planes, group * features, seqs)
    other = lax.ppermute(own, "core", swap)
    wrap = lax.ppermute(w_gate, "tp", hops[3])
    far = lax.ppermute(w_gate, "tp", hops[2])
    near = lax.ppermute(w_gate, "tp", hops[1])
    gates = [w_gate, near, far, wrap]
    keyed = turn(gain, w_query, w_forget)
    mixing = fold(gain, inputs)
    new_state = advance(
        accepted,
        prev_forget,
        prev_input.reshape(seqs, proposals, -1).transpose(1, 2, 0),
        state[:, 0],
    )

    sends, rows, scale = project(own, other, keyed, mixing)
    received = passed(sends)
    ours, theirs = turn_outward(w_out)
    theirs = lax.ppermute(theirs, "core", swap)
    shown = recur(received, new_state.reshape(-1, size), forget_floor[None], head_gain[None])
    parts = passed(shown)
    opened = gate(gain, gates, rows, scale)
    hidden = hide(parts, opened)
    kept = emit(hidden, lax.ppermute(hidden, "core", swap), ours, theirs)
    terms = lax.all_to_all(
        kept.reshape(planes * group, features, seqs), ("zy", "tp"), 0, 0, tiled=True
    )
    mixed = sums(terms.reshape(planes, group, features, seqs))
    return mixed.transpose(2, 0, 1), new_state[:, None]


def solution(mesh):
    kv, tp = mesh.shape["kv"], mesh.shape["tp"]
    finer = Mesh(mesh.devices.reshape(kv // 2, 2, tp), ("zy", "core", "tp"))
    rows = ("zy", "core")
    placed = (
        P(None, None, (*rows, "tp")),
        P(),
        P(None, rows),
        P(None, rows),
        P(rows, "tp", None),
        P(rows, "tp", None),
        P(rows),
        P("tp"),
        P(rows, None),
        P(None, rows, "tp", None),
        P(None, None, rows),
        P(None, None, rows, "tp"),
        P(),
    )

    return jax.shard_map(
        body,
        mesh=finer,
        in_specs=placed,
        out_specs=(P(None, None, (*rows, "tp")), P(None, rows, "tp", None)),
        check_vma=False,
    )
```
